32 devices in a mesh: grp: 2 (over y), ep: 8 (over z, core), tp: 2 (over x).
Axes of the slice: x: 2, y: 2, z: 4, core: 2. Of those that a mesh axis runs over, the one named last changes fastest.
Arguments:
- recurrence_query_input: bfloat16 [2048, 2048], P(('grp', 'ep'), 'tp'), parts along dimension 0, may hold values from -6 to 6
- forget_gate_input: bfloat16 [2048, 2048], P(('grp', 'ep'), 'tp'), parts along dimension 0, may hold values from -6.5 to 6.5
- recurrence_value_input: bfloat16 [2048, 2048], P(('grp', 'ep'), 'tp'), parts along dimension 0, may hold values from -6 to 6
- output_gate_input: bfloat16 [2048, 2048], P(('grp', 'ep'), 'tp'), parts along dimension 0, may hold values from -6 to 6
- forget_lower_margin: float32 [2048], P('tp'), may hold values from 0 to 0.1
- position_decay_extra: float32 [2048, 16], P(('grp', 'ep'), 'tp'), parts along dimension 0, may hold values from -2.1 to 0
- head_norm_gain: float32 [2048], P('tp'), may hold values from 0.1 to 1.9
- recurrence_out_weight: bfloat16 [2048, 2048], P('tp'), may hold values from -0.125 to 0.125
- expert_hidden_state: bfloat16 [2048, 2048], P(('grp', 'ep')), parts along dimension 0, may hold values from -6 to 6
- chosen_expert_index: int32 [2048, 4], P(('grp', 'ep')), parts along dimension 0, may hold values from 0 to 7, all different within a row; in each aligned block of 128 rows (0 to 127, 128 to 255, ...) at most 128 rows name the same one
- chosen_expert_score: float32 [2048, 4], P(('grp', 'ep')), parts along dimension 0, may hold values from 0.02 to 1
- expert_norm_gain: float32 [2048], replicated, may hold values from 0.1 to 1.9
- routed_gate_weight: bfloat16 [8, 2048, 1024], P('ep', None, 'tp'), may hold values from -0.125 to 0.125
- routed_up_weight: bfloat16 [8, 2048, 1024], P('ep', None, 'tp'), may hold values from -0.125 to 0.125
- routed_down_weight: bfloat16 [8, 1024, 2048], P('ep', None, 'tp'), may hold values from -0.1875 to 0.1875
- shared_gate_weight: bfloat16 [2048, 1024], P(None, 'tp'), may hold values from -0.125 to 0.125
- shared_up_weight: bfloat16 [2048, 1024], P(None, 'tp'), may hold values from -0.125 to 0.125
- shared_down_weight: bfloat16 [1024, 2048], P(None, 'tp'), may hold values from -0.1875 to 0.1875
Outputs:
- recurrence_output: bfloat16 [2048, 2048], P(('grp', 'ep', 'tp')), parts along dimension 0
- expert_out: bfloat16 [2048, 2048], P(('grp', 'ep'), 'tp'), parts along dimension 0
The draws below stay inside these ranges and needn't reach their ends.
There are 2 independent parts, one for each index of `grp`. The reference program is written for one: setup_inputs(seed, part) draws one part's arguments, and reference() takes and returns one part's arrays. A program takes and returns all parts, laid end to end along the dimension named above; an argument that names none is the same for every part. Nothing has to cross between parts.
Inputs may be any that keep to these rules, and one draw needn't show every extreme that they name: `chosen_expert_index`: each row names 4 different experts. In each aligned block of 128 rows (the rows of one index of ep) no expert is named by more than 128 rows, and in every draw some block names some expert exactly 128 times.
All inputs are finite; a program needn't handle non-finite values.
Results may differ from the reference program's by a relative error of at most 0.015.
Values may be sent and summed in bfloat16 or wider, within the bound.
A program may use at most 64 MiB of HBM per device.

```python
import math
import jax
import jax.numpy as jnp
import numpy as np
from jax import lax

D = 2048
HEADS = 16
HEAD_CHANNELS = 128
W = 2048
BLK = 64
FF = 1024
TOP_K = 4
EXPERTS = 8
TOKA_DEV = 128
TOKB_DEV = 128
SEQ_A = 1024
TOK_B = 1024
CAP = 128
N_EP = 8
N_TP = 2


def draw_forget_gate_input(key, part):
    noise_key, shift_key = jax.random.split(jax.random.fold_in(key, 11))
    noise = jnp.clip(jax.random.normal(noise_key, (SEQ_A, W), jnp.float32), -5.0, 5.0)
    shifts = jax.random.uniform(shift_key, (SEQ_A // TOKA_DEV, 1, 1), jnp.float32, -1.5, 1.5)
    shifted = noise.reshape(SEQ_A // TOKA_DEV, TOKA_DEV, W) + shifts
    return shifted.reshape(SEQ_A, W).astype(jnp.bfloat16)


def draw_forget_lower_margin(key, part):
    pick_key, slow_key, fast_key = jax.random.split(jax.random.fold_in(key, 23), 3)
    slow_count = HEADS // 2
    slow_heads = (jax.random.permutation(pick_key, HEADS) < slow_count)[:, None]
    slow = 2.0 * jnp.exp(jax.random.uniform(slow_key, (HEADS, HEAD_CHANNELS), jnp.float32, math.log(0.1), math.log(0.6))) / SEQ_A
    fast = jnp.exp(jax.random.uniform(fast_key, (HEADS, HEAD_CHANNELS), jnp.float32, math.log(0.03), math.log(0.09)))
    return jnp.where(slow_heads, slow, fast).reshape(W).astype(jnp.float32)


def draw_position_decay_extra(key, part):
    place_key, depth_key, count_key = jax.random.split(jax.random.fold_in(key, 37), 3)
    spots = jax.random.randint(place_key, (3, HEADS), 0, SEQ_A)
    counts = jax.random.randint(count_key, (1, HEADS), 1, 4)
    active = jnp.arange(3)[:, None] < counts
    depth = jnp.log(jax.random.uniform(depth_key, (3, HEADS), jnp.float32, 0.5, 0.8))
    positions = jnp.arange(SEQ_A)[:, None, None]
    hits = (positions == spots[None]) & active[None]
    return jnp.sum(jnp.where(hits, depth[None], 0.0), axis=1).astype(jnp.float32)


def levels(rng, shape, pieces, smallest, largest):
    def one(axis_at, parts):
        heights = jax.random.uniform(jax.random.fold_in(jax.random.fold_in(rng, 6), axis_at), (parts,), jnp.float32, smallest / len(pieces), largest / len(pieces))
        return jnp.repeat(jnp.exp(heights), shape[axis_at] // parts).reshape((-1,) + (1,) * (len(shape) - axis_at - 1))

    factor_of = one(*pieces[0])
    for cut in pieces[1:]:
        factor_of = factor_of * one(*cut)
    return factor_of


def shared_out(key, own, number, rows, number_of, top, reach, skew):
    sequence = jax.random.permutation(key, number_of)
    packed, common = load_shares(number_of, rows * top, reach, skew, True), load_shares(number_of, rows * top, reach, skew, False)
    places = jnp.arange(number_of)

    def named(tallies, turn):
        used = int((tallies > 0).sum())
        fixed = max(1, used // 4)
        moved = fixed + (places - fixed + turn * (used - fixed)) % max(1, number_of - fixed)
        return jnp.zeros((number_of,), jnp.int32).at[sequence[jnp.where(places < fixed, places, moved)]].set(jnp.asarray(tallies, jnp.int32))

    tallies = jnp.where(number % 4 == 0, named(packed, number // 4), named(common, number - number // 4 - 1))
    mixed = jax.random.permutation(jax.random.fold_in(own, 3), number_of)
    giver, taker = mixed[0:number_of // 2 * 2:2], mixed[1:number_of // 2 * 2:2]
    margin = jnp.minimum(tallies[giver] - 1, reach - tallies[taker]) // 2
    margin = jnp.where((giver == sequence[0]) | (taker == sequence[0]) | (tallies[taker] == 0), 0, jnp.maximum(margin, 0))
    moved = jax.random.randint(jax.random.fold_in(own, 4), (number_of // 2,), 0, 1 << 20) % (margin + 1)
    tallies = tallies.at[giver].add(-moved).at[taker].add(moved)
    members = jnp.searchsorted(jnp.cumsum(tallies), jnp.arange(rows * top), side="right").astype(jnp.int32)
    table = members.reshape(top, rows).T
    table = table[jax.random.permutation(jax.random.fold_in(own, 1), rows)]
    turn = jax.random.randint(jax.random.fold_in(own, 2), (rows, 1), 0, top)
    return jnp.take_along_axis(table, (jnp.arange(top)[None, :] + turn) % top, axis=1)


def load_shares(count, total, limit, lean, full):
    portions = [(1 << 20) // math.isqrt(standing ** lean) + 1 for standing in range(1, count + 1)]
    largest = limit if full else min(limit, max(-(-total // count), total * portions[0] // sum(portions)))
    least = 1 if total - largest >= count - 1 else 0
    holding, spare = [largest] + [least] * (count - 1), total - largest - least * (count - 1)
    while spare > 0:
        free = [i for i in range(1, count) if holding[i] < largest] or [i for i in range(1, count) if holding[i] < limit]
        pool, remaining = sum([portions[i] for i in free]), spare
        for i in free:
            more = min(limit - holding[i], max(1, remaining * portions[i] // pool), spare)
            holding[i] = holding[i] + more
            spare = spare - more
    return np.array(holding)


def gaussian(key, extent, width, reach, cuts=(), held_as=jnp.bfloat16):
    entries = jax.random.normal(key, extent, jnp.float32) * width
    if len(cuts) > 0:
        entries = levels(key, extent, cuts, -0.22, 0.18) * entries
    return jnp.clip(entries, min=-reach, max=reach).astype(held_as)


def setup_inputs(seed: int = 0, part: int = 0) -> dict:
    keys = jax.random.split(jax.random.key(seed), 19)
    part_splits = jax.random.split(jax.random.fold_in(keys[18], part), 19)
    recurrence_query_input = gaussian(part_splits[0], (SEQ_A, W), 1.0, 6.0, ((0, 8), (1, 2)))
    forget_gate_input = draw_forget_gate_input(jax.random.fold_in(jax.random.fold_in(keys[18], part), 71), part)
    recurrence_value_input = gaussian(part_splits[2], (SEQ_A, W), 1.0, 6.0, ((0, 8), (1, 2)))
    output_gate_input = gaussian(part_splits[3], (SEQ_A, W), 1.0, 6.0, ((0, 8), (1, 2)))
    forget_lower_margin = draw_forget_lower_margin(jax.random.fold_in(keys[18], 71), part)
    position_decay_extra = draw_position_decay_extra(jax.random.fold_in(jax.random.fold_in(keys[18], part), 71), part)
    head_norm_gain = jnp.clip(1.0 + 0.18 * jax.random.normal(keys[6], (W,), jnp.float32), 0.1, 1.9)
    recurrence_out_weight = gaussian(keys[7], (W, D), W ** -0.5, 0.125, ((0, 2),))
    expert_hidden_state = gaussian(part_splits[8], (TOK_B, D), 1.0, 6.0, ((0, 8),))
    chosen_expert_index_keys = jax.random.split(jax.random.fold_in(part_splits[9], 1), TOK_B // TOKB_DEV)
    chosen_expert_index_turns = jax.random.permutation(jax.random.fold_in(part_splits[9], 3), TOK_B // TOKB_DEV)
    chosen_expert_index = jax.vmap(lambda own, number: shared_out(jax.random.fold_in(part_splits[9], 2), own, number, TOKB_DEV, EXPERTS, TOP_K, CAP, 1))(chosen_expert_index_keys, chosen_expert_index_turns).reshape((TOK_B, TOP_K))
    chosen_expert_score = jnp.clip(jnp.exp(math.log(1.0) - 3.912023 * jax.random.uniform(part_splits[10], (TOK_B, TOP_K), jnp.float32) ** levels(part_splits[10], (TOK_B, TOP_K), ((0, 8),), -0.2, 0.2)), 0.02, 1.0)
    expert_norm_gain = jnp.clip(1.0 + 0.18 * jax.random.normal(keys[11], (D,), jnp.float32), 0.1, 1.9)
    routed_gate_weight = gaussian(keys[12], (EXPERTS, D, FF), D ** -0.5, 0.125, ((0, 8), (2, 2)))
    routed_up_weight = gaussian(keys[13], (EXPERTS, D, FF), D ** -0.5, 0.125, ((0, 8), (2, 2)))
    routed_down_weight = gaussian(keys[14], (EXPERTS, FF, D), FF ** -0.5, 0.1875, ((0, 8), (2, 2)))
    shared_gate_weight = gaussian(keys[15], (D, FF), D ** -0.5, 0.125, ((1, 2),))
    shared_up_weight = gaussian(keys[16], (D, FF), D ** -0.5, 0.125, ((1, 2),))
    shared_down_weight = gaussian(keys[17], (FF, D), FF ** -0.5, 0.1875, ((1, 2),))
    return dict(recurrence_query_input=recurrence_query_input, forget_gate_input=forget_gate_input, recurrence_value_input=recurrence_value_input, output_gate_input=output_gate_input, forget_lower_margin=forget_lower_margin, position_decay_extra=position_decay_extra, head_norm_gain=head_norm_gain, recurrence_out_weight=recurrence_out_weight, expert_hidden_state=expert_hidden_state, chosen_expert_index=chosen_expert_index, chosen_expert_score=chosen_expert_score, expert_norm_gain=expert_norm_gain, routed_gate_weight=routed_gate_weight, routed_up_weight=routed_up_weight, routed_down_weight=routed_down_weight, shared_gate_weight=shared_gate_weight, shared_up_weight=shared_up_weight, shared_down_weight=shared_down_weight)


EPSILON = 1e-06
ROUTED_SCALE = 2.5
HIGHEST_PRECISION = lax.Precision.HIGHEST

def recurrence(queries, key_gate_value, decay_logarithm, value_rows):
    length = queries.shape[0]
    blocks = length // BLK

    def split_heads(tensor):
        return tensor.reshape(blocks, BLK, HEADS, HEAD_CHANNELS).transpose(2, 0, 1, 3)
    query_heads = split_heads(queries)
    key_heads = split_heads(key_gate_value)
    value_heads = split_heads(value_rows)
    cum_decay = jnp.cumsum(split_heads(decay_logarithm), axis=2)
    middle = cum_decay[:, :, BLK // 2 - 1:BLK // 2]
    block_end = cum_decay[:, :, BLK - 1:BLK]
    scores = jnp.einsum('hncd,hnsd->hncs', query_heads * jnp.exp(cum_decay - middle), key_heads * jnp.exp(middle - cum_decay), precision=HIGHEST_PRECISION)
    causal = jnp.tril(jnp.ones((BLK, BLK), dtype=bool))
    scores = jnp.where(causal, scores, 0.0)
    within = jnp.einsum('hncs,hnse->hnce', scores, value_heads, precision=HIGHEST_PRECISION)
    updates = jnp.einsum('hncd,hnce->nhde', key_heads * jnp.exp(block_end - cum_decay), value_heads, precision=HIGHEST_PRECISION)
    block_decay = jnp.exp(block_end[:, :, 0, :]).transpose(1, 0, 2)

    def advance(carry_state, inputs):
        factor, update = inputs
        return (factor[..., None] * carry_state + update, carry_state)
    initial = jnp.zeros((HEADS, HEAD_CHANNELS, HEAD_CHANNELS), jnp.float32)
    _, starts = lax.scan(advance, initial, (block_decay, updates))
    carried = jnp.einsum('hncd,nhde->hnce', query_heads * jnp.exp(cum_decay), starts, precision=HIGHEST_PRECISION)
    return (within + carried).transpose(1, 2, 0, 3).reshape(length, HEADS, HEAD_CHANNELS)

def recurrence_reference(recurrence_query_input, forget_gate_input, recurrence_value_input, output_gate_input, forget_lower_margin, position_decay_extra, head_norm_gain, recurrence_out_weight):
    length = recurrence_query_input.shape[0]
    queries = jax.nn.silu(recurrence_query_input.astype(jnp.float32))
    key_gate_value = forget_lower_margin[None, :] * jax.nn.sigmoid(-forget_gate_input.astype(jnp.float32))
    decay_logarithm = jnp.log1p(-key_gate_value) + jnp.repeat(position_decay_extra, HEAD_CHANNELS, axis=1)
    value_rows = recurrence_value_input.astype(jnp.float32)
    outputs = recurrence(queries, key_gate_value, decay_logarithm, value_rows)
    factor = lax.rsqrt(lax.optimization_barrier(jnp.mean(outputs * outputs, axis=2, keepdims=True)) + EPSILON)
    normed = (outputs * factor).reshape(length, W) * head_norm_gain[None, :]
    gated_rows = (normed * jax.nn.silu(output_gate_input.astype(jnp.float32))).astype(jnp.bfloat16)
    columns = W // N_TP
    summed = jnp.zeros((length, D), jnp.float32)
    for member in range(N_TP):
        partial_sum = jnp.dot(gated_rows[:, member * columns:(member + 1) * columns], recurrence_out_weight[member * columns:(member + 1) * columns], preferred_element_type=jnp.float32).astype(jnp.bfloat16)
        summed = summed + lax.optimization_barrier(partial_sum).astype(jnp.float32)
    return summed.astype(jnp.bfloat16)

def expert_reference(expert_hidden_state, chosen_expert_index, chosen_expert_score, expert_norm_gain, routed_gate_weight, routed_up_weight, routed_down_weight, shared_gate_weight, shared_up_weight, shared_down_weight):
    tokens = expert_hidden_state.shape[0]
    features = expert_hidden_state.astype(jnp.float32)
    normed = (features * lax.rsqrt(lax.optimization_barrier(jnp.mean(features * features, axis=1, keepdims=True)) + EPSILON) * expert_norm_gain[None, :]).astype(jnp.bfloat16)
    gates = ROUTED_SCALE * chosen_expert_score / lax.optimization_barrier(jnp.sum(chosen_expert_score, axis=1, keepdims=True))
    blocked = chosen_expert_index.reshape(N_EP, TOKB_DEV * TOP_K)
    onehot = (blocked[:, :, None] == jnp.arange(EXPERTS, dtype=jnp.int32)[None, None, :]).astype(jnp.int32)
    places = lax.optimization_barrier(jnp.sum(onehot * (jnp.cumsum(onehot, axis=1) - 1), axis=2)).reshape(-1)
    sources = jnp.arange(tokens * TOP_K, dtype=jnp.int32) // (TOKB_DEV * TOP_K)
    slots = (chosen_expert_index.reshape(-1) * N_EP + sources) * CAP + places
    owners = jnp.full((EXPERTS * N_EP * CAP,), tokens, jnp.int32).at[slots].set(jnp.arange(tokens * TOP_K, dtype=jnp.int32) // TOP_K)
    padded = jnp.concatenate([normed, jnp.zeros((1, D), jnp.bfloat16)], axis=0)
    grouped = padded[owners].reshape(EXPERTS, N_EP * CAP, D)

    def one_expert(inputs):
        slot_rows, gate_matrix, up_matrix, down_matrix = inputs
        hidden = (jax.nn.silu(jnp.dot(slot_rows, gate_matrix, preferred_element_type=jnp.float32)) * jnp.dot(slot_rows, up_matrix, preferred_element_type=jnp.float32)).astype(jnp.bfloat16)
        return jnp.dot(hidden, down_matrix, preferred_element_type=jnp.float32).astype(jnp.bfloat16)
    results = lax.map(one_expert, (grouped, routed_gate_weight, routed_up_weight, routed_down_weight))
    picked = results.reshape(EXPERTS * N_EP * CAP, D)[slots].reshape(tokens, TOP_K, D)
    shared_hidden = (jax.nn.silu(jnp.dot(normed, shared_gate_weight, preferred_element_type=jnp.float32)) * jnp.dot(normed, shared_up_weight, preferred_element_type=jnp.float32)).astype(jnp.bfloat16)
    shared_result = jnp.dot(shared_hidden, shared_down_weight, preferred_element_type=jnp.float32)
    combined = shared_result + lax.optimization_barrier(jnp.sum(gates[:, :, None] * picked.astype(jnp.float32), axis=1))
    return combined.astype(jnp.bfloat16)

def reference(recurrence_query_input, forget_gate_input, recurrence_value_input, output_gate_input, forget_lower_margin, position_decay_extra, head_norm_gain, recurrence_out_weight, expert_hidden_state, chosen_expert_index, chosen_expert_score, expert_norm_gain, routed_gate_weight, routed_up_weight, routed_down_weight, shared_gate_weight, shared_up_weight, shared_down_weight):
    recurrence_output = recurrence_reference(recurrence_query_input, forget_gate_input, recurrence_value_input, output_gate_input, forget_lower_margin, position_decay_extra, head_norm_gain, recurrence_out_weight)
    expert_out = expert_reference(expert_hidden_state, chosen_expert_index, chosen_expert_score, expert_norm_gain, routed_gate_weight, routed_up_weight, routed_down_weight, shared_gate_weight, shared_up_weight, shared_down_weight)
    return (recurrence_output, expert_out)
```

```python
import functools

import jax
import jax.numpy as jnp
from jax import lax
from jax.experimental import pallas as pl
from jax.experimental.pallas import tpu as pltpu
from jax.sharding import PartitionSpec as P

HEAD_CHANNELS = 128
BLK = 64


EPSILON = 1e-06
ROUTED_SCALE = 2.5
PRECISION = lax.Precision.DEFAULT


DECAY_ROWS = 16


def carried_in(decay, state, axis):
    count, index = (lax.axis_size(axis), lax.axis_index(axis))
    depth = state.shape[1]
    rows = jnp.broadcast_to(decay[:, None, :], (decay.shape[0], DECAY_ROWS, decay.shape[1]))
    sent = jnp.concatenate([state, rows], axis=1).astype(jnp.bfloat16)
    everything = lax.all_gather(sent, axis)
    before = jnp.zeros_like(state)
    for k in range(count - 1):
        part = everything[k].astype(jnp.float32)
        new = part[:, depth : depth + 1] * before + part[:, :depth]
        before = jnp.where(k < index, new, before)
    return before


def mixer_half(
    recurrence_query_input,
    forget_gate_input,
    recurrence_value_input,
    output_gate_input,
    forget_lower_margin,
    position_decay_extra,
    head_norm_gain,
    recurrence_out_weight,
):
    length = recurrence_query_input.shape[0]
    head_tensor = position_decay_extra.shape[1]
    blocks = length // BLK
    queries = jax.nn.silu(recurrence_query_input.astype(jnp.float32))
    key_gate_value = forget_lower_margin[None, :] * jax.nn.sigmoid(
        -forget_gate_input.astype(jnp.float32)
    )
    decay_logarithm = jnp.log1p(-key_gate_value) + jnp.repeat(
        position_decay_extra, HEAD_CHANNELS, axis=1
    )
    value_rows = recurrence_value_input.astype(jnp.float32)

    def split_heads(tensor):
        return tensor.reshape(blocks, BLK, head_tensor, HEAD_CHANNELS).transpose(2, 0, 1, 3)

    query_heads = split_heads(queries)
    key_heads = split_heads(key_gate_value)
    value_heads = split_heads(value_rows)
    cum_decay = jnp.cumsum(split_heads(decay_logarithm), axis=2)
    middle = cum_decay[:, :, BLK // 2 - 1 : BLK // 2]
    block_end = cum_decay[:, :, BLK - 1 : BLK]
    scores = jnp.einsum(
        "hncd,hnsd->hncs",
        query_heads * jnp.exp(cum_decay - middle),
        key_heads * jnp.exp(middle - cum_decay),
        precision=PRECISION,
    )
    causal = jnp.tril(jnp.ones((BLK, BLK), dtype=bool))
    scores = jnp.where(causal, scores, 0.0)
    within = jnp.einsum("hncs,hnse->hnce", scores, value_heads, precision=PRECISION)
    updates = jnp.einsum(
        "hncd,hnce->nhed",
        key_heads * jnp.exp(block_end - cum_decay),
        value_heads,
        precision=PRECISION,
    )
    block_log = block_end[:, :, 0, :]
    block_decay = jnp.exp(block_log).transpose(1, 0, 2)

    state = jnp.zeros_like(updates[0])
    starts_list = []
    for block in range(blocks):
        starts_list.append(state)
        state = block_decay[block][:, None, :] * state + updates[block]
    local_final, local_starts = state, jnp.stack(starts_list)
    device_decay = jnp.exp(jnp.sum(block_log, axis=1))
    incoming = carried_in(device_decay, local_final, "ep")
    before = jnp.exp(jnp.cumsum(block_log, axis=1) - block_log).transpose(1, 0, 2)
    starts = local_starts + before[:, :, None, :] * incoming[None]
    carried = jnp.einsum(
        "hncd,nhed->hnce", query_heads * jnp.exp(cum_decay), starts, precision=PRECISION
    )
    outputs = (within + carried).transpose(1, 2, 0, 3).reshape(length, head_tensor, HEAD_CHANNELS)
    factor = lax.rsqrt(jnp.mean(outputs * outputs, axis=2, keepdims=True) + EPSILON)
    normed = (outputs * factor).reshape(length, head_tensor * HEAD_CHANNELS) * head_norm_gain[
        None, :
    ]
    gated_rows = (normed * jax.nn.silu(output_gate_input.astype(jnp.float32))).astype(jnp.bfloat16)
    partial = jnp.dot(
        gated_rows, recurrence_out_weight, preferred_element_type=jnp.float32
    ).astype(jnp.bfloat16)
    if lax.axis_size("tp") != 2:
        return lax.psum_scatter(partial, "tp", scatter_dimension=0, tiled=True)
    which, kept_rows = lax.axis_index("tp"), length // 2
    kept = lax.dynamic_slice_in_dim(partial, which * kept_rows, kept_rows)
    sent = lax.dynamic_slice_in_dim(partial, (1 - which) * kept_rows, kept_rows)
    received = lax.ppermute(sent, "tp", [(0, 1), (1, 0)])
    return (kept.astype(jnp.float32) + received.astype(jnp.float32)).astype(jnp.bfloat16)


def expert_half(
    expert_hidden_state,
    chosen_expert_index,
    chosen_expert_score,
    expert_norm_gain,
    routed_gate_weight,
    routed_up_weight,
    routed_down_weight,
    shared_gate_weight,
    shared_up_weight,
    shared_down_weight,
):
    tokens, top = chosen_expert_index.shape
    local_experts = routed_gate_weight.shape[0]
    devices = lax.axis_size("ep")
    experts = local_experts * devices
    capacity = min(tokens, 2 * tokens * top // experts)
    width_out = routed_down_weight.shape[2]
    features = expert_hidden_state.astype(jnp.float32)
    normed = (
        features
        * lax.rsqrt(jnp.mean(features * features, axis=1, keepdims=True) + EPSILON)
        * expert_norm_gain[None, :]
    ).astype(jnp.bfloat16)
    gates = ROUTED_SCALE * chosen_expert_score / jnp.sum(chosen_expert_score, axis=1, keepdims=True)
    flat_ids = chosen_expert_index.reshape(-1)
    onehot = (flat_ids[:, None] == jnp.arange(experts, dtype=jnp.int32)[None, :]).astype(jnp.int32)
    places = jnp.sum(onehot * (jnp.cumsum(onehot, axis=0) - 1), axis=1)
    slots = flat_ids * capacity + places
    owners = (
        jnp.full((experts * capacity,), tokens, jnp.int32)
        .at[slots]
        .set(jnp.arange(tokens * top, dtype=jnp.int32) // top)
    )
    padded = jnp.concatenate([normed, jnp.zeros((1, normed.shape[1]), jnp.bfloat16)], axis=0)
    outgoing = padded[owners].reshape(experts, capacity, normed.shape[1])
    piece = lax.all_to_all(outgoing, "ep", split_axis=0, concat_axis=0, tiled=True)
    grouped = piece.reshape(devices, local_experts, piece.shape[1], piece.shape[2])
    gate_part = jnp.einsum(
        "secd,edh->sech", grouped, routed_gate_weight, preferred_element_type=jnp.float32
    )
    up_part = jnp.einsum(
        "secd,edh->sech", grouped, routed_up_weight, preferred_element_type=jnp.float32
    )
    hidden = (jax.nn.silu(gate_part) * up_part).astype(jnp.bfloat16)
    hidden_rows = hidden.reshape(devices * local_experts, piece.shape[1], hidden.shape[3])
    flat_hidden = hidden_rows.reshape(experts * capacity, hidden_rows.shape[2])
    shared_hidden = (
        jax.nn.silu(jnp.dot(normed, shared_gate_weight, preferred_element_type=jnp.float32))
        * jnp.dot(normed, shared_up_weight, preferred_element_type=jnp.float32)
    ).astype(jnp.bfloat16)
    start_values = (
        jnp.zeros((experts * capacity, width_out), jnp.float32),
        jnp.zeros((tokens, width_out), jnp.float32),
    )
    routed_piece = lax.all_gather(flat_hidden, "tp", axis=1, tiled=True)
    shared_piece = lax.all_gather(shared_hidden, "tp", axis=1, tiled=True)
    count = routed_piece.shape[1]
    grouped = routed_piece.reshape(devices, local_experts, capacity, count)
    routed = jnp.einsum(
        "secn,enk->seck", grouped, routed_down_weight, preferred_element_type=jnp.float32
    )
    shared = jnp.dot(shared_piece, shared_down_weight, preferred_element_type=jnp.float32)
    routed_sum = routed.reshape(start_values[0].shape)
    answers = routed_sum.astype(jnp.bfloat16).reshape(experts, capacity, width_out)
    returned = lax.all_to_all(answers, "ep", split_axis=0, concat_axis=0, tiled=True)
    picked_rows = returned.reshape(experts * capacity, width_out)[slots].reshape(
        tokens, top, width_out
    )
    combined = shared + jnp.sum(gates[:, :, None] * picked_rows.astype(jnp.float32), axis=1)
    return combined.astype(jnp.bfloat16)


MESH = pl.DeviceIdType.MESH
LANES = 128
SPLIT = 2
KINDS = ("NO", "SR", "SL", "RF", "MA", "ST", "H", "D", "S", "FIN", "MB", "MO")
NUMBER = {name: place for place, name in enumerate(KINDS)}


ORDERS = (
    (
        ("SR", 0, 0), ("SR", 0, 1), ("MA", 0, 0), ("H", 4, 0), ("H", 0, 0), ("ST", 0, 0),
        ("H", 0, 1), ("MB", 0, 0), ("RF", 1, 0), ("D", 4, 0), ("D", 0, 0), ("H", 1, 0),
        ("RF", 1, 1), ("D", 0, 1), ("H", 1, 1), ("RF", 2, 0), ("MO", 0, 0), ("H", 2, 0),
        ("D", 1, 0), ("RF", 2, 1), ("S", 1, 0), ("D", 1, 1), ("H", 2, 1), ("S", 1, 1),
        ("D", 2, 0), ("RF", 3, 0), ("S", 2, 0), ("H", 3, 0), ("D", 2, 1), ("S", 2, 1),
        ("RF", 3, 1), ("H", 3, 1), ("D", 3, 0), ("S", 3, 0), ("D", 3, 1), ("S", 3, 1),
        ("FIN", 0, 0), ("FIN", 0, 1),
    ),
    (
        ("SL", 1, 0), ("SR", 1, 0), ("SL", 1, 1), ("SR", 1, 1), ("MA", 0, 0), ("H", 4, 0),
        ("H", 1, 0), ("H", 1, 1), ("RF", 0, 0), ("RF", 2, 0), ("D", 4, 0), ("H", 0, 0),
        ("H", 2, 0), ("D", 1, 0), ("RF", 0, 1), ("RF", 2, 1), ("D", 1, 1), ("H", 0, 1),
        ("ST", 0, 0), ("H", 2, 1), ("D", 0, 0), ("RF", 3, 0), ("MB", 0, 0), ("D", 2, 0),
        ("H", 3, 0), ("D", 0, 1), ("RF", 3, 1), ("D", 2, 1), ("H", 3, 1), ("MO", 0, 0),
        ("D", 3, 0), ("S", 2, 0), ("D", 3, 1), ("FIN", 1, 0), ("S", 2, 1), ("FIN", 1, 1),
        ("S", 3, 0), ("S", 3, 1), ("S", 0, 0), ("S", 0, 1),
    ),
    (
        ("SR", 2, 0), ("SL", 2, 0), ("SR", 2, 1), ("SL", 2, 1), ("MA", 0, 0), ("H", 4, 0),
        ("H", 2, 0), ("H", 2, 1), ("RF", 3, 0), ("RF", 1, 0), ("D", 4, 0), ("H", 3, 0),
        ("H", 1, 0), ("D", 2, 0), ("RF", 3, 1), ("RF", 1, 1), ("D", 2, 1), ("H", 3, 1),
        ("H", 1, 1), ("D", 3, 0), ("RF", 0, 0), ("D", 1, 0), ("H", 0, 0), ("D", 3, 1),
        ("RF", 0, 1), ("D", 1, 1), ("H", 0, 1), ("ST", 0, 0), ("D", 0, 0), ("MB", 0, 0),
        ("D", 0, 1), ("S", 1, 0), ("MO", 0, 0), ("S", 1, 1), ("FIN", 2, 0), ("FIN", 2, 1),
        ("S", 0, 0), ("S", 3, 0), ("S", 0, 1), ("S", 3, 1),
    ),
    (
        ("SL", 3, 0), ("SL", 3, 1), ("MA", 0, 0), ("H", 4, 0), ("H", 3, 0), ("H", 3, 1),
        ("RF", 2, 0), ("D", 4, 0), ("H", 2, 0), ("D", 3, 0), ("RF", 2, 1), ("D", 3, 1),
        ("H", 2, 1), ("D", 2, 0), ("RF", 1, 0), ("S", 2, 0), ("H", 1, 0), ("D", 2, 1),
        ("S", 2, 1), ("RF", 1, 1), ("H", 1, 1), ("D", 1, 0), ("S", 1, 0), ("RF", 0, 0),
        ("H", 0, 0), ("D", 1, 1), ("S", 1, 1), ("RF", 0, 1), ("H", 0, 1), ("ST", 0, 0),
        ("D", 0, 0), ("MB", 0, 0), ("S", 0, 0), ("D", 0, 1), ("S", 0, 1), ("MO", 0, 0),
        ("FIN", 3, 0), ("FIN", 3, 1),
    ),
)


def chip_orders(chips):
    return ORDERS


def packed_orders(chips):
    orders = chip_orders(chips)
    steps = max(len(order) for order in orders)
    steps = -(-steps // 3) * 3
    words = []
    for order in orders:
        codes = [NUMBER[kind] * 16 + source * SPLIT + part for kind, source, part in order]
        codes = codes + [0] * (steps - len(codes))
        words.append(
            [codes[i] + 256 * codes[i + 1] + 65536 * codes[i + 2] for i in range(0, steps, 3)]
        )
    return steps, words


def dot(a, b):
    return jnp.dot(a, b, preferred_element_type=jnp.float32)


def dot_nt(a, b):
    return lax.dot_general(a, b, (((1,), (1,)), ((), ())), preferred_element_type=jnp.float32)


def dot_tn(a, b):
    return lax.dot_general(a, b, (((0,), (0,)), ((), ())), preferred_element_type=jnp.float32)


def fused_kernel(
    count,
    query_hbm,
    forget_hbm,
    value_hbm,
    output_gate_hbm,
    out_weight_hbm,
    x_hbm,
    gate_hbm,
    up_hbm,
    down_hbm,
    shared_gate_hbm,
    shared_up_hbm,
    shared_down_hbm,
    margin_ref,
    extra_ref,
    head_gain_ref,
    index_ref,
    score_ref,
    gain_ref,
    recurrent_ref,
    expert_ref,
    query_v,
    forget_v,
    value_v,
    output_gate_v,
    out_weight_v,
    x_v,
    gate_w,
    up_w,
    down_w,
    rows,
    gates,
    own_hidden,
    peer_hidden,
    result,
    side_result,
    inward,
    inward_left,
    inward_right,
    outward,
    local_out,
    carried_query,
    own_state,
    own_decay,
    side_state,
    side_decay,
    before,
    next_state,
    gated,
    mixed,
    mixed_peer,
    load_sem,
    row_sem,
    table_sem,
    right_sem,
    left_sem,
    side_sem,
    table_right,
    table_left,
    table_side,
    hidden_send,
    hidden_recv,
    result_send,
    result_recv,
    outward_send,
    inward_recv,
    left_recv,
    right_recv,
    state_send,
    state_recv,
    mixed_send,
    mixed_recv,
):
    f32, bf16 = jnp.float32, jnp.bfloat16
    chips = count // 2
    me = lax.axis_index("ep")
    half = lax.axis_index("tp")
    chip, core = me // 2, me % 2
    other = 1 - core
    side = chip * 2 + other
    partner = 1 - half
    has_right, has_left = chip < chips - 1, chip > 0
    length = query_v.shape[0]
    heads = extra_ref.shape[1]
    mine = heads // 2
    part_rows = rows.shape[1]
    units = gate_w.shape[2]
    routed = chips * SPLIT
    steps, words = packed_orders(chips)

    def half_rows(ref, which):
        return ref.at[pl.ds(pl.multiple_of(which * units, units), units), :]

    loads = [
        (x_hbm, x_v),
        (forget_hbm, forget_v),
        (query_hbm, query_v),
        (value_hbm, value_v),
        (shared_gate_hbm, gate_w.at[1]),
        (shared_up_hbm, up_w.at[1]),
        (gate_hbm.at[0], gate_w.at[0]),
        (up_hbm.at[0], up_w.at[0]),
        (half_rows(shared_down_hbm, half), down_w.at[1, 0]),
        (half_rows(shared_down_hbm, partner), down_w.at[1, 1]),
        (half_rows(down_hbm.at[0], half), down_w.at[0, 0]),
        (half_rows(down_hbm.at[0], partner), down_w.at[0, 1]),
        (output_gate_hbm, output_gate_v),
        (out_weight_hbm, out_weight_v),
    ]
    copies = [
        pltpu.make_async_copy(source, target, load_sem.at[i])
        for i, (source, target) in enumerate(loads)
    ]
    for copy in copies:
        copy.start()

    barrier = pltpu.get_barrier_semaphore()
    pl.semaphore_signal(barrier, inc=1, device_id={"ep": side}, device_id_type=MESH)
    pl.semaphore_signal(barrier, inc=1, device_id={"tp": partner}, device_id_type=MESH)

    @pl.when(has_right)
    def _():
        pl.semaphore_signal(barrier, inc=1, device_id={"ep": me + 2}, device_id_type=MESH)

    @pl.when(has_left)
    def _():
        pl.semaphore_signal(barrier, inc=1, device_id={"ep": me - 2}, device_id_type=MESH)

    def remote(source, target, send, recv, **device):
        return pltpu.make_async_remote_copy(
            src_ref=source,
            dst_ref=target,
            send_sem=send,
            recv_sem=recv,
            device_id=device,
            device_id_type=MESH,
        )

    def row_copy(arg, sems, target):
        block = arg * 2 + core
        return remote(rows.at[block], rows.at[block], sems.at[arg], row_sem.at[block], ep=target)

    def table_copy(source, sems, target):
        block = source * 2 + core
        return remote(
            gates.at[block], gates.at[block], sems.at[source], table_sem.at[block], ep=target
        )

    def arrived_row(block):
        remote(rows.at[block], rows.at[block], side_sem.at[0], row_sem.at[block], ep=side).wait_recv()

    def arrived_table(block):
        remote(
            gates.at[block], gates.at[block], table_side.at[0], table_sem.at[block], ep=side
        ).wait_recv()

    def hidden_copy(arg):
        return remote(
            own_hidden.at[arg],
            peer_hidden.at[arg],
            hidden_send.at[arg],
            hidden_recv.at[arg],
            tp=partner,
        )

    def result_copy(arg):
        return remote(
            result.at[arg, other],
            side_result.at[arg],
            result_send.at[arg],
            result_recv.at[arg],
            ep=side,
        )

    def outward_copy(arg, target, target_sem, to):
        return remote(outward.at[arg], target, outward_send.at[arg], target_sem, ep=to)

    own_heads = pl.ds(core * mine, mine)
    state_copies = dict(
        state=lambda: remote(
            own_state, side_state, state_send.at[0], state_recv.at[0], ep=side
        ),
        decay=lambda: remote(
            own_decay, side_decay, state_send.at[1], state_recv.at[1], ep=side
        ),
        before=lambda: remote(
            before.at[own_heads],
            before.at[own_heads],
            state_send.at[2],
            state_recv.at[2],
            ep=side,
        ),
        chain=lambda: remote(
            next_state, before.at[own_heads], state_send.at[3], state_recv.at[3], ep=me + 2
        ),
        mixed=lambda: remote(
            mixed.at[partner], mixed_peer, mixed_send.at[0], mixed_recv.at[0], tp=partner
        ),
    )

    copies[0].wait()
    x = x_v[...].astype(f32)
    normed = (
        x * lax.rsqrt(jnp.mean(x * x, axis=1, keepdims=True) + EPSILON) * gain_ref[...]
    ).astype(bf16)
    for part in range(SPLIT):
        rows[(chip * SPLIT + part) * 2 + core] = normed[part * part_rows : (part + 1) * part_rows]
    score = score_ref[...]
    weight = ROUTED_SCALE * score / jnp.sum(score, axis=1, keepdims=True)
    lane = lax.broadcasted_iota(jnp.int32, (length, LANES), 1)
    table = jnp.zeros((length, LANES), f32)
    for k in range(score.shape[1]):
        table = table + jnp.where(lane == index_ref[:, k : k + 1], weight[:, k : k + 1], 0.0)
    gates[chip * 2 + core] = table.T[:count]

    pl.semaphore_wait(barrier, 2 + has_right.astype(jnp.int32) + has_left.astype(jnp.int32))

    @pl.when(has_right)
    def _():
        table_copy(chip, table_right, me + 2).start()

    @pl.when(has_left)
    def _():
        table_copy(chip, table_left, me - 2).start()

    for part in range(SPLIT):
        row_copy(chip * SPLIT + part, side_sem, side).start()
    table_copy(chip, table_side, side).start()

    def send_right(arg):
        row_copy(arg, right_sem, me + 2).start()

    def send_left(arg):
        row_copy(arg, left_sem, me - 2).start()

    def forward(arg):
        source, part = arg // SPLIT, arg % SPLIT
        arrived_row(arg * 2 + core)
        to_right = jnp.logical_and(source < chip, has_right)
        to_left = jnp.logical_and(source > chip, has_left)

        @pl.when(part == 0)
        def _():
            arrived_table(source * 2 + core)

            @pl.when(to_right)
            def _():
                table_copy(source, table_right, me + 2).start()

            @pl.when(to_left)
            def _():
                table_copy(source, table_left, me - 2).start()

            table_copy(source, table_side, side).start()

        @pl.when(to_right)
        def _():
            send_right(arg)

        @pl.when(to_left)
        def _():
            send_left(arg)

        row_copy(arg, side_sem, side).start()

    def mix_local(arg):
        for i in (1, 2, 3):
            copies[i].wait()
        row = lax.broadcasted_iota(jnp.int32, (length, length), 0)
        column = lax.broadcasted_iota(jnp.int32, (length, length), 1)
        upper = row < BLK
        left = column < BLK
        causal = jnp.logical_and(row >= column, upper == left)
        crossed = jnp.logical_and(jnp.logical_not(upper), left)
        ones = causal.astype(f32).astype(bf16)
        head_lane = lax.broadcasted_iota(jnp.int32, (length, heads), 1)
        middle = BLK // 2 - 1

        def one_head(h, _):
            lanes = pl.ds(pl.multiple_of(h * HEAD_CHANNELS, HEAD_CHANNELS), HEAD_CHANNELS)
            query = jax.nn.silu(query_v[:, lanes].astype(f32))
            key = margin_ref[:, lanes] * jax.nn.sigmoid(-forget_v[:, lanes].astype(f32))
            extra = jnp.sum(
                jnp.where(head_lane == h, extra_ref[...], 0.0), axis=1, keepdims=True
            )
            decay = jnp.log1p(-key) + extra
            high = decay.astype(bf16)
            rest = decay - high.astype(f32)
            mid = rest.astype(bf16)
            low = (rest - mid.astype(f32)).astype(bf16)
            total = dot(ones, high) + dot(ones, mid) + dot(ones, low)
            center = jnp.where(upper, total[middle : middle + 1], total[BLK + middle : BLK + middle + 1])
            end = jnp.where(upper, total[BLK - 1 : BLK], total[2 * BLK - 1 : 2 * BLK])
            first = jnp.exp(total[BLK - 1 : BLK])
            second = jnp.exp(total[2 * BLK - 1 : 2 * BLK])
            query_end = query * jnp.exp(total)
            key_end = key * jnp.exp(end - total)
            near = dot_nt(
                (query * jnp.exp(total - center)).astype(bf16),
                (key * jnp.exp(center - total)).astype(bf16),
            )
            far = dot_nt(query_end.astype(bf16), key_end.astype(bf16))
            scores = jnp.where(causal, near, jnp.where(crossed, far, 0.0)).astype(bf16)
            value = value_v[:, lanes]
            local_out[:, lanes] = dot(scores, value)
            carried_query[:, lanes] = jnp.where(upper, query_end, query_end * first).astype(bf16)
            key_state = jnp.where(upper, key_end * second, key_end).astype(bf16)
            own_state[h] = dot_tn(value, key_state).astype(bf16)
            own_decay[pl.ds(h, 1), :] = first * second
            return 0

        lax.fori_loop(0, heads, one_head, 0)
        state_copies["state"]().start()
        state_copies["decay"]().start()

    def mix_state(arg):
        state_copies["state"]().wait_recv()
        state_copies["decay"]().wait_recv()

        @pl.when(has_left)
        def _():
            state_copies["chain"]().wait_recv()
            state_copies["before"]().start()

        @pl.when(jnp.logical_not(has_left))
        def _():
            before[...] = jnp.zeros(before.shape, bf16)

        @pl.when(has_right)
        def _():
            def one_head(i, _):
                h = core * mine + i
                own, beside = own_state[h].astype(f32), side_state[h].astype(f32)
                own_d, beside_d = own_decay[pl.ds(h, 1), :], side_decay[pl.ds(h, 1), :]
                state0 = jnp.where(core == 0, own, beside)
                state1 = jnp.where(core == 0, beside, own)
                decay1 = jnp.where(core == 0, beside_d, own_d)
                carried = before[h].astype(f32) * (own_d * beside_d)
                next_state[i] = (carried + decay1 * state0 + state1).astype(bf16)
                return 0

            lax.fori_loop(0, mine, one_head, 0)
            state_copies["chain"]().start()

    def mix_finish(arg):
        copies[12].wait()
        copies[13].wait()

        @pl.when(has_left)
        def _():
            state_copies["before"]().wait_recv()

        def one_head(h, _):
            lanes = pl.ds(pl.multiple_of(h * HEAD_CHANNELS, HEAD_CHANNELS), HEAD_CHANNELS)
            state = before[h].astype(f32)
            beside = side_state[h].astype(f32)
            later = side_decay[pl.ds(h, 1), :] * state + beside
            state = jnp.where(core == 0, state, later).astype(bf16)
            out = local_out[:, lanes] + dot_nt(carried_query[:, lanes], state)
            factor = lax.rsqrt(jnp.mean(out * out, axis=1, keepdims=True) + EPSILON)
            gate = jax.nn.silu(output_gate_v[:, lanes].astype(f32))
            gated[:, lanes] = (out * factor * head_gain_ref[:, lanes] * gate).astype(bf16)
            return 0

        lax.fori_loop(0, heads, one_head, 0)
        tile = 512
        kept = length // 2

        def one_tile(n, _):
            lanes = pl.ds(pl.multiple_of(n * tile, tile), tile)
            partial = dot(gated[...], out_weight_v[:, lanes]).astype(bf16)
            mixed[0, :, lanes] = partial[:kept]
            mixed[1, :, lanes] = partial[kept:]
            return 0

        lax.fori_loop(0, out_weight_v.shape[1] // tile, one_tile, 0)
        state_copies["mixed"]().start()

    def mix_out(arg):
        state_copies["mixed"]().wait_recv()
        recurrent_ref[...] = (mixed[half].astype(f32) + mixed_peer[...].astype(f32)).astype(bf16)

    def hidden_part(arg):
        shared = arg == routed
        source, part = arg // SPLIT, arg % SPLIT

        @pl.when(shared)
        def _():
            for i in range(4, 12):
                copies[i].wait()

        @pl.when(jnp.logical_not(shared))
        def _():
            arrived_row(arg * 2 + other)

            @pl.when(part == 0)
            def _():
                arrived_table(source * 2 + other)

        which = shared.astype(jnp.int32)
        low = jnp.where(shared, chip * SPLIT * 2 + core, arg * 2)
        high = jnp.where(shared, chip * SPLIT * 2 + core + 2, arg * 2 + 1)
        x = jnp.concatenate([rows[low], rows[high]], axis=0)
        lane = lax.broadcasted_iota(jnp.int32, (length, count), 1)
        block_low = jnp.where(shared, chip * 2 + core, source * 2)
        block_high = jnp.where(shared, chip * 2 + core, source * 2 + 1)

        def own_gate(place):
            column = jnp.sum(
                jnp.where(lane == me, gates[place].T, 0.0), axis=1, keepdims=True
            )
            return jnp.where(part == 0, column[:part_rows], column[part_rows:])

        routed_gate = jnp.concatenate([own_gate(block_low), own_gate(block_high)], axis=0)
        scale = jnp.where(shared, 1.0, routed_gate)
        gate_part = dot(x, gate_w[which])
        up_part = dot(x, up_w[which])
        own_hidden[arg] = (jax.nn.silu(gate_part) * up_part * scale).astype(bf16)
        hidden_copy(arg).start()

    def down_part(arg):
        shared = arg == routed
        which = shared.astype(jnp.int32)
        hidden_copy(arg).wait_recv()
        out = dot(own_hidden[arg], down_w[which, 0]) + dot(peer_hidden[arg], down_w[which, 1])
        out = out.astype(bf16)
        result[arg, 0] = out[:part_rows]
        result[arg, 1] = out[part_rows:]

        @pl.when(jnp.logical_not(shared))
        def _():
            result_copy(arg).start()

    def chip_sum(arg):
        result_copy(arg).wait_recv()
        return result[arg, core].astype(f32) + side_result[arg].astype(f32)

    def to_neighbour(arg):
        source = arg // SPLIT
        return source > chip, jnp.abs(source - chip) == 1

    def outward_to(arg, place):
        part = arg % SPLIT
        target, sem, to = (
            (inward_left.at[part], left_recv.at[part], me + 2),
            (inward.at[arg], inward_recv.at[arg], me + 2),
            (inward_right.at[part], right_recv.at[part], me - 2),
            (inward.at[arg], inward_recv.at[arg], me - 2),
        )[place]
        return outward_copy(arg, target, sem, to)

    def send_sum(arg):
        right, adjacent = to_neighbour(arg)
        inner = jnp.logical_and(has_left, has_right)
        total = chip_sum(arg)

        @pl.when(inner)
        def _():
            outward_to(arg, 1).wait_recv()
            outward[arg] = (total + inward[arg].astype(f32)).astype(bf16)

        @pl.when(jnp.logical_not(inner))
        def _():
            outward[arg] = total.astype(bf16)

        far = jnp.logical_not(adjacent)
        for place, (direction, distance) in enumerate(
            (
                (right, adjacent),
                (right, far),
                (jnp.logical_not(right), adjacent),
                (jnp.logical_not(right), far),
            )
        ):

            @pl.when(jnp.logical_and(direction, distance))
            def _():
                outward_to(arg, place).start()

    def finish(arg):
        part = arg % SPLIT
        total = chip_sum(arg) + result[routed, part].astype(f32)
        place = pl.ds(pl.multiple_of(part * part_rows, part_rows), part_rows)

        @pl.when(has_left)
        def _():
            outward_to(arg, 0).wait_recv()

        @pl.when(has_right)
        def _():
            outward_to(arg, 2).wait_recv()

        from_left = jnp.where(has_left, inward_left[part].astype(f32), 0.0)
        from_right = jnp.where(has_right, inward_right[part].astype(f32), 0.0)
        expert_ref[place, :] = (total + from_left + from_right).astype(bf16)

    actions = dict(
        SR=send_right,
        SL=send_left,
        RF=forward,
        MA=mix_local,
        ST=mix_state,
        H=hidden_part,
        D=down_part,
        S=send_sum,
        FIN=finish,
        MB=mix_finish,
        MO=mix_out,
    )
    mine_words = []
    for n in range(steps // 3):
        word = jnp.int32(words[0][n])
        for c in range(1, chips):
            word = jnp.where(chip == c, words[c][n], word)
        mine_words.append(word)

    def turn(i, _):
        place, digit = i // 3, i % 3
        word = mine_words[0]
        for n in range(1, steps // 3):
            word = jnp.where(place == n, mine_words[n], word)
        code = jnp.where(
            digit == 0, word % 256, jnp.where(digit == 1, word // 256 % 256, word // 65536)
        )
        kind, arg = code // 16, code % 16
        for name, action in actions.items():

            @pl.when(kind == NUMBER[name])
            def _():
                action(arg)

        return 0

    lax.fori_loop(0, steps, turn, 0)

    def drain(arg, _):
        source, part = arg // SPLIT, arg % SPLIT
        hidden_copy(arg).wait_send()
        result_copy(arg).wait_send()
        row_copy(arg, side_sem, side).wait_send()
        to_right = jnp.logical_and(source <= chip, has_right)
        to_left = jnp.logical_and(source >= chip, has_left)

        @pl.when(to_right)
        def _():
            row_copy(arg, right_sem, me + 2).wait_send()

        @pl.when(to_left)
        def _():
            row_copy(arg, left_sem, me - 2).wait_send()

        @pl.when(source != chip)
        def _():
            outward_copy(arg, inward.at[arg], inward_recv.at[arg], side).wait_send()

        @pl.when(part == 0)
        def _():
            table_copy(source, table_side, side).wait_send()

            @pl.when(to_right)
            def _():
                table_copy(source, table_right, me + 2).wait_send()

            @pl.when(to_left)
            def _():
                table_copy(source, table_left, me - 2).wait_send()

        return 0

    lax.fori_loop(0, routed, drain, 0)
    hidden_copy(routed).wait_send()
    state_copies["state"]().wait_send()
    state_copies["decay"]().wait_send()

    @pl.when(has_left)
    def _():
        state_copies["before"]().wait_send()

    @pl.when(has_right)
    def _():
        state_copies["chain"]().wait_send()

    state_copies["mixed"]().wait_send()


def fused_fits(position_decay_extra, chosen_expert_index, routed_gate_weight):
    count, tensor = lax.axis_size("ep"), lax.axis_size("tp")
    length, heads = position_decay_extra.shape
    tokens, top = chosen_expert_index.shape
    every_row_fits = 2 * top >= count and routed_gate_weight.shape[0] == 1
    sizes = length == tokens == 2 * BLK and heads % 2 == 0
    return every_row_fits and sizes and tensor == 2 and count % 2 == 0 and count == 2 * len(ORDERS)


def fused_layer(
    recurrence_query_input,
    forget_gate_input,
    recurrence_value_input,
    output_gate_input,
    forget_lower_margin,
    position_decay_extra,
    head_norm_gain,
    recurrence_out_weight,
    expert_hidden_state,
    chosen_expert_index,
    chosen_expert_score,
    expert_norm_gain,
    routed_gate_weight,
    routed_up_weight,
    routed_down_weight,
    shared_gate_weight,
    shared_up_weight,
    shared_down_weight,
):
    f32, bf16 = jnp.float32, jnp.bfloat16
    count = lax.axis_size("ep")
    chips = count // 2
    routed = chips * SPLIT
    length, channels = recurrence_query_input.shape
    heads = position_decay_extra.shape[1]
    width, width_out = expert_hidden_state.shape[1], recurrence_out_weight.shape[1]
    units, features = routed_gate_weight.shape[2], routed_down_weight.shape[2]
    part_rows = length // SPLIT
    hbm = pl.BlockSpec(memory_space=pl.ANY)
    vmem = pl.BlockSpec(memory_space=pltpu.VMEM)
    dma = pltpu.SemaphoreType.DMA
    mixer_rows = pltpu.VMEM((length, channels), bf16)
    hidden = pltpu.VMEM((routed + 1, 2 * part_rows, units), bf16)
    partial = pltpu.VMEM((routed, part_rows, features), bf16)
    edge = pltpu.VMEM((SPLIT, part_rows, features), bf16)
    state = pltpu.VMEM((heads, HEAD_CHANNELS, HEAD_CHANNELS), bf16)
    decay = pltpu.VMEM((heads, HEAD_CHANNELS), f32)
    return pl.pallas_call(
        functools.partial(fused_kernel, count),
        out_shape=(
            jax.ShapeDtypeStruct((length // 2, width_out), bf16),
            jax.ShapeDtypeStruct((length, features), bf16),
        ),
        in_specs=[hbm] * 12 + [vmem] * 6,
        out_specs=(vmem, vmem),
        scratch_shapes=[
            mixer_rows,
            mixer_rows,
            mixer_rows,
            mixer_rows,
            pltpu.VMEM(recurrence_out_weight.shape, bf16),
            pltpu.VMEM((length, width), bf16),
            pltpu.VMEM((2, width, units), bf16),
            pltpu.VMEM((2, width, units), bf16),
            pltpu.VMEM((2, 2, units, features), bf16),
            pltpu.VMEM((routed * 2, part_rows, width), bf16),
            pltpu.VMEM((count, count, length), f32),
            hidden,
            hidden,
            pltpu.VMEM((routed + 1, 2, part_rows, features), bf16),
            partial,
            partial,
            edge,
            edge,
            partial,
            pltpu.VMEM((length, channels), f32),
            mixer_rows,
            state,
            decay,
            state,
            decay,
            state,
            pltpu.VMEM((heads // 2, HEAD_CHANNELS, HEAD_CHANNELS), bf16),
            mixer_rows,
            pltpu.VMEM((2, length // 2, width_out), bf16),
            pltpu.VMEM((length // 2, width_out), bf16),
            dma((14,)),
            dma((routed * 2,)),
            dma((count,)),
            dma((routed,)),
            dma((routed,)),
            dma((routed,)),
            dma((chips,)),
            dma((chips,)),
            dma((chips,)),
            dma((routed + 1,)),
            dma((routed + 1,)),
            dma((routed,)),
            dma((routed,)),
            dma((routed,)),
            dma((routed,)),
            dma((SPLIT,)),
            dma((SPLIT,)),
            dma((4,)),
            dma((4,)),
            dma((1,)),
            dma((1,)),
        ],
        compiler_params=pltpu.CompilerParams(
            collective_id=0, has_side_effects=True, vmem_limit_bytes=56 * 1024 * 1024
        ),
        cost_estimate=pl.CostEstimate(
            flops=9_000_000_000, bytes_accessed=18_000_000, transcendentals=0
        ),
        name="fused_kernel",
    )(
        recurrence_query_input,
        forget_gate_input,
        recurrence_value_input,
        output_gate_input,
        recurrence_out_weight,
        expert_hidden_state,
        routed_gate_weight,
        routed_up_weight,
        routed_down_weight,
        shared_gate_weight,
        shared_up_weight,
        shared_down_weight,
        forget_lower_margin[None, :],
        position_decay_extra,
        head_norm_gain[None, :],
        chosen_expert_index,
        chosen_expert_score,
        expert_norm_gain[None, :],
    )


def per_device(
    recurrence_query_input,
    forget_gate_input,
    recurrence_value_input,
    output_gate_input,
    forget_lower_margin,
    position_decay_extra,
    head_norm_gain,
    recurrence_out_weight,
    expert_hidden_state,
    chosen_expert_index,
    chosen_expert_score,
    expert_norm_gain,
    routed_gate_weight,
    routed_up_weight,
    routed_down_weight,
    shared_gate_weight,
    shared_up_weight,
    shared_down_weight,
):
    if fused_fits(position_decay_extra, chosen_expert_index, routed_gate_weight):
        return fused_layer(
            recurrence_query_input,
            forget_gate_input,
            recurrence_value_input,
            output_gate_input,
            forget_lower_margin,
            position_decay_extra,
            head_norm_gain,
            recurrence_out_weight,
            expert_hidden_state,
            chosen_expert_index,
            chosen_expert_score,
            expert_norm_gain,
            routed_gate_weight,
            routed_up_weight,
            routed_down_weight,
            shared_gate_weight,
            shared_up_weight,
            shared_down_weight,
        )
    recurrence_output = mixer_half(
        recurrence_query_input,
        forget_gate_input,
        recurrence_value_input,
        output_gate_input,
        forget_lower_margin,
        position_decay_extra,
        head_norm_gain,
        recurrence_out_weight,
    )
    expert_out = expert_half(
        expert_hidden_state,
        chosen_expert_index,
        chosen_expert_score,
        expert_norm_gain,
        routed_gate_weight,
        routed_up_weight,
        routed_down_weight,
        shared_gate_weight,
        shared_up_weight,
        shared_down_weight,
    )
    return (recurrence_output, expert_out)


def solution(mesh):
    in_specs = (
        P(("grp", "ep"), "tp"),
        P(("grp", "ep"), "tp"),
        P(("grp", "ep"), "tp"),
        P(("grp", "ep"), "tp"),
        P("tp"),
        P(("grp", "ep"), "tp"),
        P("tp"),
        P("tp", None),
        P(("grp", "ep"), None),
        P(("grp", "ep"), None),
        P(("grp", "ep"), None),
        P(),
        P("ep", None, "tp"),
        P("ep", None, "tp"),
        P("ep", None, "tp"),
        P(None, "tp"),
        P(None, "tp"),
        P(None, "tp"),
    )
    out_specs = (P(("grp", "ep", "tp"), None), P(("grp", "ep"), "tp"))
    return jax.shard_map(
        per_device, mesh=mesh, in_specs=in_specs, out_specs=out_specs, check_vma=False
    )
```

```python
import functools

import jax
import jax.numpy as jnp
from jax import lax
from jax.experimental import pallas as pl
from jax.experimental.pallas import tpu as pltpu
from jax.sharding import PartitionSpec as P

HEAD_CHANNELS = 128
BLK = 64


EPSILON = 1e-06
ROUTED_SCALE = 2.5
PRECISION = lax.Precision.DEFAULT


DECAY_ROWS = 16


def carried_in(decay, state, axis):
    count, index = (lax.axis_size(axis), lax.axis_index(axis))
    depth = state.shape[1]
    rows = jnp.broadcast_to(decay[:, None, :], (decay.shape[0], DECAY_ROWS, decay.shape[1]))
    sent = jnp.concatenate([state, rows], axis=1).astype(jnp.bfloat16)
    everything = lax.all_gather(sent, axis)
    before = jnp.zeros_like(state)
    for k in range(count - 1):
        part = everything[k].astype(jnp.float32)
        new = part[:, depth : depth + 1] * before + part[:, :depth]
        before = jnp.where(k < index, new, before)
    return before


def mixer_half(
    recurrence_query_input,
    forget_gate_input,
    recurrence_value_input,
    output_gate_input,
    forget_lower_margin,
    position_decay_extra,
    head_norm_gain,
    recurrence_out_weight,
):
    length = recurrence_query_input.shape[0]
    head_tensor = position_decay_extra.shape[1]
    blocks = length // BLK
    queries = jax.nn.silu(recurrence_query_input.astype(jnp.float32))
    key_gate_value = forget_lower_margin[None, :] * jax.nn.sigmoid(
        -forget_gate_input.astype(jnp.float32)
    )
    decay_logarithm = jnp.log1p(-key_gate_value) + jnp.repeat(
        position_decay_extra, HEAD_CHANNELS, axis=1
    )
    value_rows = recurrence_value_input.astype(jnp.float32)

    def split_heads(tensor):
        return tensor.reshape(blocks, BLK, head_tensor, HEAD_CHANNELS).transpose(2, 0, 1, 3)

    query_heads = split_heads(queries)
    key_heads = split_heads(key_gate_value)
    value_heads = split_heads(value_rows)
    cum_decay = jnp.cumsum(split_heads(decay_logarithm), axis=2)
    middle = cum_decay[:, :, BLK // 2 - 1 : BLK // 2]
    block_end = cum_decay[:, :, BLK - 1 : BLK]
    scores = jnp.einsum(
        "hncd,hnsd->hncs",
        query_heads * jnp.exp(cum_decay - middle),
        key_heads * jnp.exp(middle - cum_decay),
        precision=PRECISION,
    )
    causal = jnp.tril(jnp.ones((BLK, BLK), dtype=bool))
    scores = jnp.where(causal, scores, 0.0)
    within = jnp.einsum("hncs,hnse->hnce", scores, value_heads, precision=PRECISION)
    updates = jnp.einsum(
        "hncd,hnce->nhed",
        key_heads * jnp.exp(block_end - cum_decay),
        value_heads,
        precision=PRECISION,
    )
    block_log = block_end[:, :, 0, :]
    block_decay = jnp.exp(block_log).transpose(1, 0, 2)

    state = jnp.zeros_like(updates[0])
    starts_list = []
    for block in range(blocks):
        starts_list.append(state)
        state = block_decay[block][:, None, :] * state + updates[block]
    local_final, local_starts = state, jnp.stack(starts_list)
    device_decay = jnp.exp(jnp.sum(block_log, axis=1))
    incoming = carried_in(device_decay, local_final, "ep")
    before = jnp.exp(jnp.cumsum(block_log, axis=1) - block_log).transpose(1, 0, 2)
    starts = local_starts + before[:, :, None, :] * incoming[None]
    carried = jnp.einsum(
        "hncd,nhed->hnce", query_heads * jnp.exp(cum_decay), starts, precision=PRECISION
    )
    outputs = (within + carried).transpose(1, 2, 0, 3).reshape(length, head_tensor, HEAD_CHANNELS)
    factor = lax.rsqrt(jnp.mean(outputs * outputs, axis=2, keepdims=True) + EPSILON)
    normed = (outputs * factor).reshape(length, head_tensor * HEAD_CHANNELS) * head_norm_gain[
        None, :
    ]
    gated_rows = (normed * jax.nn.silu(output_gate_input.astype(jnp.float32))).astype(jnp.bfloat16)
    partial = jnp.dot(
        gated_rows, recurrence_out_weight, preferred_element_type=jnp.float32
    ).astype(jnp.bfloat16)
    if lax.axis_size("tp") != 2:
        return lax.psum_scatter(partial, "tp", scatter_dimension=0, tiled=True)
    which, kept_rows = lax.axis_index("tp"), length // 2
    kept = lax.dynamic_slice_in_dim(partial, which * kept_rows, kept_rows)
    sent = lax.dynamic_slice_in_dim(partial, (1 - which) * kept_rows, kept_rows)
    received = lax.ppermute(sent, "tp", [(0, 1), (1, 0)])
    return (kept.astype(jnp.float32) + received.astype(jnp.float32)).astype(jnp.bfloat16)


def expert_half(
    expert_hidden_state,
    chosen_expert_index,
    chosen_expert_score,
    expert_norm_gain,
    routed_gate_weight,
    routed_up_weight,
    routed_down_weight,
    shared_gate_weight,
    shared_up_weight,
    shared_down_weight,
):
    tokens, top = chosen_expert_index.shape
    local_experts = routed_gate_weight.shape[0]
    devices = lax.axis_size("ep")
    experts = local_experts * devices
    capacity = min(tokens, 2 * tokens * top // experts)
    width_out = routed_down_weight.shape[2]
    features = expert_hidden_state.astype(jnp.float32)
    normed = (
        features
        * lax.rsqrt(jnp.mean(features * features, axis=1, keepdims=True) + EPSILON)
        * expert_norm_gain[None, :]
    ).astype(jnp.bfloat16)
    gates = ROUTED_SCALE * chosen_expert_score / jnp.sum(chosen_expert_score, axis=1, keepdims=True)
    flat_ids = chosen_expert_index.reshape(-1)
    onehot = (flat_ids[:, None] == jnp.arange(experts, dtype=jnp.int32)[None, :]).astype(jnp.int32)
    places = jnp.sum(onehot * (jnp.cumsum(onehot, axis=0) - 1), axis=1)
    slots = flat_ids * capacity + places
    owners = (
        jnp.full((experts * capacity,), tokens, jnp.int32)
        .at[slots]
        .set(jnp.arange(tokens * top, dtype=jnp.int32) // top)
    )
    padded = jnp.concatenate([normed, jnp.zeros((1, normed.shape[1]), jnp.bfloat16)], axis=0)
    outgoing = padded[owners].reshape(experts, capacity, normed.shape[1])
    piece = lax.all_to_all(outgoing, "ep", split_axis=0, concat_axis=0, tiled=True)
    grouped = piece.reshape(devices, local_experts, piece.shape[1], piece.shape[2])
    gate_part = jnp.einsum(
        "secd,edh->sech", grouped, routed_gate_weight, preferred_element_type=jnp.float32
    )
    up_part = jnp.einsum(
        "secd,edh->sech", grouped, routed_up_weight, preferred_element_type=jnp.float32
    )
    hidden = (jax.nn.silu(gate_part) * up_part).astype(jnp.bfloat16)
    hidden_rows = hidden.reshape(devices * local_experts, piece.shape[1], hidden.shape[3])
    flat_hidden = hidden_rows.reshape(experts * capacity, hidden_rows.shape[2])
    shared_hidden = (
        jax.nn.silu(jnp.dot(normed, shared_gate_weight, preferred_element_type=jnp.float32))
        * jnp.dot(normed, shared_up_weight, preferred_element_type=jnp.float32)
    ).astype(jnp.bfloat16)
    start_values = (
        jnp.zeros((experts * capacity, width_out), jnp.float32),
        jnp.zeros((tokens, width_out), jnp.float32),
    )
    routed_piece = lax.all_gather(flat_hidden, "tp", axis=1, tiled=True)
    shared_piece = lax.all_gather(shared_hidden, "tp", axis=1, tiled=True)
    count = routed_piece.shape[1]
    grouped = routed_piece.reshape(devices, local_experts, capacity, count)
    routed = jnp.einsum(
        "secn,enk->seck", grouped, routed_down_weight, preferred_element_type=jnp.float32
    )
    shared = jnp.dot(shared_piece, shared_down_weight, preferred_element_type=jnp.float32)
    routed_sum = routed.reshape(start_values[0].shape)
    answers = routed_sum.astype(jnp.bfloat16).reshape(experts, capacity, width_out)
    returned = lax.all_to_all(answers, "ep", split_axis=0, concat_axis=0, tiled=True)
    picked_rows = returned.reshape(experts * capacity, width_out)[slots].reshape(
        tokens, top, width_out
    )
    combined = shared + jnp.sum(gates[:, :, None] * picked_rows.astype(jnp.float32), axis=1)
    return combined.astype(jnp.bfloat16)


MESH = pl.DeviceIdType.MESH
LANES = 128
SPLIT = 4
COARSE = 2
GROUP = SPLIT // COARSE
CROSSED = True
KINDS = (
    "NO",
    "SR",
    "SL",
    "RF",
    "RX",
    "MA",
    "ST",
    "H",
    "D",
    "S",
    "SX",
    "FIN",
    "FL",
    "FR",
    "FB",
    "MB",
    "MP",
    "MO",
)
NUMBER = {name: place for place, name in enumerate(KINDS)}


ORDERS = (
    (
        ("SR", 0, 1, 0), ("SR", 0, 0, 0), ("SR", 0, 2, 0), ("H", 4, 0, 0), ("MA", 0, 0, 0),
        ("MA", 0, 1, 0), ("MA", 0, 2, 0), ("MA", 0, 3, 0), ("H", 0, 0, 0), ("H", 0, 2, 0),
        ("ST", 0, 0, 0), ("SR", 0, 3, 0), ("D", 4, 0, 0), ("MB", 0, 0, 0), ("MB", 0, 1, 0),
        ("MB", 0, 2, 0), ("RX", 1, 0, 1), ("D", 0, 0, 0), ("RF", 2, 0, 0), ("D", 0, 2, 0),
        ("RX", 1, 1, 1), ("RF", 1, 2, 1), ("H", 1, 0, 1), ("RF", 2, 1, 0), ("H", 2, 0, 0),
        ("RF", 1, 3, 1), ("RF", 3, 0, 0), ("H", 1, 2, 1), ("D", 1, 2, 1), ("RF", 3, 1, 0),
        ("S", 1, 2, 1), ("S", 1, 3, 1), ("H", 3, 0, 0), ("D", 2, 0, 0), ("RF", 3, 2, 0),
        ("S", 2, 0, 0), ("S", 2, 1, 0), ("RF", 3, 3, 0), ("H", 3, 2, 0), ("D", 3, 0, 0),
        ("RF", 2, 2, 0), ("S", 3, 0, 0), ("SX", 3, 1, 0), ("RF", 2, 3, 0), ("MB", 0, 3, 0),
        ("MP", 0, 0, 0), ("MP", 0, 1, 0), ("H", 2, 2, 0), ("D", 3, 2, 0), ("MP", 0, 2, 0),
        ("MP", 0, 3, 0), ("S", 3, 2, 0), ("S", 3, 3, 0), ("D", 1, 0, 1), ("S", 1, 0, 1),
        ("S", 1, 1, 1), ("D", 2, 2, 0), ("S", 2, 2, 0), ("S", 2, 3, 0), ("MO", 0, 0, 0),
        ("FR", 0, 2, 0), ("FIN", 0, 0, 0), ("FR", 0, 3, 0), ("FIN", 0, 1, 0),
    ),
    (
        ("SR", 1, 0, 0), ("SR", 1, 1, 0), ("SR", 1, 2, 0), ("H", 4, 0, 0), ("MA", 0, 0, 0),
        ("H", 1, 0, 0), ("H", 1, 2, 0), ("SL", 1, 0, 1), ("MA", 0, 1, 0), ("MA", 0, 2, 0),
        ("MA", 0, 3, 0), ("RF", 2, 0, 0), ("D", 4, 0, 0), ("SL", 1, 1, 1), ("RF", 0, 0, 0),
        ("RF", 0, 1, 0), ("RF", 2, 1, 0), ("D", 1, 0, 0), ("H", 0, 0, 0), ("H", 2, 0, 0),
        ("RF", 3, 0, 0), ("D", 1, 2, 0), ("RF", 0, 2, 0), ("RF", 3, 1, 0), ("D", 0, 0, 0),
        ("RF", 0, 3, 0), ("SR", 1, 3, 0), ("ST", 0, 0, 0), ("H", 3, 0, 0), ("H", 0, 2, 0),
        ("D", 2, 0, 0), ("MB", 0, 0, 0), ("RF", 3, 2, 0), ("MB", 0, 1, 0), ("MB", 0, 2, 0),
        ("RF", 3, 3, 0), ("MB", 0, 3, 0), ("MP", 0, 0, 0), ("MP", 0, 1, 0), ("H", 3, 2, 0),
        ("D", 3, 0, 0), ("RF", 2, 2, 0), ("MP", 0, 2, 0), ("MP", 0, 3, 0), ("D", 0, 2, 0),
        ("RF", 2, 3, 0), ("SX", 0, 2, 0), ("SX", 0, 3, 0), ("H", 2, 2, 0), ("D", 3, 2, 0),
        ("S", 2, 0, 0), ("S", 2, 1, 0), ("MO", 0, 0, 0), ("S", 3, 0, 0), ("D", 2, 2, 0),
        ("SX", 3, 1, 0), ("S", 3, 2, 0), ("S", 0, 0, 0), ("S", 3, 3, 0), ("S", 0, 1, 0),
        ("S", 2, 2, 0), ("S", 2, 3, 0), ("FIN", 1, 2, 1), ("FIN", 1, 0, 1), ("FIN", 1, 1, 1),
        ("FIN", 1, 3, 1),
    ),
    (
        ("H", 4, 0, 0), ("SL", 2, 0, 0), ("SL", 2, 1, 0), ("SR", 2, 1, 1), ("MA", 0, 0, 0),
        ("H", 2, 0, 0), ("H", 2, 2, 0), ("MA", 0, 1, 0), ("MA", 0, 2, 0), ("RF", 1, 0, 0),
        ("SR", 2, 0, 1), ("RF", 3, 0, 0), ("MA", 0, 3, 0), ("D", 4, 0, 0), ("RF", 1, 1, 0),
        ("D", 2, 0, 0), ("H", 1, 0, 0), ("RF", 3, 1, 0), ("D", 2, 2, 0), ("H", 3, 0, 0),
        ("RF", 0, 0, 0), ("RF", 3, 2, 0), ("RF", 3, 3, 0), ("SL", 2, 2, 0), ("SL", 2, 3, 0),
        ("H", 3, 2, 0), ("D", 1, 0, 0), ("RF", 0, 1, 0), ("RF", 1, 2, 0), ("D", 3, 0, 0),
        ("H", 0, 0, 0), ("RF", 0, 2, 0), ("D", 3, 2, 0), ("RF", 0, 3, 0), ("H", 0, 2, 0),
        ("RF", 1, 3, 0), ("D", 0, 0, 0), ("H", 1, 2, 0), ("ST", 0, 0, 0), ("MB", 0, 0, 0),
        ("MB", 0, 1, 0), ("MB", 0, 2, 0), ("MB", 0, 3, 0), ("D", 0, 2, 0), ("MP", 0, 0, 0),
        ("MP", 0, 1, 0), ("MP", 0, 2, 0), ("MP", 0, 3, 0), ("SX", 0, 2, 0), ("SX", 0, 3, 0),
        ("D", 1, 2, 0), ("S", 1, 0, 0), ("S", 1, 1, 0), ("S", 0, 0, 0), ("MO", 0, 0, 0),
        ("S", 0, 1, 0), ("S", 3, 0, 0), ("SX", 3, 1, 0), ("S", 3, 2, 0), ("S", 3, 3, 0),
        ("S", 1, 2, 0), ("S", 1, 3, 0), ("FIN", 2, 2, 1), ("FIN", 2, 3, 1), ("FIN", 2, 0, 1),
        ("FIN", 2, 1, 1),
    ),
    (
        ("SL", 3, 0, 0), ("SL", 3, 3, 0), ("SL", 3, 1, 0), ("SL", 3, 2, 0), ("H", 4, 0, 0),
        ("MA", 0, 0, 0), ("MA", 0, 1, 0), ("H", 3, 0, 0), ("H", 3, 2, 0), ("MA", 0, 2, 0),
        ("MA", 0, 3, 0), ("D", 4, 0, 0), ("D", 3, 0, 0), ("RF", 1, 0, 0), ("D", 3, 2, 0),
        ("RX", 2, 0, 1), ("RX", 2, 1, 1), ("RF", 1, 1, 0), ("H", 2, 0, 1), ("H", 1, 0, 0),
        ("RF", 2, 2, 1), ("RF", 0, 0, 0), ("RF", 2, 3, 1), ("RF", 0, 1, 0), ("H", 2, 2, 1),
        ("H", 0, 0, 0), ("D", 2, 2, 1), ("RF", 1, 2, 0), ("S", 2, 2, 1), ("S", 2, 3, 1),
        ("D", 1, 0, 0), ("RF", 0, 2, 0), ("S", 1, 0, 0), ("S", 1, 1, 0), ("D", 2, 0, 1),
        ("RF", 0, 3, 0), ("S", 2, 0, 1), ("S", 2, 1, 1), ("H", 0, 2, 0), ("D", 0, 0, 0),
        ("RF", 1, 3, 0), ("S", 0, 0, 0), ("S", 0, 1, 0), ("H", 1, 2, 0), ("ST", 0, 0, 0),
        ("MB", 0, 0, 0), ("D", 0, 2, 0), ("MB", 0, 1, 0), ("MB", 0, 2, 0), ("MB", 0, 3, 0),
        ("MP", 0, 0, 0), ("SX", 0, 2, 0), ("SX", 0, 3, 0), ("MP", 0, 1, 0), ("MP", 0, 2, 0),
        ("MP", 0, 3, 0), ("D", 1, 2, 0), ("S", 1, 2, 0), ("S", 1, 3, 0), ("FIN", 3, 0, 0),
        ("FL", 3, 1, 0), ("MO", 0, 0, 0), ("FIN", 3, 2, 0), ("FIN", 3, 3, 0),
    ),
)


def chip_orders(chips):
    return ORDERS


def packed_orders(chips):
    orders = chip_orders(chips)
    steps = max(len(order) for order in orders)
    steps = -(-steps // 2) * 2
    words = []
    for order in orders:
        codes = [
            (NUMBER[kind] * 64 + source * SPLIT + part) * 2 + turned
            for kind, source, part, turned in order
        ]
        codes = codes + [0] * (steps - len(codes))
        words.append(
            [codes[i] + 32768 * codes[i + 1] for i in range(0, steps, 2)]
        )
    return steps, words


def dot(a, b):
    return jnp.dot(a, b, preferred_element_type=jnp.float32)


def dot_nt(a, b):
    return lax.dot_general(a, b, (((1,), (1,)), ((), ())), preferred_element_type=jnp.float32)


def dot_tn(a, b):
    return lax.dot_general(a, b, (((0,), (0,)), ((), ())), preferred_element_type=jnp.float32)


def fused_kernel(
    count,
    query_hbm,
    forget_hbm,
    value_hbm,
    output_gate_hbm,
    out_weight_hbm,
    x_hbm,
    gate_hbm,
    up_hbm,
    down_hbm,
    shared_gate_hbm,
    shared_up_hbm,
    shared_down_hbm,
    margin_hbm,
    extra_hbm,
    head_gain_hbm,
    index_hbm,
    score_hbm,
    gain_hbm,
    recurrent_ref,
    expert_ref,
    margin_ref,
    extra_ref,
    head_gain_ref,
    index_ref,
    score_ref,
    gain_ref,
    query_v,
    forget_v,
    value_v,
    output_gate_v,
    out_weight_v,
    x_v,
    gate_w,
    up_w,
    down_w,
    rows,
    gates,
    own_hidden,
    peer_hidden,
    result,
    side_result,
    inward,
    final,
    outward,
    local_out,
    carried_query,
    own_state,
    own_decay,
    side_state,
    side_decay,
    before,
    next_state,
    gated,
    mixed,
    mixed_peer,
    load_sem,
    row_sem,
    table_sem,
    right_sem,
    left_sem,
    side_sem,
    cross_sem,
    table_right,
    table_left,
    table_side,
    hidden_send,
    hidden_recv,
    result_send,
    result_recv,
    outward_send,
    inward_recv,
    final_recv,
    state_send,
    state_recv,
    mixed_send,
    mixed_recv,
):
    f32, bf16 = jnp.float32, jnp.bfloat16
    chips = count // 2
    me = lax.axis_index("ep")
    half = lax.axis_index("tp")
    chip, core = me // 2, me % 2
    other = 1 - core
    side = chip * 2 + other
    partner = 1 - half
    has_right, has_left = chip < chips - 1, chip > 0
    length = query_v.shape[0]
    heads = extra_ref.shape[0]
    mine = heads // 2
    part_rows = rows.shape[1]
    units = gate_w.shape[2]
    routed = chips * SPLIT
    last = chips * COARSE
    coarse_rows = GROUP * part_rows
    tiles = 4
    tile = out_weight_v.shape[1] // tiles
    steps, words = packed_orders(chips)

    def half_rows(ref, which):
        return ref.at[pl.ds(pl.multiple_of(which * units, units), units), :]

    loads = dict(
        x=(x_hbm, x_v),
        gain=(gain_hbm, gain_ref),
        index=(index_hbm, index_ref),
        score=(score_hbm, score_ref),
        shared_gate=(shared_gate_hbm, gate_w.at[1]),
        shared_up=(shared_up_hbm, up_w.at[1]),
        forget=(forget_hbm, forget_v),
        query=(query_hbm, query_v),
        value=(value_hbm, value_v),
        margin=(margin_hbm, margin_ref),
        extra=(extra_hbm, extra_ref),
        gate=(gate_hbm.at[0], gate_w.at[0]),
        up=(up_hbm.at[0], up_w.at[0]),
        shared_down0=(half_rows(shared_down_hbm, half), down_w.at[1, 0]),
        shared_down1=(half_rows(shared_down_hbm, partner), down_w.at[1, 1]),
        down0=(half_rows(down_hbm.at[0], half), down_w.at[0, 0]),
        down1=(half_rows(down_hbm.at[0], partner), down_w.at[0, 1]),
        output_gate=(output_gate_hbm, output_gate_v),
        head_gain=(head_gain_hbm, head_gain_ref),
        out_weight=(out_weight_hbm, out_weight_v),
    )
    copies = {
        name: pltpu.make_async_copy(source, target, load_sem.at[i])
        for i, (name, (source, target)) in enumerate(loads.items())
    }
    for copy in copies.values():
        copy.start()

    def loaded(*names):
        for name in names:
            copies[name].wait()

    barrier = pltpu.get_barrier_semaphore()
    pl.semaphore_signal(barrier, inc=1, device_id={"ep": side}, device_id_type=MESH)
    pl.semaphore_signal(barrier, inc=1, device_id={"tp": partner}, device_id_type=MESH)
    for distance in range(1, chips):
        there = (chip + distance) % chips * 2 + core
        pl.semaphore_signal(barrier, inc=1, device_id={"ep": there}, device_id_type=MESH)

    def remote(source, target, send, recv, **device):
        return pltpu.make_async_remote_copy(
            src_ref=source,
            dst_ref=target,
            send_sem=send,
            recv_sem=recv,
            device_id=device,
            device_id_type=MESH,
        )

    def row_copy(arg, sems, target):
        block = arg * 2 + core
        return remote(rows.at[block], rows.at[block], sems.at[arg], row_sem.at[block], ep=target)

    def cross_copy(arg):
        block = arg * 2 + core
        return remote(
            rows.at[block], rows.at[block], cross_sem.at[arg], row_sem.at[block], tp=partner
        )

    def table_copy(source, sems, target):
        block = source * 2 + core
        return remote(
            gates.at[block], gates.at[block], sems.at[source], table_sem.at[block], ep=target
        )

    def arrived_row(block):
        remote(rows.at[block], rows.at[block], side_sem.at[0], row_sem.at[block], ep=side).wait_recv()

    def arrived_table(block):
        remote(
            gates.at[block], gates.at[block], table_side.at[0], table_sem.at[block], ep=side
        ).wait_recv()

    def hidden_copy(arg):
        return remote(
            own_hidden.at[arg],
            peer_hidden.at[arg],
            hidden_send.at[arg],
            hidden_recv.at[arg],
            tp=partner,
        )

    def result_copy(arg):
        return remote(
            result.at[arg, other],
            side_result.at[arg],
            result_send.at[arg],
            result_recv.at[arg],
            ep=side,
        )

    def outward_copy(arg, target, target_sem, to):
        return remote(outward.at[arg], target, outward_send.at[arg], target_sem, ep=to)

    own_heads = pl.ds(core * mine, mine)
    state_copies = dict(
        state=lambda: remote(
            own_state, side_state, state_send.at[0], state_recv.at[0], ep=side
        ),
        decay=lambda: remote(
            own_decay, side_decay, state_send.at[1], state_recv.at[1], ep=side
        ),
        before=lambda: remote(
            before.at[own_heads],
            before.at[own_heads],
            state_send.at[2],
            state_recv.at[2],
            ep=side,
        ),
        chain=lambda: remote(
            next_state, before.at[own_heads], state_send.at[3], state_recv.at[3], ep=me + 2
        ),
    )

    def mixed_copy(n):
        lanes = pl.ds(pl.multiple_of(n * tile, tile), tile)
        return remote(
            mixed.at[partner, :, lanes],
            mixed_peer.at[:, lanes],
            mixed_send.at[n],
            mixed_recv.at[n],
            tp=partner,
        )

    loaded("x", "gain", "index", "score")
    x = x_v[...].astype(f32)
    normed = (
        x * lax.rsqrt(jnp.mean(x * x, axis=1, keepdims=True) + EPSILON) * gain_ref[...]
    ).astype(bf16)
    for part in range(SPLIT):
        rows[(chip * SPLIT + part) * 2 + core] = normed[part * part_rows : (part + 1) * part_rows]
    score = score_ref[...]
    weight = ROUTED_SCALE * score / jnp.sum(score, axis=0, keepdims=True)
    expert = lax.broadcasted_iota(jnp.int32, (count, length), 0)
    table = jnp.zeros((count, length), f32)
    for k in range(score.shape[0]):
        table = table + jnp.where(expert == index_ref[k : k + 1, :], weight[k : k + 1, :], 0.0)
    gates[chip * 2 + core] = table

    pl.semaphore_wait(barrier, chips + 1)

    @pl.when(has_right)
    def _():
        table_copy(chip, table_right, me + 2).start()

    @pl.when(has_left)
    def _():
        table_copy(chip, table_left, me - 2).start()

    for part in range(SPLIT):
        row_copy(chip * SPLIT + part, side_sem, side).start()
    table_copy(chip, table_side, side).start()

    def send_right(arg, first):
        row_copy(arg, right_sem, me + 2).start()

    def send_left(arg, first):
        row_copy(arg, left_sem, me - 2).start()

    def forward(arg, first):
        source = arg // SPLIT
        arrived_row(arg * 2 + core)
        to_right = jnp.logical_and(source < chip, has_right)
        to_left = jnp.logical_and(source > chip, has_left)

        @pl.when(first)
        def _():
            arrived_table(source * 2 + core)

            @pl.when(to_right)
            def _():
                table_copy(source, table_right, me + 2).start()

            @pl.when(to_left)
            def _():
                table_copy(source, table_left, me - 2).start()

            table_copy(source, table_side, side).start()

        @pl.when(to_right)
        def _():
            send_right(arg, first)

        @pl.when(to_left)
        def _():
            send_left(arg, first)

        row_copy(arg, side_sem, side).start()

    def cross(arg, first):
        forward(arg, first)
        cross_copy(arg).start()

    def mix_local(arg, first):
        @pl.when(arg == 0)
        def _():
            loaded("forget", "query", "value", "margin", "extra")

        row = lax.broadcasted_iota(jnp.int32, (length, length), 0)
        column = lax.broadcasted_iota(jnp.int32, (length, length), 1)
        upper = row < BLK
        left = column < BLK
        causal = jnp.logical_and(row >= column, upper == left)
        crossed = jnp.logical_and(jnp.logical_not(upper), left)
        ones = causal.astype(f32).astype(bf16)
        head_lane = lax.broadcasted_iota(jnp.int32, (length, heads), 1)
        extra_columns = extra_ref[...].T
        middle = BLK // 2 - 1

        def one_head(h):
            lanes = pl.ds(pl.multiple_of(h * HEAD_CHANNELS, HEAD_CHANNELS), HEAD_CHANNELS)
            query = jax.nn.silu(query_v[:, lanes].astype(f32))
            key = margin_ref[:, lanes] * jax.nn.sigmoid(-forget_v[:, lanes].astype(f32))
            extra = jnp.sum(
                jnp.where(head_lane == h, extra_columns, 0.0), axis=1, keepdims=True
            )
            decay = jnp.log1p(-key) + extra
            high = decay.astype(bf16)
            rest = decay - high.astype(f32)
            mid = rest.astype(bf16)
            low = (rest - mid.astype(f32)).astype(bf16)
            total = dot(ones, high) + dot(ones, mid) + dot(ones, low)
            center = jnp.where(upper, total[middle : middle + 1], total[BLK + middle : BLK + middle + 1])
            end = jnp.where(upper, total[BLK - 1 : BLK], total[2 * BLK - 1 : 2 * BLK])
            first = jnp.exp(total[BLK - 1 : BLK])
            second = jnp.exp(total[2 * BLK - 1 : 2 * BLK])
            query_end = query * jnp.exp(total)
            key_end = key * jnp.exp(end - total)
            near = dot_nt(
                (query * jnp.exp(total - center)).astype(bf16),
                (key * jnp.exp(center - total)).astype(bf16),
            )
            far = dot_nt(query_end.astype(bf16), key_end.astype(bf16))
            scores = jnp.where(causal, near, jnp.where(crossed, far, 0.0)).astype(bf16)
            value = value_v[:, lanes]
            local_out[:, lanes] = dot(scores, value)
            carried_query[:, lanes] = jnp.where(upper, query_end, query_end * first).astype(bf16)
            key_state = jnp.where(upper, key_end * second, key_end).astype(bf16)
            own_state[h] = dot_tn(value, key_state).astype(bf16)
            own_decay[pl.ds(h, 1), :] = first * second

        one_head(2 * arg)
        one_head(2 * arg + 1)

        @pl.when(arg == heads // 2 - 1)
        def _():
            state_copies["state"]().start()
            state_copies["decay"]().start()

    def mix_state(arg, first):
        state_copies["state"]().wait_recv()
        state_copies["decay"]().wait_recv()

        @pl.when(has_left)
        def _():
            state_copies["chain"]().wait_recv()
            state_copies["before"]().start()

        @pl.when(jnp.logical_not(has_left))
        def _():
            before[...] = jnp.zeros(before.shape, bf16)

        @pl.when(has_right)
        def _():
            def one_head(i, _):
                h = core * mine + i
                own, beside = own_state[h].astype(f32), side_state[h].astype(f32)
                own_d, beside_d = own_decay[pl.ds(h, 1), :], side_decay[pl.ds(h, 1), :]
                state0 = jnp.where(core == 0, own, beside)
                state1 = jnp.where(core == 0, beside, own)
                decay1 = jnp.where(core == 0, beside_d, own_d)
                carried = before[h].astype(f32) * (own_d * beside_d)
                next_state[i] = (carried + decay1 * state0 + state1).astype(bf16)
                return 0

            lax.fori_loop(0, mine, one_head, 0)
            state_copies["chain"]().start()

    def mix_finish(arg, first):
        @pl.when(arg == 0)
        def _():
            loaded("output_gate", "head_gain")

        @pl.when(jnp.logical_and(arg == 0, has_left))
        def _():
            state_copies["before"]().wait_recv()

        def one_head(h):
            lanes = pl.ds(pl.multiple_of(h * HEAD_CHANNELS, HEAD_CHANNELS), HEAD_CHANNELS)
            state = before[h].astype(f32)
            beside = side_state[h].astype(f32)
            later = side_decay[pl.ds(h, 1), :] * state + beside
            state = jnp.where(core == 0, state, later).astype(bf16)
            out = local_out[:, lanes] + dot_nt(carried_query[:, lanes], state)
            factor = lax.rsqrt(jnp.mean(out * out, axis=1, keepdims=True) + EPSILON)
            gate = jax.nn.silu(output_gate_v[:, lanes].astype(f32))
            gated[:, lanes] = (out * factor * head_gain_ref[:, lanes] * gate).astype(bf16)

        one_head(2 * arg)
        one_head(2 * arg + 1)

    def mix_project(arg, first):
        @pl.when(arg == 0)
        def _():
            loaded("out_weight")

        kept = length // 2
        lanes = pl.ds(pl.multiple_of(arg * tile, tile), tile)
        partial = dot(gated[...], out_weight_v[:, lanes]).astype(bf16)
        mixed[0, :, lanes] = partial[:kept]
        mixed[1, :, lanes] = partial[kept:]

        mixed_copy(arg).start()

    def mix_out(arg, first):
        for n in range(tiles):
            mixed_copy(n).wait_recv()

        recurrent_ref[...] = (mixed[half].astype(f32) + mixed_peer[...].astype(f32)).astype(bf16)

    def hidden_part(arg, first):
        shared = arg == routed
        chunk = arg // GROUP
        source, place = chunk // COARSE, chunk % COARSE

        @pl.when(shared)
        def _():
            loaded("shared_gate", "shared_up")

        @pl.when(jnp.logical_and(source == chip, first))
        def _():
            loaded("gate", "up")

        @pl.when(jnp.logical_not(shared))
        def _():
            for p in range(GROUP):
                arrived_row((arg + p) * 2 + other)

            @pl.when(first)
            def _():
                arrived_table(source * 2 + other)

        which = shared.astype(jnp.int32)
        pieces = []
        for parity in range(2):
            for p in range(GROUP):
                own = (chip * SPLIT + parity * GROUP + p) * 2 + core
                pieces.append(rows[jnp.where(shared, own, (arg + p) * 2 + parity)])
        x = jnp.concatenate(pieces, axis=0)
        lane = lax.broadcasted_iota(jnp.int32, (length, count), 1)
        block_low = jnp.where(shared, chip * 2 + core, source * 2)
        block_high = jnp.where(shared, chip * 2 + core, source * 2 + 1)

        def own_gate(block):
            column = jnp.sum(jnp.where(lane == me, gates[block].T, 0.0), axis=1, keepdims=True)
            return jnp.where(place == 0, column[:coarse_rows], column[coarse_rows:])

        routed_gate = jnp.concatenate([own_gate(block_low), own_gate(block_high)], axis=0)
        scale = jnp.where(shared, 1.0, routed_gate)
        gate_part = dot(x, gate_w[which])
        up_part = dot(x, up_w[which])
        own_hidden[chunk] = (jax.nn.silu(gate_part) * up_part * scale).astype(bf16)
        hidden_copy(chunk).start()

    def down_part(arg, first):
        shared = arg == routed
        chunk = arg // GROUP
        which = shared.astype(jnp.int32)

        @pl.when(shared)
        def _():
            loaded("shared_down0", "shared_down1")

        @pl.when(jnp.logical_and(chunk // COARSE == chip, first))
        def _():
            loaded("down0", "down1")

        hidden_copy(chunk).wait_recv()
        out = dot(own_hidden[chunk], down_w[which, 0]) + dot(peer_hidden[chunk], down_w[which, 1])
        out = out.astype(bf16)
        result[chunk, 0] = out[:coarse_rows]
        result[chunk, 1] = out[coarse_rows:]

        @pl.when(jnp.logical_not(shared))
        def _():
            result_copy(chunk).start()

    def part_slice(arg):
        return pl.ds(pl.multiple_of(arg % GROUP * part_rows, part_rows), part_rows)

    def chip_sum(arg, awaited):
        chunk = arg // GROUP

        @pl.when(awaited)
        def _():
            result_copy(chunk).wait_recv()

        inside = part_slice(arg)
        return result[chunk, core, inside].astype(f32) + side_result[chunk, inside].astype(f32)

    def final_copy(arg):
        slot = chip * SPLIT + arg % SPLIT
        there = arg // SPLIT * 2 + core
        return outward_copy(arg, final.at[slot], final_recv.at[slot], there)

    def send_sum(arg, first, direct):
        target = arg // SPLIT
        adjacent = jnp.abs(target - chip) == 1
        total = chip_sum(arg, arg % GROUP == 0)
        if direct:
            outward[arg] = total.astype(bf16)
            final_copy(arg).start()
            return
        inner = jnp.logical_and(has_left, has_right)
        towards = jnp.where(target > chip, me + 2, me - 2)
        relay = outward_copy(arg, inward.at[arg], inward_recv.at[arg], towards)

        @pl.when(inner)
        def _():
            relay.wait_recv()
            outward[arg] = (total + inward[arg].astype(f32)).astype(bf16)

        @pl.when(jnp.logical_not(inner))
        def _():
            outward[arg] = total.astype(bf16)

        @pl.when(adjacent)
        def _():
            final_copy(arg).start()

        @pl.when(jnp.logical_not(adjacent))
        def _():
            relay.start()

    def finish(arg, first, left_all, right_all):
        part = arg % SPLIT
        place = pl.ds(pl.multiple_of(part * part_rows, part_rows), part_rows)
        shared = result[last, part // GROUP, part_slice(arg)].astype(f32)
        total = chip_sum(arg, arg % GROUP == 0) + shared
        for s in range(chips):
            taken = jnp.abs(chip - s) == 1
            if left_all:
                taken = jnp.logical_or(taken, chip > s)
            if right_all:
                taken = jnp.logical_or(taken, chip < s)
            slot = s * SPLIT + part

            @pl.when(taken)
            def _():
                outward_copy(arg, final.at[slot], final_recv.at[slot], side).wait_recv()

            total = total + jnp.where(taken, final[slot].astype(f32), 0.0)
        expert_ref[place, :] = total.astype(bf16)

    actions = dict(
        SR=send_right,
        SL=send_left,
        RF=forward,
        RX=cross,
        MA=mix_local,
        ST=mix_state,
        H=hidden_part,
        D=down_part,
        S=functools.partial(send_sum, direct=False),
        SX=functools.partial(send_sum, direct=True),
        FIN=functools.partial(finish, left_all=False, right_all=False),
        FL=functools.partial(finish, left_all=True, right_all=False),
        FR=functools.partial(finish, left_all=False, right_all=True),
        FB=functools.partial(finish, left_all=True, right_all=True),
        MB=mix_finish,
        MP=mix_project,
        MO=mix_out,
    )
    mine_words = []
    for n in range(steps // 2):
        word = jnp.int32(words[0][n])
        for c in range(1, chips):
            word = jnp.where(chip == c, words[c][n], word)
        mine_words.append(word)

    def turn(i, _):
        place, digit = i // 2, i % 2
        word = mine_words[0]
        for n in range(1, steps // 2):
            word = jnp.where(place == n, mine_words[n], word)
        code = jnp.where(
            digit == 0, word % 32768, word // 32768
        )
        kind, arg, turned = code // 128, code // 2 % 64, code % 2
        first = arg % SPLIT == 0
        shift = (arg % SPLIT + half * (SPLIT // 2)) % SPLIT
        arg = jnp.where(turned == 1, arg // SPLIT * SPLIT + shift, arg)
        for name, action in actions.items():

            @pl.when(kind == NUMBER[name])
            def _():
                action(arg, first)

        return 0

    lax.fori_loop(0, steps, turn, 0)

    def drain(arg, _):
        source, part = arg // SPLIT, arg % SPLIT
        row_copy(arg, side_sem, side).wait_send()
        to_right = jnp.logical_and(source <= chip, has_right)
        to_left = jnp.logical_and(source >= chip, has_left)
        row_right, row_left = to_right, to_left
        if CROSSED:
            kept = (part + half * (SPLIT // 2)) % SPLIT < SPLIT // 2
            own = source == chip
            right_end = jnp.logical_and(own, chip == chips - 2)
            left_end = jnp.logical_and(own, chip == 1)
            row_right = jnp.logical_and(to_right, jnp.logical_or(kept, jnp.logical_not(right_end)))
            row_left = jnp.logical_and(to_left, jnp.logical_or(kept, jnp.logical_not(left_end)))
            ends = jnp.logical_or(
                jnp.logical_and(chip == chips - 1, source == chips - 2),
                jnp.logical_and(chip == 0, source == 1),
            )

            @pl.when(jnp.logical_and(ends, kept))
            def _():
                cross_copy(arg).wait_send()


        @pl.when(row_right)
        def _():
            row_copy(arg, right_sem, me + 2).wait_send()

        @pl.when(row_left)
        def _():
            row_copy(arg, left_sem, me - 2).wait_send()

        @pl.when(source != chip)
        def _():
            outward_copy(arg, inward.at[arg], inward_recv.at[arg], side).wait_send()

        @pl.when(part == 0)
        def _():
            table_copy(source, table_side, side).wait_send()

            @pl.when(to_right)
            def _():
                table_copy(source, table_right, me + 2).wait_send()

            @pl.when(to_left)
            def _():
                table_copy(source, table_left, me - 2).wait_send()

        return 0

    lax.fori_loop(0, routed, drain, 0)

    def drain_chunk(chunk, _):
        hidden_copy(chunk).wait_send()
        result_copy(chunk).wait_send()
        return 0

    lax.fori_loop(0, last, drain_chunk, 0)
    hidden_copy(last).wait_send()
    state_copies["state"]().wait_send()
    state_copies["decay"]().wait_send()

    @pl.when(has_left)
    def _():
        state_copies["before"]().wait_send()

    @pl.when(has_right)
    def _():
        state_copies["chain"]().wait_send()

    for n in range(tiles):
        mixed_copy(n).wait_send()


def fused_fits(position_decay_extra, chosen_expert_index, routed_gate_weight):
    count, tensor = lax.axis_size("ep"), lax.axis_size("tp")
    length, heads = position_decay_extra.shape
    tokens, top = chosen_expert_index.shape
    every_row_fits = 2 * top >= count and routed_gate_weight.shape[0] == 1
    sizes = length == tokens == 2 * BLK and heads % 2 == 0
    return every_row_fits and sizes and tensor == 2 and count % 2 == 0 and count == 2 * len(ORDERS)


def fused_layer(
    recurrence_query_input,
    forget_gate_input,
    recurrence_value_input,
    output_gate_input,
    forget_lower_margin,
    position_decay_extra,
    head_norm_gain,
    recurrence_out_weight,
    expert_hidden_state,
    chosen_expert_index,
    chosen_expert_score,
    expert_norm_gain,
    routed_gate_weight,
    routed_up_weight,
    routed_down_weight,
    shared_gate_weight,
    shared_up_weight,
    shared_down_weight,
):
    f32, bf16 = jnp.float32, jnp.bfloat16
    count = lax.axis_size("ep")
    chips = count // 2
    routed = chips * SPLIT
    length, channels = recurrence_query_input.shape
    heads = position_decay_extra.shape[1]
    width, width_out = expert_hidden_state.shape[1], recurrence_out_weight.shape[1]
    units, features = routed_gate_weight.shape[2], routed_down_weight.shape[2]
    part_rows = length // SPLIT
    hbm = pl.BlockSpec(memory_space=pltpu.HBM)
    vmem = pl.BlockSpec(memory_space=pltpu.VMEM)
    dma = pltpu.SemaphoreType.DMA
    mixer_rows = pltpu.VMEM((length, channels), bf16)
    coarse_rows = length // COARSE
    chunks = chips * COARSE + 1
    hidden = pltpu.VMEM((chunks, 2 * coarse_rows, units), bf16)
    partial = pltpu.VMEM((routed, part_rows, features), bf16)
    state = pltpu.VMEM((heads, HEAD_CHANNELS, HEAD_CHANNELS), bf16)
    decay = pltpu.VMEM((heads, HEAD_CHANNELS), f32)
    large = [
        pltpu.with_memory_space_constraint(array, pltpu.HBM)
        for array in (
            recurrence_query_input,
            forget_gate_input,
            recurrence_value_input,
            output_gate_input,
            recurrence_out_weight,
            expert_hidden_state,
            routed_gate_weight,
            routed_up_weight,
            routed_down_weight,
            shared_gate_weight,
            shared_up_weight,
            shared_down_weight,
            forget_lower_margin[None, :],
            position_decay_extra.T,
            head_norm_gain[None, :],
            chosen_expert_index.T,
            chosen_expert_score.T,
            expert_norm_gain[None, :],
        )
    ]
    return pl.pallas_call(
        functools.partial(fused_kernel, count),
        out_shape=(
            jax.ShapeDtypeStruct((length // 2, width_out), bf16),
            jax.ShapeDtypeStruct((length, features), bf16),
        ),
        in_specs=[hbm] * 18,
        out_specs=(vmem, vmem),
        scratch_shapes=[
            *(pltpu.VMEM(array.shape, array.dtype) for array in large[12:]),
            mixer_rows,
            mixer_rows,
            mixer_rows,
            mixer_rows,
            pltpu.VMEM(recurrence_out_weight.shape, bf16),
            pltpu.VMEM((length, width), bf16),
            pltpu.VMEM((2, width, units), bf16),
            pltpu.VMEM((2, width, units), bf16),
            pltpu.VMEM((2, 2, units, features), bf16),
            pltpu.VMEM((routed * 2, part_rows, width), bf16),
            pltpu.VMEM((count, count, length), f32),
            hidden,
            hidden,
            pltpu.VMEM((chunks, 2, coarse_rows, features), bf16),
            pltpu.VMEM((chunks, coarse_rows, features), bf16),
            partial,
            partial,
            partial,
            pltpu.VMEM((length, channels), f32),
            mixer_rows,
            state,
            decay,
            state,
            decay,
            state,
            pltpu.VMEM((heads // 2, HEAD_CHANNELS, HEAD_CHANNELS), bf16),
            mixer_rows,
            pltpu.VMEM((2, length // 2, width_out), bf16),
            pltpu.VMEM((length // 2, width_out), bf16),
            dma((20,)),
            dma((routed * 2,)),
            dma((count,)),
            dma((routed,)),
            dma((routed,)),
            dma((routed,)),
            dma((routed,)),
            dma((chips,)),
            dma((chips,)),
            dma((chips,)),
            dma((chunks,)),
            dma((chunks,)),
            dma((chunks,)),
            dma((chunks,)),
            dma((routed,)),
            dma((routed,)),
            dma((routed,)),
            dma((4,)),
            dma((4,)),
            dma((4,)),
            dma((4,)),
        ],
        compiler_params=pltpu.CompilerParams(
            collective_id=0, has_side_effects=True, vmem_limit_bytes=46 * 1024 * 1024
        ),
        cost_estimate=pl.CostEstimate(
            flops=9_000_000_000, bytes_accessed=18_000_000, transcendentals=0
        ),
        name="fused_kernel",
    )(
        *large,
    )


def per_device(
    recurrence_query_input,
    forget_gate_input,
    recurrence_value_input,
    output_gate_input,
    forget_lower_margin,
    position_decay_extra,
    head_norm_gain,
    recurrence_out_weight,
    expert_hidden_state,
    chosen_expert_index,
    chosen_expert_score,
    expert_norm_gain,
    routed_gate_weight,
    routed_up_weight,
    routed_down_weight,
    shared_gate_weight,
    shared_up_weight,
    shared_down_weight,
):
    if fused_fits(position_decay_extra, chosen_expert_index, routed_gate_weight):
        return fused_layer(
            recurrence_query_input,
            forget_gate_input,
            recurrence_value_input,
            output_gate_input,
            forget_lower_margin,
            position_decay_extra,
            head_norm_gain,
            recurrence_out_weight,
            expert_hidden_state,
            chosen_expert_index,
            chosen_expert_score,
            expert_norm_gain,
            routed_gate_weight,
            routed_up_weight,
            routed_down_weight,
            shared_gate_weight,
            shared_up_weight,
            shared_down_weight,
        )
    recurrence_output = mixer_half(
        recurrence_query_input,
        forget_gate_input,
        recurrence_value_input,
        output_gate_input,
        forget_lower_margin,
        position_decay_extra,
        head_norm_gain,
        recurrence_out_weight,
    )
    expert_out = expert_half(
        expert_hidden_state,
        chosen_expert_index,
        chosen_expert_score,
        expert_norm_gain,
        routed_gate_weight,
        routed_up_weight,
        routed_down_weight,
        shared_gate_weight,
        shared_up_weight,
        shared_down_weight,
    )
    return (recurrence_output, expert_out)


def solution(mesh):
    in_specs = (
        P(("grp", "ep"), "tp"),
        P(("grp", "ep"), "tp"),
        P(("grp", "ep"), "tp"),
        P(("grp", "ep"), "tp"),
        P("tp"),
        P(("grp", "ep"), "tp"),
        P("tp"),
        P("tp", None),
        P(("grp", "ep"), None),
        P(("grp", "ep"), None),
        P(("grp", "ep"), None),
        P(),
        P("ep", None, "tp"),
        P("ep", None, "tp"),
        P("ep", None, "tp"),
        P(None, "tp"),
        P(None, "tp"),
        P(None, "tp"),
    )
    out_specs = (P(("grp", "ep", "tp"), None), P(("grp", "ep"), "tp"))
    return jax.shard_map(
        per_device, mesh=mesh, in_specs=in_specs, out_specs=out_specs, check_vma=False
    )
```

```python
import functools

import jax
import jax.numpy as jnp
from jax import lax
from jax.experimental import pallas as pl
from jax.experimental.pallas import tpu as pltpu
from jax.sharding import PartitionSpec as P

HEAD_CHANNELS = 128
BLK = 64


EPSILON = 1e-06
ROUTED_SCALE = 2.5
PRECISION = lax.Precision.DEFAULT


DECAY_ROWS = 16


def carried_in(decay, state, axis):
    count, index = (lax.axis_size(axis), lax.axis_index(axis))
    depth = state.shape[1]
    rows = jnp.broadcast_to(decay[:, None, :], (decay.shape[0], DECAY_ROWS, decay.shape[1]))
    sent = jnp.concatenate([state, rows], axis=1).astype(jnp.bfloat16)
    everything = lax.all_gather(sent, axis)
    before = jnp.zeros_like(state)
    for k in range(count - 1):
        part = everything[k].astype(jnp.float32)
        new = part[:, depth : depth + 1] * before + part[:, :depth]
        before = jnp.where(k < index, new, before)
    return before


def mixer_half(
    recurrence_query_input,
    forget_gate_input,
    recurrence_value_input,
    output_gate_input,
    forget_lower_margin,
    position_decay_extra,
    head_norm_gain,
    recurrence_out_weight,
):
    length = recurrence_query_input.shape[0]
    head_tensor = position_decay_extra.shape[1]
    blocks = length // BLK
    queries = jax.nn.silu(recurrence_query_input.astype(jnp.float32))
    key_gate_value = forget_lower_margin[None, :] * jax.nn.sigmoid(
        -forget_gate_input.astype(jnp.float32)
    )
    decay_logarithm = jnp.log1p(-key_gate_value) + jnp.repeat(
        position_decay_extra, HEAD_CHANNELS, axis=1
    )
    value_rows = recurrence_value_input.astype(jnp.float32)

    def split_heads(tensor):
        return tensor.reshape(blocks, BLK, head_tensor, HEAD_CHANNELS).transpose(2, 0, 1, 3)

    query_heads = split_heads(queries)
    key_heads = split_heads(key_gate_value)
    value_heads = split_heads(value_rows)
    cum_decay = jnp.cumsum(split_heads(decay_logarithm), axis=2)
    middle = cum_decay[:, :, BLK // 2 - 1 : BLK // 2]
    block_end = cum_decay[:, :, BLK - 1 : BLK]
    scores = jnp.einsum(
        "hncd,hnsd->hncs",
        query_heads * jnp.exp(cum_decay - middle),
        key_heads * jnp.exp(middle - cum_decay),
        precision=PRECISION,
    )
    causal = jnp.tril(jnp.ones((BLK, BLK), dtype=bool))
    scores = jnp.where(causal, scores, 0.0)
    within = jnp.einsum("hncs,hnse->hnce", scores, value_heads, precision=PRECISION)
    updates = jnp.einsum(
        "hncd,hnce->nhed",
        key_heads * jnp.exp(block_end - cum_decay),
        value_heads,
        precision=PRECISION,
    )
    block_log = block_end[:, :, 0, :]
    block_decay = jnp.exp(block_log).transpose(1, 0, 2)

    state = jnp.zeros_like(updates[0])
    starts_list = []
    for block in range(blocks):
        starts_list.append(state)
        state = block_decay[block][:, None, :] * state + updates[block]
    local_final, local_starts = state, jnp.stack(starts_list)
    device_decay = jnp.exp(jnp.sum(block_log, axis=1))
    incoming = carried_in(device_decay, local_final, "ep")
    before = jnp.exp(jnp.cumsum(block_log, axis=1) - block_log).transpose(1, 0, 2)
    starts = local_starts + before[:, :, None, :] * incoming[None]
    carried = jnp.einsum(
        "hncd,nhed->hnce", query_heads * jnp.exp(cum_decay), starts, precision=PRECISION
    )
    outputs = (within + carried).transpose(1, 2, 0, 3).reshape(length, head_tensor, HEAD_CHANNELS)
    factor = lax.rsqrt(jnp.mean(outputs * outputs, axis=2, keepdims=True) + EPSILON)
    normed = (outputs * factor).reshape(length, head_tensor * HEAD_CHANNELS) * head_norm_gain[
        None, :
    ]
    gated_rows = (normed * jax.nn.silu(output_gate_input.astype(jnp.float32))).astype(jnp.bfloat16)
    partial = jnp.dot(
        gated_rows, recurrence_out_weight, preferred_element_type=jnp.float32
    ).astype(jnp.bfloat16)
    if lax.axis_size("tp") != 2:
        return lax.psum_scatter(partial, "tp", scatter_dimension=0, tiled=True)
    which, kept_rows = lax.axis_index("tp"), length // 2
    kept = lax.dynamic_slice_in_dim(partial, which * kept_rows, kept_rows)
    sent = lax.dynamic_slice_in_dim(partial, (1 - which) * kept_rows, kept_rows)
    received = lax.ppermute(sent, "tp", [(0, 1), (1, 0)])
    return (kept.astype(jnp.float32) + received.astype(jnp.float32)).astype(jnp.bfloat16)


def expert_half(
    expert_hidden_state,
    chosen_expert_index,
    chosen_expert_score,
    expert_norm_gain,
    routed_gate_weight,
    routed_up_weight,
    routed_down_weight,
    shared_gate_weight,
    shared_up_weight,
    shared_down_weight,
):
    tokens, top = chosen_expert_index.shape
    local_experts = routed_gate_weight.shape[0]
    devices = lax.axis_size("ep")
    experts = local_experts * devices
    capacity = min(tokens, 2 * tokens * top // experts)
    width_out = routed_down_weight.shape[2]
    features = expert_hidden_state.astype(jnp.float32)
    normed = (
        features
        * lax.rsqrt(jnp.mean(features * features, axis=1, keepdims=True) + EPSILON)
        * expert_norm_gain[None, :]
    ).astype(jnp.bfloat16)
    gates = ROUTED_SCALE * chosen_expert_score / jnp.sum(chosen_expert_score, axis=1, keepdims=True)
    flat_ids = chosen_expert_index.reshape(-1)
    onehot = (flat_ids[:, None] == jnp.arange(experts, dtype=jnp.int32)[None, :]).astype(jnp.int32)
    places = jnp.sum(onehot * (jnp.cumsum(onehot, axis=0) - 1), axis=1)
    slots = flat_ids * capacity + places
    owners = (
        jnp.full((experts * capacity,), tokens, jnp.int32)
        .at[slots]
        .set(jnp.arange(tokens * top, dtype=jnp.int32) // top)
    )
    padded = jnp.concatenate([normed, jnp.zeros((1, normed.shape[1]), jnp.bfloat16)], axis=0)
    outgoing = padded[owners].reshape(experts, capacity, normed.shape[1])
    piece = lax.all_to_all(outgoing, "ep", split_axis=0, concat_axis=0, tiled=True)
    grouped = piece.reshape(devices, local_experts, piece.shape[1], piece.shape[2])
    gate_part = jnp.einsum(
        "secd,edh->sech", grouped, routed_gate_weight, preferred_element_type=jnp.float32
    )
    up_part = jnp.einsum(
        "secd,edh->sech", grouped, routed_up_weight, preferred_element_type=jnp.float32
    )
    hidden = (jax.nn.silu(gate_part) * up_part).astype(jnp.bfloat16)
    hidden_rows = hidden.reshape(devices * local_experts, piece.shape[1], hidden.shape[3])
    flat_hidden = hidden_rows.reshape(experts * capacity, hidden_rows.shape[2])
    shared_hidden = (
        jax.nn.silu(jnp.dot(normed, shared_gate_weight, preferred_element_type=jnp.float32))
        * jnp.dot(normed, shared_up_weight, preferred_element_type=jnp.float32)
    ).astype(jnp.bfloat16)
    start_values = (
        jnp.zeros((experts * capacity, width_out), jnp.float32),
        jnp.zeros((tokens, width_out), jnp.float32),
    )
    routed_piece = lax.all_gather(flat_hidden, "tp", axis=1, tiled=True)
    shared_piece = lax.all_gather(shared_hidden, "tp", axis=1, tiled=True)
    count = routed_piece.shape[1]
    grouped = routed_piece.reshape(devices, local_experts, capacity, count)
    routed = jnp.einsum(
        "secn,enk->seck", grouped, routed_down_weight, preferred_element_type=jnp.float32
    )
    shared = jnp.dot(shared_piece, shared_down_weight, preferred_element_type=jnp.float32)
    routed_sum = routed.reshape(start_values[0].shape)
    answers = routed_sum.astype(jnp.bfloat16).reshape(experts, capacity, width_out)
    returned = lax.all_to_all(answers, "ep", split_axis=0, concat_axis=0, tiled=True)
    picked_rows = returned.reshape(experts * capacity, width_out)[slots].reshape(
        tokens, top, width_out
    )
    combined = shared + jnp.sum(gates[:, :, None] * picked_rows.astype(jnp.float32), axis=1)
    return combined.astype(jnp.bfloat16)


MESH = pl.DeviceIdType.MESH
LANES = 128
SPLIT = 4
COARSE = 2
GROUP = SPLIT // COARSE
CROSSED = 1
KINDS = (
    "NO",
    "SR",
    "SL",
    "RF",
    "RX",
    "RN",
    "MA",
    "ST",
    "H",
    "D",
    "S",
    "SX",
    "FIN",
    "FL",
    "FR",
    "FB",
    "MB",
    "MP",
    "MO",
    "DR",
)
NUMBER = {name: place for place, name in enumerate(KINDS)}


ORDERS = (
    (
        ("SR", 0, 0, 0), ("SR", 0, 1, 0), ("SR", 0, 3, 0), ("SR", 0, 2, 0), ("H", 4, 0, 0),
        ("MA", 0, 0, 0), ("H", 0, 0, 0), ("H", 0, 2, 0), ("MA", 0, 1, 0), ("MA", 0, 2, 0),
        ("MA", 0, 3, 0), ("RX", 1, 0, 1), ("D", 4, 0, 0), ("ST", 0, 0, 0), ("RX", 1, 1, 1),
        ("D", 0, 0, 0), ("H", 1, 0, 1), ("D", 0, 2, 0), ("RF", 2, 0, 1), ("RF", 1, 2, 1),
        ("RF", 2, 1, 1), ("H", 2, 0, 1), ("RF", 1, 3, 1), ("RF", 3, 0, 0), ("H", 1, 2, 1),
        ("D", 1, 2, 1), ("RF", 3, 1, 0), ("S", 1, 2, 1), ("S", 1, 3, 1), ("H", 3, 0, 0),
        ("RF", 3, 2, 0), ("D", 1, 0, 1), ("RF", 3, 3, 0), ("S", 1, 0, 1), ("S", 1, 1, 1),
        ("H", 3, 2, 0), ("RF", 2, 2, 1), ("D", 3, 0, 0), ("S", 3, 0, 0), ("S", 3, 1, 0),
        ("RF", 2, 3, 1), ("H", 2, 2, 1), ("D", 3, 2, 0), ("D", 2, 2, 1), ("S", 3, 2, 0),
        ("S", 3, 3, 0), ("MB", 0, 0, 0), ("S", 2, 2, 1), ("S", 2, 3, 1), ("MB", 0, 1, 0),
        ("MB", 0, 2, 0), ("MB", 0, 3, 0), ("MP", 0, 0, 0), ("MP", 0, 1, 0), ("D", 2, 0, 1),
        ("MP", 0, 2, 0), ("MP", 0, 3, 0), ("S", 2, 0, 1), ("S", 2, 1, 1), ("FIN", 0, 0, 0),
        ("FIN", 0, 1, 0), ("MO", 0, 0, 0), ("FIN", 0, 2, 0), ("DR", 0, 0, 0), ("FIN", 0, 3, 0),
    ),
    (
        ("SR", 1, 0, 1), ("SR", 1, 1, 1), ("SL", 1, 0, 1), ("SL", 1, 1, 1), ("H", 4, 0, 0),
        ("MA", 0, 0, 0), ("MA", 0, 1, 0), ("MA", 0, 2, 0), ("H", 1, 0, 0), ("H", 1, 2, 0),
        ("RF", 0, 0, 0), ("RF", 2, 0, 1), ("RF", 0, 1, 0), ("H", 0, 0, 0), ("RF", 2, 1, 1),
        ("D", 1, 0, 0), ("H", 2, 0, 1), ("RF", 3, 0, 0), ("RF", 0, 2, 0), ("D", 1, 2, 0),
        ("RF", 0, 3, 0), ("SR", 1, 2, 1), ("SR", 1, 3, 1), ("RF", 3, 1, 0), ("H", 0, 2, 0),
        ("D", 0, 0, 0), ("H", 3, 0, 0), ("RF", 3, 2, 0), ("MA", 0, 3, 0), ("RF", 3, 3, 0),
        ("ST", 0, 0, 0), ("D", 0, 2, 0), ("H", 3, 2, 0), ("MB", 0, 0, 0), ("RF", 2, 2, 1),
        ("MB", 0, 1, 0), ("MB", 0, 2, 0), ("MB", 0, 3, 0), ("D", 3, 0, 0), ("MP", 0, 0, 0),
        ("MP", 0, 1, 0), ("RF", 2, 3, 1), ("MP", 0, 2, 0), ("MP", 0, 3, 0), ("H", 2, 2, 1),
        ("D", 3, 2, 0), ("D", 2, 2, 1), ("MO", 0, 0, 0), ("S", 3, 0, 0), ("S", 3, 1, 0),
        ("D", 2, 0, 1), ("S", 3, 2, 0), ("S", 0, 0, 0), ("S", 3, 3, 0), ("S", 0, 1, 0),
        ("S", 2, 2, 1), ("S", 0, 2, 0), ("S", 2, 3, 1), ("D", 4, 0, 0), ("S", 0, 3, 0),
        ("S", 2, 0, 1), ("FIN", 1, 2, 1), ("S", 2, 1, 1), ("FIN", 1, 3, 1), ("FIN", 1, 0, 1),
        ("DR", 0, 0, 0), ("FIN", 1, 1, 1),
    ),
    (
        ("SR", 2, 1, 1), ("SR", 2, 0, 1), ("SL", 2, 0, 1), ("SL", 2, 1, 1), ("H", 4, 0, 0),
        ("MA", 0, 0, 0), ("H", 2, 0, 0), ("H", 2, 2, 0), ("RF", 1, 0, 1), ("MA", 0, 1, 0),
        ("MA", 0, 2, 0), ("RF", 3, 0, 0), ("MA", 0, 3, 0), ("D", 4, 0, 0), ("RF", 1, 1, 1),
        ("RF", 3, 1, 0), ("H", 1, 0, 1), ("D", 2, 0, 0), ("RF", 0, 0, 0), ("RF", 3, 2, 0),
        ("D", 2, 2, 0), ("RF", 0, 1, 0), ("RF", 3, 3, 0), ("SL", 2, 2, 1), ("SL", 2, 3, 1),
        ("H", 0, 0, 0), ("RF", 0, 2, 0), ("RF", 0, 3, 0), ("D", 0, 0, 0), ("H", 0, 2, 0),
        ("RF", 1, 2, 1), ("H", 3, 0, 0), ("RF", 1, 3, 1), ("H", 1, 2, 1), ("D", 1, 2, 1),
        ("D", 0, 2, 0), ("ST", 0, 0, 0), ("D", 3, 0, 0), ("MB", 0, 0, 0), ("MB", 0, 1, 0),
        ("MB", 0, 2, 0), ("MB", 0, 3, 0), ("MP", 0, 0, 0), ("H", 3, 2, 0), ("D", 1, 0, 1),
        ("MP", 0, 1, 0), ("MP", 0, 2, 0), ("MP", 0, 3, 0), ("S", 0, 0, 0), ("S", 0, 1, 0),
        ("S", 3, 0, 0), ("S", 0, 2, 0), ("S", 3, 1, 0), ("D", 3, 2, 0), ("S", 0, 3, 0),
        ("S", 1, 2, 1), ("S", 3, 2, 0), ("S", 1, 3, 1), ("MO", 0, 0, 0), ("S", 3, 3, 0),
        ("S", 1, 0, 1), ("FIN", 2, 2, 1), ("S", 1, 1, 1), ("FIN", 2, 3, 1), ("FIN", 2, 0, 1),
        ("DR", 0, 0, 0), ("FIN", 2, 1, 1),
    ),
    (
        ("SL", 3, 0, 0), ("SL", 3, 1, 0), ("SL", 3, 2, 0), ("H", 4, 0, 0), ("SL", 3, 3, 0),
        ("MA", 0, 0, 0), ("MA", 0, 1, 0), ("H", 3, 0, 0), ("H", 3, 2, 0), ("MA", 0, 2, 0),
        ("MA", 0, 3, 0), ("D", 4, 0, 0), ("RX", 2, 0, 1), ("RX", 2, 1, 1), ("H", 2, 0, 1),
        ("RF", 1, 0, 1), ("D", 3, 0, 0), ("D", 3, 2, 0), ("RF", 1, 1, 1), ("H", 1, 0, 1),
        ("RF", 2, 2, 1), ("RF", 0, 0, 0), ("RF", 2, 3, 1), ("RF", 0, 1, 0), ("H", 2, 2, 1),
        ("H", 0, 0, 0), ("D", 2, 2, 1), ("RF", 0, 2, 0), ("S", 2, 2, 1), ("S", 2, 3, 1),
        ("RF", 0, 3, 0), ("H", 0, 2, 0), ("D", 2, 0, 1), ("RF", 1, 2, 1), ("S", 2, 0, 1),
        ("D", 0, 0, 0), ("S", 2, 1, 1), ("RF", 1, 3, 1), ("S", 0, 0, 0), ("S", 0, 1, 0),
        ("H", 1, 2, 1), ("D", 0, 2, 0), ("D", 1, 2, 1), ("ST", 0, 0, 0), ("S", 0, 2, 0),
        ("S", 0, 3, 0), ("S", 1, 2, 1), ("S", 1, 3, 1), ("MB", 0, 0, 0), ("MB", 0, 1, 0),
        ("MB", 0, 2, 0), ("MB", 0, 3, 0), ("MP", 0, 0, 0), ("MP", 0, 1, 0), ("D", 1, 0, 1),
        ("MP", 0, 2, 0), ("MP", 0, 3, 0), ("S", 1, 0, 1), ("S", 1, 1, 1), ("FIN", 3, 0, 0),
        ("FIN", 3, 1, 0), ("MO", 0, 0, 0), ("FIN", 3, 2, 0), ("DR", 0, 0, 0), ("FIN", 3, 3, 0),
    ),
)


def chip_orders(chips):
    return ORDERS


def packed_orders(chips):
    orders = chip_orders(chips)
    steps = max(len(order) for order in orders)
    steps = -(-steps // 2) * 2
    words = []
    for order in orders:
        codes = [
            (NUMBER[kind] * 64 + source * SPLIT + part) * 2 + turned
            for kind, source, part, turned in order
        ]
        codes = codes + [0] * (steps - len(codes))
        words.append(
            [codes[i] + 32768 * codes[i + 1] for i in range(0, steps, 2)]
        )
    return steps, words


def dot(a, b):
    return jnp.dot(a, b, preferred_element_type=jnp.float32)


def dot_nt(a, b):
    return lax.dot_general(a, b, (((1,), (1,)), ((), ())), preferred_element_type=jnp.float32)


def dot_tn(a, b):
    return lax.dot_general(a, b, (((0,), (0,)), ((), ())), preferred_element_type=jnp.float32)


def fused_kernel(
    count,
    query_hbm,
    forget_hbm,
    value_hbm,
    output_gate_hbm,
    out_weight_hbm,
    x_hbm,
    gate_hbm,
    up_hbm,
    down_hbm,
    shared_gate_hbm,
    shared_up_hbm,
    shared_down_hbm,
    margin_hbm,
    extra_hbm,
    head_gain_hbm,
    index_hbm,
    score_hbm,
    gain_hbm,
    recurrent_ref,
    expert_ref,
    margin_ref,
    extra_ref,
    head_gain_ref,
    index_ref,
    score_ref,
    gain_ref,
    query_v,
    forget_v,
    value_v,
    output_gate_v,
    out_weight_v,
    x_v,
    gate_w,
    up_w,
    down_w,
    rows,
    gates,
    own_hidden,
    peer_hidden,
    result,
    side_result,
    inward,
    final,
    outward,
    local_out,
    carried_query,
    own_state,
    own_decay,
    side_state,
    side_decay,
    before,
    next_state,
    gated,
    mixed,
    mixed_peer,
    load_sem,
    row_sem,
    table_sem,
    right_sem,
    left_sem,
    side_sem,
    cross_sem,
    table_right,
    table_left,
    table_side,
    hidden_send,
    hidden_recv,
    result_send,
    result_recv,
    outward_send,
    inward_recv,
    final_recv,
    state_send,
    state_recv,
    mixed_send,
    mixed_recv,
):
    f32, bf16 = jnp.float32, jnp.bfloat16
    chips = count // 2
    me = lax.axis_index("ep")
    half = lax.axis_index("tp")
    chip, core = me // 2, me % 2
    other = 1 - core
    side = chip * 2 + other
    partner = 1 - half
    has_right, has_left = chip < chips - 1, chip > 0
    length = query_v.shape[0]
    heads = extra_ref.shape[0]
    mine = heads // 2
    part_rows = rows.shape[1]
    units = gate_w.shape[2]
    routed = chips * SPLIT
    last = chips * COARSE
    coarse_rows = GROUP * part_rows
    tiles = 4
    tile = out_weight_v.shape[1] // tiles
    steps, words = packed_orders(chips)

    def half_rows(ref, which):
        return ref.at[pl.ds(pl.multiple_of(which * units, units), units), :]

    loads = dict(
        x=(x_hbm, x_v),
        gain=(gain_hbm, gain_ref),
        index=(index_hbm, index_ref),
        score=(score_hbm, score_ref),
        shared_gate=(shared_gate_hbm, gate_w.at[1]),
        shared_up=(shared_up_hbm, up_w.at[1]),
        forget=(forget_hbm, forget_v),
        query=(query_hbm, query_v),
        value=(value_hbm, value_v),
        margin=(margin_hbm, margin_ref),
        extra=(extra_hbm, extra_ref),
        gate=(gate_hbm.at[0], gate_w.at[0]),
        up=(up_hbm.at[0], up_w.at[0]),
        shared_down0=(half_rows(shared_down_hbm, half), down_w.at[1, 0]),
        shared_down1=(half_rows(shared_down_hbm, partner), down_w.at[1, 1]),
        down0=(half_rows(down_hbm.at[0], half), down_w.at[0, 0]),
        down1=(half_rows(down_hbm.at[0], partner), down_w.at[0, 1]),
        output_gate=(output_gate_hbm, output_gate_v),
        head_gain=(head_gain_hbm, head_gain_ref),
        out_weight=(out_weight_hbm, out_weight_v),
    )
    copies = {
        name: pltpu.make_async_copy(source, target, load_sem.at[i])
        for i, (name, (source, target)) in enumerate(loads.items())
    }
    early = ("x", "gain", "index", "score")
    for name in early:
        copies[name].start()

    barrier = pltpu.get_barrier_semaphore()
    pl.semaphore_signal(barrier, inc=1, device_id={"ep": side}, device_id_type=MESH)
    pl.semaphore_signal(barrier, inc=1, device_id={"tp": partner}, device_id_type=MESH)

    def greet(there):
        pl.semaphore_signal(barrier, inc=1, device_id={"ep": there}, device_id_type=MESH)

    greeted = 2
    if any(kind == "SX" for order in chip_orders(chips) for kind, *_ in order):
        for distance in range(1, chips):
            greet((chip + distance) % chips * 2 + core)
        greeted = greeted + chips - 1
    else:
        pl.when(has_right)(functools.partial(greet, me + 2))
        pl.when(has_left)(functools.partial(greet, me - 2))
        greeted = greeted + has_right.astype(jnp.int32) + has_left.astype(jnp.int32)

    for name in copies:
        if name not in early:
            copies[name].start()

    def loaded(*names):
        for name in names:
            copies[name].wait()

    def remote(source, target, send, recv, **device):
        return pltpu.make_async_remote_copy(
            src_ref=source,
            dst_ref=target,
            send_sem=send,
            recv_sem=recv,
            device_id=device,
            device_id_type=MESH,
        )

    def row_copy(arg, sems, target):
        block = arg * 2 + core
        return remote(rows.at[block], rows.at[block], sems.at[arg], row_sem.at[block], ep=target)

    def cross_copy(arg):
        block = arg * 2 + core
        return remote(
            rows.at[block], rows.at[block], cross_sem.at[arg], row_sem.at[block], tp=partner
        )

    def table_copy(source, sems, target):
        block = source * 2 + core
        return remote(
            gates.at[block], gates.at[block], sems.at[source], table_sem.at[block], ep=target
        )

    def arrived_row(block):
        remote(rows.at[block], rows.at[block], side_sem.at[0], row_sem.at[block], ep=side).wait_recv()

    def arrived_table(block):
        remote(
            gates.at[block], gates.at[block], table_side.at[0], table_sem.at[block], ep=side
        ).wait_recv()

    def hidden_copy(arg):
        return remote(
            own_hidden.at[arg],
            peer_hidden.at[arg],
            hidden_send.at[arg],
            hidden_recv.at[arg],
            tp=partner,
        )

    def result_copy(arg):
        return remote(
            result.at[arg, other],
            side_result.at[arg],
            result_send.at[arg],
            result_recv.at[arg],
            ep=side,
        )

    def outward_copy(arg, target, target_sem, to):
        return remote(outward.at[arg], target, outward_send.at[arg], target_sem, ep=to)

    own_heads = pl.ds(core * mine, mine)
    state_copies = dict(
        state=lambda: remote(
            own_state, side_state, state_send.at[0], state_recv.at[0], ep=side
        ),
        decay=lambda: remote(
            own_decay, side_decay, state_send.at[1], state_recv.at[1], ep=side
        ),
        before=lambda: remote(
            before.at[own_heads],
            before.at[own_heads],
            state_send.at[2],
            state_recv.at[2],
            ep=side,
        ),
        chain=lambda: remote(
            next_state, before.at[own_heads], state_send.at[3], state_recv.at[3], ep=me + 2
        ),
    )

    def mixed_copy(n):
        lanes = pl.ds(pl.multiple_of(n * tile, tile), tile)
        return remote(
            mixed.at[partner, :, lanes],
            mixed_peer.at[:, lanes],
            mixed_send.at[n],
            mixed_recv.at[n],
            tp=partner,
        )

    loaded("x", "gain")
    x = x_v[...].astype(f32)
    normed = (
        x * lax.rsqrt(jnp.mean(x * x, axis=1, keepdims=True) + EPSILON) * gain_ref[...]
    ).astype(bf16)
    for part in range(SPLIT):
        rows[(chip * SPLIT + part) * 2 + core] = normed[part * part_rows : (part + 1) * part_rows]
    loaded("index", "score")
    score = score_ref[...]
    weight = ROUTED_SCALE * score / jnp.sum(score, axis=0, keepdims=True)
    expert = lax.broadcasted_iota(jnp.int32, (count, length), 0)
    table = jnp.zeros((count, length), f32)
    for k in range(score.shape[0]):
        table = table + jnp.where(expert == index_ref[k : k + 1, :], weight[k : k + 1, :], 0.0)
    gates[chip * 2 + core] = table

    pl.semaphore_wait(barrier, greeted)

    @pl.when(has_right)
    def _():
        table_copy(chip, table_right, me + 2).start()

    @pl.when(has_left)
    def _():
        table_copy(chip, table_left, me - 2).start()

    for part in range(SPLIT):
        row_copy(chip * SPLIT + part, side_sem, side).start()
    table_copy(chip, table_side, side).start()

    def send_right(arg, first):
        row_copy(arg, right_sem, me + 2).start()

    def send_left(arg, first):
        row_copy(arg, left_sem, me - 2).start()

    def forward(arg, first, onward=True):
        source = arg // SPLIT
        arrived_row(arg * 2 + core)
        to_right = jnp.logical_and(source < chip, has_right)
        to_left = jnp.logical_and(source > chip, has_left)

        @pl.when(first)
        def _():
            arrived_table(source * 2 + core)

            @pl.when(to_right)
            def _():
                table_copy(source, table_right, me + 2).start()

            @pl.when(to_left)
            def _():
                table_copy(source, table_left, me - 2).start()

            table_copy(source, table_side, side).start()

        if onward:

            @pl.when(to_right)
            def _():
                send_right(arg, first)

            @pl.when(to_left)
            def _():
                send_left(arg, first)

        row_copy(arg, side_sem, side).start()

    def cross(arg, first):
        forward(arg, first)
        cross_copy(arg).start()

    def mix_local(arg, first):
        @pl.when(arg == 0)
        def _():
            loaded("forget", "query", "value", "margin", "extra")

        row = lax.broadcasted_iota(jnp.int32, (length, length), 0)
        column = lax.broadcasted_iota(jnp.int32, (length, length), 1)
        upper = row < BLK
        left = column < BLK
        causal = jnp.logical_and(row >= column, upper == left)
        crossed = jnp.logical_and(jnp.logical_not(upper), left)
        ones = causal.astype(f32).astype(bf16)
        head_lane = lax.broadcasted_iota(jnp.int32, (length, heads), 1)
        extra_columns = extra_ref[...].T
        middle = BLK // 2 - 1

        def one_head(h):
            lanes = pl.ds(pl.multiple_of(h * HEAD_CHANNELS, HEAD_CHANNELS), HEAD_CHANNELS)
            query = jax.nn.silu(query_v[:, lanes].astype(f32))
            key = margin_ref[:, lanes] * jax.nn.sigmoid(-forget_v[:, lanes].astype(f32))
            extra = jnp.sum(
                jnp.where(head_lane == h, extra_columns, 0.0), axis=1, keepdims=True
            )
            decay = jnp.log1p(-key) + extra
            high = decay.astype(bf16)
            rest = decay - high.astype(f32)
            mid = rest.astype(bf16)
            low = (rest - mid.astype(f32)).astype(bf16)
            total = dot(ones, high) + dot(ones, mid) + dot(ones, low)
            center = jnp.where(upper, total[middle : middle + 1], total[BLK + middle : BLK + middle + 1])
            end = jnp.where(upper, total[BLK - 1 : BLK], total[2 * BLK - 1 : 2 * BLK])
            first = jnp.exp(total[BLK - 1 : BLK])
            second = jnp.exp(total[2 * BLK - 1 : 2 * BLK])
            query_end = query * jnp.exp(total)
            key_end = key * jnp.exp(end - total)
            near = dot_nt(
                (query * jnp.exp(total - center)).astype(bf16),
                (key * jnp.exp(center - total)).astype(bf16),
            )
            far = dot_nt(query_end.astype(bf16), key_end.astype(bf16))
            scores = jnp.where(causal, near, jnp.where(crossed, far, 0.0)).astype(bf16)
            value = value_v[:, lanes]
            local_out[:, lanes] = dot(scores, value)
            carried_query[:, lanes] = jnp.where(upper, query_end, query_end * first).astype(bf16)
            key_state = jnp.where(upper, key_end * second, key_end).astype(bf16)
            own_state[h] = dot_tn(value, key_state).astype(bf16)
            own_decay[pl.ds(h, 1), :] = first * second

        one_head(2 * arg)
        one_head(2 * arg + 1)

        @pl.when(arg == heads // 2 - 1)
        def _():
            state_copies["state"]().start()
            state_copies["decay"]().start()

    def mix_state(arg, first):
        state_copies["state"]().wait_recv()
        state_copies["decay"]().wait_recv()

        @pl.when(has_left)
        def _():
            state_copies["chain"]().wait_recv()
            state_copies["before"]().start()

        @pl.when(jnp.logical_not(has_left))
        def _():
            before[...] = jnp.zeros(before.shape, bf16)

        @pl.when(has_right)
        def _():
            def one_head(i, _):
                h = core * mine + i
                own, beside = own_state[h].astype(f32), side_state[h].astype(f32)
                own_d, beside_d = own_decay[pl.ds(h, 1), :], side_decay[pl.ds(h, 1), :]
                state0 = jnp.where(core == 0, own, beside)
                state1 = jnp.where(core == 0, beside, own)
                decay1 = jnp.where(core == 0, beside_d, own_d)
                carried = before[h].astype(f32) * (own_d * beside_d)
                next_state[i] = (carried + decay1 * state0 + state1).astype(bf16)
                return 0

            lax.fori_loop(0, mine, one_head, 0)
            state_copies["chain"]().start()

    def mix_finish(arg, first):
        @pl.when(arg == 0)
        def _():
            loaded("output_gate", "head_gain")

        @pl.when(jnp.logical_and(arg == 0, has_left))
        def _():
            state_copies["before"]().wait_recv()

        def one_head(h):
            lanes = pl.ds(pl.multiple_of(h * HEAD_CHANNELS, HEAD_CHANNELS), HEAD_CHANNELS)
            state = before[h].astype(f32)
            beside = side_state[h].astype(f32)
            later = side_decay[pl.ds(h, 1), :] * state + beside
            state = jnp.where(core == 0, state, later).astype(bf16)
            out = local_out[:, lanes] + dot_nt(carried_query[:, lanes], state)
            factor = lax.rsqrt(jnp.mean(out * out, axis=1, keepdims=True) + EPSILON)
            gate = jax.nn.silu(output_gate_v[:, lanes].astype(f32))
            gated[:, lanes] = (out * factor * head_gain_ref[:, lanes] * gate).astype(bf16)

        one_head(2 * arg)
        one_head(2 * arg + 1)

    def mix_project(arg, first):
        @pl.when(arg == 0)
        def _():
            loaded("out_weight")

        kept = length // 2
        lanes = pl.ds(pl.multiple_of(arg * tile, tile), tile)
        partial = dot(gated[...], out_weight_v[:, lanes]).astype(bf16)
        mixed[0, :, lanes] = partial[:kept]
        mixed[1, :, lanes] = partial[kept:]

        mixed_copy(arg).start()

    def mix_out(arg, first):
        for n in range(tiles):
            mixed_copy(n).wait_recv()

        recurrent_ref[...] = (mixed[half].astype(f32) + mixed_peer[...].astype(f32)).astype(bf16)

    def hidden_part(arg, first):
        shared = arg == routed
        chunk = arg // GROUP
        source, place = chunk // COARSE, chunk % COARSE

        @pl.when(shared)
        def _():
            loaded("shared_gate", "shared_up")

        @pl.when(jnp.logical_and(source == chip, first))
        def _():
            loaded("gate", "up")

        @pl.when(jnp.logical_not(shared))
        def _():
            for p in range(GROUP):
                arrived_row((arg + p) * 2 + other)

            @pl.when(first)
            def _():
                arrived_table(source * 2 + other)

        which = shared.astype(jnp.int32)
        pieces = []
        for parity in range(2):
            for p in range(GROUP):
                own = (chip * SPLIT + parity * GROUP + p) * 2 + core
                pieces.append(rows[jnp.where(shared, own, (arg + p) * 2 + parity)])
        x = jnp.concatenate(pieces, axis=0)
        lane = lax.broadcasted_iota(jnp.int32, (length, count), 1)
        block_low = jnp.where(shared, chip * 2 + core, source * 2)
        block_high = jnp.where(shared, chip * 2 + core, source * 2 + 1)

        def own_gate(block):
            column = jnp.sum(jnp.where(lane == me, gates[block].T, 0.0), axis=1, keepdims=True)
            return jnp.where(place == 0, column[:coarse_rows], column[coarse_rows:])

        routed_gate = jnp.concatenate([own_gate(block_low), own_gate(block_high)], axis=0)
        scale = jnp.where(shared, 1.0, routed_gate)
        gate_part = dot(x, gate_w[which])
        up_part = dot(x, up_w[which])
        own_hidden[chunk] = (jax.nn.silu(gate_part) * up_part * scale).astype(bf16)
        hidden_copy(chunk).start()

    def down_part(arg, first):
        shared = arg == routed
        chunk = arg // GROUP
        which = shared.astype(jnp.int32)

        @pl.when(shared)
        def _():
            loaded("shared_down0", "shared_down1")

        @pl.when(jnp.logical_and(chunk // COARSE == chip, first))
        def _():
            loaded("down0", "down1")

        hidden_copy(chunk).wait_recv()
        out = dot(own_hidden[chunk], down_w[which, 0]) + dot(peer_hidden[chunk], down_w[which, 1])
        out = out.astype(bf16)
        result[chunk, 0] = out[:coarse_rows]
        result[chunk, 1] = out[coarse_rows:]

        @pl.when(jnp.logical_not(shared))
        def _():
            result_copy(chunk).start()

    def part_slice(arg):
        return pl.ds(pl.multiple_of(arg % GROUP * part_rows, part_rows), part_rows)

    def chip_sum(arg, awaited):
        chunk = arg // GROUP

        @pl.when(awaited)
        def _():
            result_copy(chunk).wait_recv()

        inside = part_slice(arg)
        return result[chunk, core, inside].astype(f32) + side_result[chunk, inside].astype(f32)

    def final_copy(arg):
        slot = chip * SPLIT + arg % SPLIT
        there = arg // SPLIT * 2 + core
        return outward_copy(arg, final.at[slot], final_recv.at[slot], there)

    def send_sum(arg, first, direct):
        target = arg // SPLIT
        adjacent = jnp.abs(target - chip) == 1
        total = chip_sum(arg, arg % GROUP == 0)
        if direct:
            outward[arg] = total.astype(bf16)
            final_copy(arg).start()
            return
        inner = jnp.logical_and(has_left, has_right)
        towards = jnp.where(target > chip, me + 2, me - 2)
        relay = outward_copy(arg, inward.at[arg], inward_recv.at[arg], towards)

        @pl.when(inner)
        def _():
            relay.wait_recv()
            outward[arg] = (total + inward[arg].astype(f32)).astype(bf16)

        @pl.when(jnp.logical_not(inner))
        def _():
            outward[arg] = total.astype(bf16)

        @pl.when(adjacent)
        def _():
            final_copy(arg).start()

        @pl.when(jnp.logical_not(adjacent))
        def _():
            relay.start()

    def finish(arg, first, left_all, right_all):
        part = arg % SPLIT
        place = pl.ds(pl.multiple_of(part * part_rows, part_rows), part_rows)
        shared = result[last, part // GROUP, part_slice(arg)].astype(f32)
        total = chip_sum(arg, arg % GROUP == 0) + shared
        for s in range(chips):
            taken = jnp.abs(chip - s) == 1
            if left_all:
                taken = jnp.logical_or(taken, chip > s)
            if right_all:
                taken = jnp.logical_or(taken, chip < s)
            slot = s * SPLIT + part

            @pl.when(taken)
            def _():
                outward_copy(arg, final.at[slot], final_recv.at[slot], side).wait_recv()

            total = total + jnp.where(taken, final[slot].astype(f32), 0.0)
        expert_ref[place, :] = total.astype(bf16)

    def drain_all(_, first):
        def drain(arg, _):
            source, part = arg // SPLIT, arg % SPLIT
            row_copy(arg, side_sem, side).wait_send()
            to_right = jnp.logical_and(source <= chip, has_right)
            to_left = jnp.logical_and(source >= chip, has_left)
            row_right, row_left = to_right, to_left
            if CROSSED:
                inner = jnp.logical_and(source > 0, source < chips - 1)
                kept = (part + half * (SPLIT // 2)) % SPLIT < SPLIT // 2

                def crosses(end):
                    if CROSSED == 2:
                        return inner
                    return jnp.logical_and(inner, jnp.abs(source - end) == 1)

                held = jnp.logical_not(kept)
                to_last = jnp.logical_and(chip == chips - 2, crosses(chips - 1))
                to_first = jnp.logical_and(chip == 1, crosses(0))
                row_right = jnp.logical_and(to_right, jnp.logical_not(jnp.logical_and(held, to_last)))
                row_left = jnp.logical_and(to_left, jnp.logical_not(jnp.logical_and(held, to_first)))
                ends = jnp.logical_or(
                    jnp.logical_and(chip == chips - 1, crosses(chips - 1)),
                    jnp.logical_and(chip == 0, crosses(0)),
                )

                @pl.when(jnp.logical_and(ends, kept))
                def _():
                    cross_copy(arg).wait_send()

            @pl.when(row_right)
            def _():
                row_copy(arg, right_sem, me + 2).wait_send()

            @pl.when(row_left)
            def _():
                row_copy(arg, left_sem, me - 2).wait_send()

            @pl.when(source != chip)
            def _():
                outward_copy(arg, inward.at[arg], inward_recv.at[arg], side).wait_send()

            @pl.when(part == 0)
            def _():
                table_copy(source, table_side, side).wait_send()

                @pl.when(to_right)
                def _():
                    table_copy(source, table_right, me + 2).wait_send()

                @pl.when(to_left)
                def _():
                    table_copy(source, table_left, me - 2).wait_send()

            return 0

        lax.fori_loop(0, routed, drain, 0)

        def drain_chunk(chunk, _):
            hidden_copy(chunk).wait_send()
            result_copy(chunk).wait_send()
            return 0

        lax.fori_loop(0, last, drain_chunk, 0)
        hidden_copy(last).wait_send()
        state_copies["state"]().wait_send()
        state_copies["decay"]().wait_send()

        @pl.when(has_left)
        def _():
            state_copies["before"]().wait_send()

        @pl.when(has_right)
        def _():
            state_copies["chain"]().wait_send()

        for n in range(tiles):
            mixed_copy(n).wait_send()

    actions = dict(
        SR=send_right,
        SL=send_left,
        RF=forward,
        RX=cross,
        RN=functools.partial(forward, onward=False),
        MA=mix_local,
        ST=mix_state,
        H=hidden_part,
        D=down_part,
        S=functools.partial(send_sum, direct=False),
        SX=functools.partial(send_sum, direct=True),
        FIN=functools.partial(finish, left_all=False, right_all=False),
        FL=functools.partial(finish, left_all=True, right_all=False),
        FR=functools.partial(finish, left_all=False, right_all=True),
        FB=functools.partial(finish, left_all=True, right_all=True),
        MB=mix_finish,
        MP=mix_project,
        MO=mix_out,
        DR=drain_all,
    )
    mine_words = []
    for n in range(steps // 2):
        word = jnp.int32(words[0][n])
        for c in range(1, chips):
            word = jnp.where(chip == c, words[c][n], word)
        mine_words.append(word)

    def turn(i, _):
        place, digit = i // 2, i % 2
        word = mine_words[0]
        for n in range(1, steps // 2):
            word = jnp.where(place == n, mine_words[n], word)
        code = jnp.where(
            digit == 0, word % 32768, word // 32768
        )
        kind, arg, turned = code // 128, code // 2 % 64, code % 2
        first = arg % SPLIT == 0
        shift = (arg % SPLIT + half * (SPLIT // 2)) % SPLIT
        arg = jnp.where(turned == 1, arg // SPLIT * SPLIT + shift, arg)
        for name, action in actions.items():

            @pl.when(kind == NUMBER[name])
            def _():
                action(arg, first)

        return 0

    lax.fori_loop(0, steps, turn, 0)


def fused_fits(position_decay_extra, chosen_expert_index, routed_gate_weight):
    count, tensor = lax.axis_size("ep"), lax.axis_size("tp")
    length, heads = position_decay_extra.shape
    tokens, top = chosen_expert_index.shape
    every_row_fits = 2 * top >= count and routed_gate_weight.shape[0] == 1
    sizes = length == tokens == 2 * BLK and heads % 2 == 0
    return every_row_fits and sizes and tensor == 2 and count % 2 == 0 and count == 2 * len(ORDERS)


def fused_layer(
    recurrence_query_input,
    forget_gate_input,
    recurrence_value_input,
    output_gate_input,
    forget_lower_margin,
    position_decay_extra,
    head_norm_gain,
    recurrence_out_weight,
    expert_hidden_state,
    chosen_expert_index,
    chosen_expert_score,
    expert_norm_gain,
    routed_gate_weight,
    routed_up_weight,
    routed_down_weight,
    shared_gate_weight,
    shared_up_weight,
    shared_down_weight,
):
    f32, bf16 = jnp.float32, jnp.bfloat16
    count = lax.axis_size("ep")
    chips = count // 2
    routed = chips * SPLIT
    length, channels = recurrence_query_input.shape
    heads = position_decay_extra.shape[1]
    width, width_out = expert_hidden_state.shape[1], recurrence_out_weight.shape[1]
    units, features = routed_gate_weight.shape[2], routed_down_weight.shape[2]
    part_rows = length // SPLIT
    hbm = pl.BlockSpec(memory_space=pltpu.HBM)
    vmem = pl.BlockSpec(memory_space=pltpu.VMEM)
    dma = pltpu.SemaphoreType.DMA
    mixer_rows = pltpu.VMEM((length, channels), bf16)
    coarse_rows = length // COARSE
    chunks = chips * COARSE + 1
    hidden = pltpu.VMEM((chunks, 2 * coarse_rows, units), bf16)
    partial = pltpu.VMEM((routed, part_rows, features), bf16)
    state = pltpu.VMEM((heads, HEAD_CHANNELS, HEAD_CHANNELS), bf16)
    decay = pltpu.VMEM((heads, HEAD_CHANNELS), f32)
    large = [
        pltpu.with_memory_space_constraint(array, pltpu.HBM)
        for array in (
            recurrence_query_input,
            forget_gate_input,
            recurrence_value_input,
            output_gate_input,
            recurrence_out_weight,
            expert_hidden_state,
            routed_gate_weight,
            routed_up_weight,
            routed_down_weight,
            shared_gate_weight,
            shared_up_weight,
            shared_down_weight,
            forget_lower_margin[None, :],
            position_decay_extra.T,
            head_norm_gain[None, :],
            chosen_expert_index.T,
            chosen_expert_score.T,
            expert_norm_gain[None, :],
        )
    ]
    return pl.pallas_call(
        functools.partial(fused_kernel, count),
        out_shape=(
            jax.ShapeDtypeStruct((length // 2, width_out), bf16),
            jax.ShapeDtypeStruct((length, features), bf16),
        ),
        in_specs=[hbm] * 18,
        out_specs=(vmem, vmem),
        scratch_shapes=[
            *(pltpu.VMEM(array.shape, array.dtype) for array in large[12:]),
            mixer_rows,
            mixer_rows,
            mixer_rows,
            mixer_rows,
            pltpu.VMEM(recurrence_out_weight.shape, bf16),
            pltpu.VMEM((length, width), bf16),
            pltpu.VMEM((2, width, units), bf16),
            pltpu.VMEM((2, width, units), bf16),
            pltpu.VMEM((2, 2, units, features), bf16),
            pltpu.VMEM((routed * 2, part_rows, width), bf16),
            pltpu.VMEM((count, count, length), f32),
            hidden,
            hidden,
            pltpu.VMEM((chunks, 2, coarse_rows, features), bf16),
            pltpu.VMEM((chunks, coarse_rows, features), bf16),
            partial,
            partial,
            partial,
            pltpu.VMEM((length, channels), f32),
            mixer_rows,
            state,
            decay,
            state,
            decay,
            state,
            pltpu.VMEM((heads // 2, HEAD_CHANNELS, HEAD_CHANNELS), bf16),
            mixer_rows,
            pltpu.VMEM((2, length // 2, width_out), bf16),
            pltpu.VMEM((length // 2, width_out), bf16),
            dma((20,)),
            dma((routed * 2,)),
            dma((count,)),
            dma((routed,)),
            dma((routed,)),
            dma((routed,)),
            dma((routed,)),
            dma((chips,)),
            dma((chips,)),
            dma((chips,)),
            dma((chunks,)),
            dma((chunks,)),
            dma((chunks,)),
            dma((chunks,)),
            dma((routed,)),
            dma((routed,)),
            dma((routed,)),
            dma((4,)),
            dma((4,)),
            dma((4,)),
            dma((4,)),
        ],
        compiler_params=pltpu.CompilerParams(
            collective_id=0, has_side_effects=True, vmem_limit_bytes=46 * 1024 * 1024
        ),
        cost_estimate=pl.CostEstimate(
            flops=9_000_000_000, bytes_accessed=18_000_000, transcendentals=0
        ),
        name="fused_kernel",
    )(
        *large,
    )


def per_device(
    recurrence_query_input,
    forget_gate_input,
    recurrence_value_input,
    output_gate_input,
    forget_lower_margin,
    position_decay_extra,
    head_norm_gain,
    recurrence_out_weight,
    expert_hidden_state,
    chosen_expert_index,
    chosen_expert_score,
    expert_norm_gain,
    routed_gate_weight,
    routed_up_weight,
    routed_down_weight,
    shared_gate_weight,
    shared_up_weight,
    shared_down_weight,
):
    if fused_fits(position_decay_extra, chosen_expert_index, routed_gate_weight):
        return fused_layer(
            recurrence_query_input,
            forget_gate_input,
            recurrence_value_input,
            output_gate_input,
            forget_lower_margin,
            position_decay_extra,
            head_norm_gain,
            recurrence_out_weight,
            expert_hidden_state,
            chosen_expert_index,
            chosen_expert_score,
            expert_norm_gain,
            routed_gate_weight,
            routed_up_weight,
            routed_down_weight,
            shared_gate_weight,
            shared_up_weight,
            shared_down_weight,
        )
    recurrence_output = mixer_half(
        recurrence_query_input,
        forget_gate_input,
        recurrence_value_input,
        output_gate_input,
        forget_lower_margin,
        position_decay_extra,
        head_norm_gain,
        recurrence_out_weight,
    )
    expert_out = expert_half(
        expert_hidden_state,
        chosen_expert_index,
        chosen_expert_score,
        expert_norm_gain,
        routed_gate_weight,
        routed_up_weight,
        routed_down_weight,
        shared_gate_weight,
        shared_up_weight,
        shared_down_weight,
    )
    return (recurrence_output, expert_out)


def solution(mesh):
    in_specs = (
        P(("grp", "ep"), "tp"),
        P(("grp", "ep"), "tp"),
        P(("grp", "ep"), "tp"),
        P(("grp", "ep"), "tp"),
        P("tp"),
        P(("grp", "ep"), "tp"),
        P("tp"),
        P("tp", None),
        P(("grp", "ep"), None),
        P(("grp", "ep"), None),
        P(("grp", "ep"), None),
        P(),
        P("ep", None, "tp"),
        P("ep", None, "tp"),
        P("ep", None, "tp"),
        P(None, "tp"),
        P(None, "tp"),
        P(None, "tp"),
    )
    out_specs = (P(("grp", "ep", "tp"), None), P(("grp", "ep"), "tp"))
    return jax.shard_map(
        per_device, mesh=mesh, in_specs=in_specs, out_specs=out_specs, check_vma=False
    )
```

```python
import functools

import jax
import jax.numpy as jnp
from jax import lax
from jax.experimental import pallas as pl
from jax.experimental.pallas import tpu as pltpu
from jax.sharding import PartitionSpec as P

HEAD_CHANNELS = 128
BLK = 64


EPSILON = 1e-06
ROUTED_SCALE = 2.5
PRECISION = lax.Precision.DEFAULT


DECAY_ROWS = 16


def carried_in(decay, state, axis):
    count, index = (lax.axis_size(axis), lax.axis_index(axis))
    depth = state.shape[1]
    rows = jnp.broadcast_to(decay[:, None, :], (decay.shape[0], DECAY_ROWS, decay.shape[1]))
    sent = jnp.concatenate([state, rows], axis=1).astype(jnp.bfloat16)
    everything = lax.all_gather(sent, axis)
    before = jnp.zeros_like(state)
    for k in range(count - 1):
        part = everything[k].astype(jnp.float32)
        new = part[:, depth : depth + 1] * before + part[:, :depth]
        before = jnp.where(k < index, new, before)
    return before


def mixer_half(
    recurrence_query_input,
    forget_gate_input,
    recurrence_value_input,
    output_gate_input,
    forget_lower_margin,
    position_decay_extra,
    head_norm_gain,
    recurrence_out_weight,
):
    length = recurrence_query_input.shape[0]
    head_tensor = position_decay_extra.shape[1]
    blocks = length // BLK
    queries = jax.nn.silu(recurrence_query_input.astype(jnp.float32))
    key_gate_value = forget_lower_margin[None, :] * jax.nn.sigmoid(
        -forget_gate_input.astype(jnp.float32)
    )
    decay_logarithm = jnp.log1p(-key_gate_value) + jnp.repeat(
        position_decay_extra, HEAD_CHANNELS, axis=1
    )
    value_rows = recurrence_value_input.astype(jnp.float32)

    def split_heads(tensor):
        return tensor.reshape(blocks, BLK, head_tensor, HEAD_CHANNELS).transpose(2, 0, 1, 3)

    query_heads = split_heads(queries)
    key_heads = split_heads(key_gate_value)
    value_heads = split_heads(value_rows)
    cum_decay = jnp.cumsum(split_heads(decay_logarithm), axis=2)
    middle = cum_decay[:, :, BLK // 2 - 1 : BLK // 2]
    block_end = cum_decay[:, :, BLK - 1 : BLK]
    scores = jnp.einsum(
        "hncd,hnsd->hncs",
        query_heads * jnp.exp(cum_decay - middle),
        key_heads * jnp.exp(middle - cum_decay),
        precision=PRECISION,
    )
    causal = jnp.tril(jnp.ones((BLK, BLK), dtype=bool))
    scores = jnp.where(causal, scores, 0.0)
    within = jnp.einsum("hncs,hnse->hnce", scores, value_heads, precision=PRECISION)
    updates = jnp.einsum(
        "hncd,hnce->nhed",
        key_heads * jnp.exp(block_end - cum_decay),
        value_heads,
        precision=PRECISION,
    )
    block_log = block_end[:, :, 0, :]
    block_decay = jnp.exp(block_log).transpose(1, 0, 2)

    state = jnp.zeros_like(updates[0])
    starts_list = []
    for block in range(blocks):
        starts_list.append(state)
        state = block_decay[block][:, None, :] * state + updates[block]
    local_final, local_starts = state, jnp.stack(starts_list)
    device_decay = jnp.exp(jnp.sum(block_log, axis=1))
    incoming = carried_in(device_decay, local_final, "ep")
    before = jnp.exp(jnp.cumsum(block_log, axis=1) - block_log).transpose(1, 0, 2)
    starts = local_starts + before[:, :, None, :] * incoming[None]
    carried = jnp.einsum(
        "hncd,nhed->hnce", query_heads * jnp.exp(cum_decay), starts, precision=PRECISION
    )
    outputs = (within + carried).transpose(1, 2, 0, 3).reshape(length, head_tensor, HEAD_CHANNELS)
    factor = lax.rsqrt(jnp.mean(outputs * outputs, axis=2, keepdims=True) + EPSILON)
    normed = (outputs * factor).reshape(length, head_tensor * HEAD_CHANNELS) * head_norm_gain[
        None, :
    ]
    gated_rows = (normed * jax.nn.silu(output_gate_input.astype(jnp.float32))).astype(jnp.bfloat16)
    partial = jnp.dot(
        gated_rows, recurrence_out_weight, preferred_element_type=jnp.float32
    ).astype(jnp.bfloat16)
    if lax.axis_size("tp") != 2:
        return lax.psum_scatter(partial, "tp", scatter_dimension=0, tiled=True)
    which, kept_rows = lax.axis_index("tp"), length // 2
    kept = lax.dynamic_slice_in_dim(partial, which * kept_rows, kept_rows)
    sent = lax.dynamic_slice_in_dim(partial, (1 - which) * kept_rows, kept_rows)
    received = lax.ppermute(sent, "tp", [(0, 1), (1, 0)])
    return (kept.astype(jnp.float32) + received.astype(jnp.float32)).astype(jnp.bfloat16)


def expert_half(
    expert_hidden_state,
    chosen_expert_index,
    chosen_expert_score,
    expert_norm_gain,
    routed_gate_weight,
    routed_up_weight,
    routed_down_weight,
    shared_gate_weight,
    shared_up_weight,
    shared_down_weight,
):
    tokens, top = chosen_expert_index.shape
    local_experts = routed_gate_weight.shape[0]
    devices = lax.axis_size("ep")
    experts = local_experts * devices
    capacity = min(tokens, 2 * tokens * top // experts)
    width_out = routed_down_weight.shape[2]
    features = expert_hidden_state.astype(jnp.float32)
    normed = (
        features
        * lax.rsqrt(jnp.mean(features * features, axis=1, keepdims=True) + EPSILON)
        * expert_norm_gain[None, :]
    ).astype(jnp.bfloat16)
    gates = ROUTED_SCALE * chosen_expert_score / jnp.sum(chosen_expert_score, axis=1, keepdims=True)
    flat_ids = chosen_expert_index.reshape(-1)
    onehot = (flat_ids[:, None] == jnp.arange(experts, dtype=jnp.int32)[None, :]).astype(jnp.int32)
    places = jnp.sum(onehot * (jnp.cumsum(onehot, axis=0) - 1), axis=1)
    slots = flat_ids * capacity + places
    owners = (
        jnp.full((experts * capacity,), tokens, jnp.int32)
        .at[slots]
        .set(jnp.arange(tokens * top, dtype=jnp.int32) // top)
    )
    padded = jnp.concatenate([normed, jnp.zeros((1, normed.shape[1]), jnp.bfloat16)], axis=0)
    outgoing = padded[owners].reshape(experts, capacity, normed.shape[1])
    piece = lax.all_to_all(outgoing, "ep", split_axis=0, concat_axis=0, tiled=True)
    grouped = piece.reshape(devices, local_experts, piece.shape[1], piece.shape[2])
    gate_part = jnp.einsum(
        "secd,edh->sech", grouped, routed_gate_weight, preferred_element_type=jnp.float32
    )
    up_part = jnp.einsum(
        "secd,edh->sech", grouped, routed_up_weight, preferred_element_type=jnp.float32
    )
    hidden = (jax.nn.silu(gate_part) * up_part).astype(jnp.bfloat16)
    hidden_rows = hidden.reshape(devices * local_experts, piece.shape[1], hidden.shape[3])
    flat_hidden = hidden_rows.reshape(experts * capacity, hidden_rows.shape[2])
    shared_hidden = (
        jax.nn.silu(jnp.dot(normed, shared_gate_weight, preferred_element_type=jnp.float32))
        * jnp.dot(normed, shared_up_weight, preferred_element_type=jnp.float32)
    ).astype(jnp.bfloat16)
    start_values = (
        jnp.zeros((experts * capacity, width_out), jnp.float32),
        jnp.zeros((tokens, width_out), jnp.float32),
    )
    routed_piece = lax.all_gather(flat_hidden, "tp", axis=1, tiled=True)
    shared_piece = lax.all_gather(shared_hidden, "tp", axis=1, tiled=True)
    count = routed_piece.shape[1]
    grouped = routed_piece.reshape(devices, local_experts, capacity, count)
    routed = jnp.einsum(
        "secn,enk->seck", grouped, routed_down_weight, preferred_element_type=jnp.float32
    )
    shared = jnp.dot(shared_piece, shared_down_weight, preferred_element_type=jnp.float32)
    routed_sum = routed.reshape(start_values[0].shape)
    answers = routed_sum.astype(jnp.bfloat16).reshape(experts, capacity, width_out)
    returned = lax.all_to_all(answers, "ep", split_axis=0, concat_axis=0, tiled=True)
    picked_rows = returned.reshape(experts * capacity, width_out)[slots].reshape(
        tokens, top, width_out
    )
    combined = shared + jnp.sum(gates[:, :, None] * picked_rows.astype(jnp.float32), axis=1)
    return combined.astype(jnp.bfloat16)


MESH = pl.DeviceIdType.MESH
LANES = 128
SPLIT = 4
COARSE = 2
GROUP = SPLIT // COARSE
CROSSED = 1
KINDS = (
    "NO",
    "SR",
    "SL",
    "RF",
    "RX",
    "RN",
    "MA",
    "ST",
    "H",
    "D",
    "S",
    "SX",
    "FIN",
    "FL",
    "FR",
    "FB",
    "MB",
    "MP",
    "MO",
    "DR",
)
NUMBER = {name: place for place, name in enumerate(KINDS)}


ORDERS = (
    (
        ("SR", 0, 1, 0), ("SR", 0, 2, 0), ("SR", 0, 3, 0), ("H", 4, 0, 0), ("MA", 0, 0, 0),
        ("H", 0, 0, 0), ("MA", 0, 1, 0), ("MA", 0, 2, 0), ("H", 0, 2, 0), ("MA", 0, 3, 0),
        ("D", 4, 0, 0), ("ST", 0, 0, 0), ("MB", 0, 0, 0), ("RX", 1, 0, 1), ("MB", 0, 1, 0),
        ("D", 0, 0, 0), ("MB", 0, 2, 0), ("RX", 1, 1, 1), ("D", 0, 2, 0), ("H", 1, 0, 1),
        ("RF", 2, 0, 1), ("RF", 1, 2, 1), ("RF", 2, 1, 1), ("H", 2, 0, 1), ("RF", 1, 3, 1),
        ("RF", 3, 0, 0), ("H", 1, 2, 1), ("D", 1, 2, 1), ("RF", 3, 1, 0), ("S", 1, 2, 1),
        ("S", 1, 3, 1), ("MB", 0, 3, 0), ("H", 3, 0, 0), ("RF", 3, 2, 0), ("MP", 0, 0, 0),
        ("D", 1, 0, 1), ("RF", 3, 3, 0), ("S", 1, 0, 1), ("S", 1, 1, 1), ("H", 3, 2, 0),
        ("RF", 2, 2, 1), ("D", 3, 0, 0), ("S", 3, 0, 0), ("S", 3, 1, 0), ("RF", 2, 3, 1),
        ("H", 2, 2, 1), ("D", 3, 2, 0), ("D", 2, 2, 1), ("S", 3, 2, 0), ("S", 3, 3, 0),
        ("S", 2, 2, 1), ("S", 2, 3, 1), ("MP", 0, 1, 0), ("MP", 0, 2, 0), ("MP", 0, 3, 0),
        ("D", 2, 0, 1), ("S", 2, 0, 1), ("S", 2, 1, 1), ("FIN", 0, 0, 0), ("MO", 0, 0, 0),
        ("FIN", 0, 1, 0), ("FIN", 0, 2, 0), ("DR", 0, 0, 0), ("FIN", 0, 3, 0),
    ),
    (
        ("SL", 1, 1, 1), ("SL", 1, 0, 1), ("H", 4, 0, 0), ("SR", 1, 1, 1), ("MA", 0, 0, 0),
        ("MA", 0, 1, 0), ("MA", 0, 2, 0), ("H", 1, 0, 0), ("H", 1, 2, 0), ("RF", 0, 0, 0),
        ("MA", 0, 3, 0), ("RF", 2, 0, 1), ("D", 4, 0, 0), ("RF", 0, 1, 0), ("RF", 2, 1, 1),
        ("H", 0, 0, 0), ("D", 1, 0, 0), ("RF", 0, 2, 0), ("H", 2, 0, 1), ("RF", 3, 0, 0),
        ("RF", 0, 3, 0), ("SR", 1, 2, 1), ("D", 1, 2, 0), ("SR", 1, 3, 1), ("H", 0, 2, 0),
        ("RF", 3, 1, 0), ("ST", 0, 0, 0), ("D", 0, 0, 0), ("H", 3, 0, 0), ("MB", 0, 0, 0),
        ("RF", 3, 2, 0), ("MB", 0, 1, 0), ("MB", 0, 2, 0), ("MB", 0, 3, 0), ("MP", 0, 0, 0),
        ("MP", 0, 1, 0), ("MP", 0, 2, 0), ("RF", 3, 3, 0), ("MP", 0, 3, 0), ("D", 0, 2, 0),
        ("H", 3, 2, 0), ("RF", 2, 2, 1), ("D", 3, 0, 0), ("RF", 2, 3, 1), ("H", 2, 2, 1),
        ("D", 2, 2, 1), ("MO", 0, 0, 0), ("D", 3, 2, 0), ("S", 3, 0, 0), ("D", 2, 0, 1),
        ("S", 3, 1, 0), ("S", 0, 0, 0), ("S", 3, 2, 0), ("S", 0, 1, 0), ("S", 3, 3, 0),
        ("S", 2, 2, 1), ("S", 0, 2, 0), ("S", 2, 3, 1), ("S", 0, 3, 0), ("S", 2, 0, 1),
        ("FIN", 1, 2, 1), ("S", 2, 1, 1), ("FIN", 1, 3, 1), ("FIN", 1, 0, 1), ("DR", 0, 0, 0),
        ("FIN", 1, 1, 1),
    ),
    (
        ("SL", 2, 1, 1), ("SR", 2, 1, 1), ("H", 4, 0, 0), ("MA", 0, 0, 0), ("H", 2, 0, 0),
        ("H", 2, 2, 0), ("RF", 1, 0, 1), ("MA", 0, 1, 0), ("MA", 0, 2, 0), ("RF", 3, 0, 0),
        ("MA", 0, 3, 0), ("D", 4, 0, 0), ("RF", 1, 1, 1), ("RF", 3, 1, 0), ("H", 1, 0, 1),
        ("H", 3, 0, 0), ("RF", 0, 0, 0), ("RF", 3, 2, 0), ("D", 2, 0, 0), ("D", 2, 2, 0),
        ("RF", 0, 1, 0), ("RF", 3, 3, 0), ("SL", 2, 2, 1), ("SL", 2, 3, 1), ("H", 0, 0, 0),
        ("RF", 0, 2, 0), ("H", 3, 2, 0), ("D", 3, 0, 0), ("RF", 0, 3, 0), ("H", 0, 2, 0),
        ("RF", 1, 2, 1), ("D", 0, 0, 0), ("D", 3, 2, 0), ("RF", 1, 3, 1), ("H", 1, 2, 1),
        ("ST", 0, 0, 0), ("D", 0, 2, 0), ("D", 1, 2, 1), ("MB", 0, 0, 0), ("MB", 0, 1, 0),
        ("MB", 0, 2, 0), ("MB", 0, 3, 0), ("MP", 0, 0, 0), ("MP", 0, 1, 0), ("MP", 0, 2, 0),
        ("MP", 0, 3, 0), ("D", 1, 0, 1), ("S", 0, 0, 0), ("S", 0, 1, 0), ("S", 3, 0, 0),
        ("S", 0, 2, 0), ("MO", 0, 0, 0), ("S", 3, 1, 0), ("S", 0, 3, 0), ("S", 1, 2, 1),
        ("S", 1, 3, 1), ("S", 3, 2, 0), ("S", 1, 0, 1), ("S", 3, 3, 0), ("S", 1, 1, 1),
        ("FIN", 2, 2, 1), ("FIN", 2, 3, 1), ("FIN", 2, 0, 1), ("DR", 0, 0, 0), ("FIN", 2, 1, 1),
    ),
    (
        ("SL", 3, 1, 0), ("H", 4, 0, 0), ("MA", 0, 0, 0), ("H", 3, 0, 0), ("MA", 0, 1, 0),
        ("MA", 0, 2, 0), ("MA", 0, 3, 0), ("RX", 2, 0, 1), ("SL", 3, 2, 0), ("SL", 3, 3, 0),
        ("D", 4, 0, 0), ("RX", 2, 1, 1), ("H", 2, 0, 1), ("D", 3, 0, 0), ("RF", 1, 0, 1),
        ("RF", 2, 2, 1), ("RF", 2, 3, 1), ("RF", 0, 0, 0), ("H", 2, 2, 1), ("RF", 1, 1, 1),
        ("D", 2, 2, 1), ("H", 1, 0, 1), ("RF", 0, 1, 0), ("S", 2, 2, 1), ("S", 2, 3, 1),
        ("H", 0, 0, 0), ("RF", 0, 2, 0), ("D", 2, 0, 1), ("RF", 0, 3, 0), ("S", 2, 0, 1),
        ("S", 2, 1, 1), ("H", 0, 2, 0), ("RF", 1, 2, 1), ("D", 0, 0, 0), ("H", 3, 2, 0),
        ("RF", 1, 3, 1), ("S", 0, 0, 0), ("S", 0, 1, 0), ("H", 1, 2, 1), ("D", 0, 2, 0),
        ("ST", 0, 0, 0), ("D", 1, 2, 1), ("S", 0, 2, 0), ("S", 0, 3, 0), ("MB", 0, 0, 0),
        ("MB", 0, 1, 0), ("S", 1, 2, 1), ("S", 1, 3, 1), ("MB", 0, 2, 0), ("MB", 0, 3, 0),
        ("MP", 0, 0, 0), ("MP", 0, 1, 0), ("D", 1, 0, 1), ("MP", 0, 2, 0), ("MP", 0, 3, 0),
        ("D", 3, 2, 0), ("S", 1, 0, 1), ("S", 1, 1, 1), ("FIN", 3, 0, 0), ("FIN", 3, 1, 0),
        ("MO", 0, 0, 0), ("FIN", 3, 2, 0), ("DR", 0, 0, 0), ("FIN", 3, 3, 0),
    ),
)
HEADS = (
    (1, 0, 0),
    (1, 0, 0),
    (1, 1, 0),
    (0, 1, 0),
)


def chip_orders(chips):
    return ORDERS


def packed_orders(chips):
    orders = chip_orders(chips)
    steps = max(len(order) for order in orders)
    steps = -(-steps // 2) * 2
    words = []
    for order in orders:
        codes = [
            (NUMBER[kind] * 64 + source * SPLIT + part) * 2 + turned
            for kind, source, part, turned in order
        ]
        codes = codes + [0] * (steps - len(codes))
        words.append(
            [codes[i] + 32768 * codes[i + 1] for i in range(0, steps, 2)]
        )
    return steps, words


def dot(a, b):
    return jnp.dot(a, b, preferred_element_type=jnp.float32)


def dot_nt(a, b):
    return lax.dot_general(a, b, (((1,), (1,)), ((), ())), preferred_element_type=jnp.float32)


def dot_tn(a, b):
    return lax.dot_general(a, b, (((0,), (0,)), ((), ())), preferred_element_type=jnp.float32)


def fused_kernel(
    count,
    query_hbm,
    forget_hbm,
    value_hbm,
    output_gate_hbm,
    out_weight_hbm,
    x_hbm,
    gate_hbm,
    up_hbm,
    down_hbm,
    shared_gate_hbm,
    shared_up_hbm,
    shared_down_hbm,
    margin_hbm,
    extra_hbm,
    head_gain_hbm,
    index_hbm,
    score_hbm,
    gain_hbm,
    recurrent_ref,
    expert_ref,
    margin_ref,
    extra_ref,
    head_gain_ref,
    index_ref,
    score_ref,
    gain_ref,
    query_v,
    forget_v,
    value_v,
    output_gate_v,
    out_weight_v,
    x_v,
    gate_w,
    up_w,
    down_w,
    rows,
    gates,
    own_hidden,
    peer_hidden,
    result,
    side_result,
    inward,
    final,
    outward,
    local_out,
    carried_query,
    own_state,
    own_decay,
    side_state,
    side_decay,
    before,
    next_state,
    gated,
    mixed,
    mixed_peer,
    load_sem,
    row_sem,
    table_sem,
    right_sem,
    left_sem,
    side_sem,
    cross_sem,
    table_right,
    table_left,
    table_side,
    hidden_send,
    hidden_recv,
    result_send,
    result_recv,
    outward_send,
    inward_recv,
    final_recv,
    state_send,
    state_recv,
    mixed_send,
    mixed_recv,
):
    f32, bf16 = jnp.float32, jnp.bfloat16
    chips = count // 2
    me = lax.axis_index("ep")
    half = lax.axis_index("tp")
    chip, core = me // 2, me % 2
    other = 1 - core
    side = chip * 2 + other
    partner = 1 - half
    has_right, has_left = chip < chips - 1, chip > 0
    length = query_v.shape[0]
    heads = extra_ref.shape[0]
    mine = heads // 2
    part_rows = rows.shape[1]
    units = gate_w.shape[2]
    routed = chips * SPLIT
    last = chips * COARSE
    coarse_rows = GROUP * part_rows
    tiles = 4
    tile = out_weight_v.shape[1] // tiles
    steps, words = packed_orders(chips)

    def half_rows(ref, which):
        return ref.at[pl.ds(pl.multiple_of(which * units, units), units), :]

    loads = dict(
        x=(x_hbm, x_v),
        gain=(gain_hbm, gain_ref),
        index=(index_hbm, index_ref),
        score=(score_hbm, score_ref),
        shared_gate=(shared_gate_hbm, gate_w.at[1]),
        shared_up=(shared_up_hbm, up_w.at[1]),
        forget=(forget_hbm, forget_v),
        query=(query_hbm, query_v),
        value=(value_hbm, value_v),
        margin=(margin_hbm, margin_ref),
        extra=(extra_hbm, extra_ref),
        gate=(gate_hbm.at[0], gate_w.at[0]),
        up=(up_hbm.at[0], up_w.at[0]),
        shared_down0=(half_rows(shared_down_hbm, half), down_w.at[1, 0]),
        shared_down1=(half_rows(shared_down_hbm, partner), down_w.at[1, 1]),
        down0=(half_rows(down_hbm.at[0], half), down_w.at[0, 0]),
        down1=(half_rows(down_hbm.at[0], partner), down_w.at[0, 1]),
        output_gate=(output_gate_hbm, output_gate_v),
        head_gain=(head_gain_hbm, head_gain_ref),
        out_weight=(out_weight_hbm, out_weight_v),
    )
    copies = {
        name: pltpu.make_async_copy(source, target, load_sem.at[i])
        for i, (name, (source, target)) in enumerate(loads.items())
    }
    early = ("x", "gain", "index", "score")
    for name in early:
        copies[name].start()

    barrier = pltpu.get_barrier_semaphore()
    pl.semaphore_signal(barrier, inc=1, device_id={"ep": side}, device_id_type=MESH)
    pl.semaphore_signal(barrier, inc=1, device_id={"tp": partner}, device_id_type=MESH)

    def greet(there):
        pl.semaphore_signal(barrier, inc=1, device_id={"ep": there}, device_id_type=MESH)

    greeted = 2
    if any(kind == "SX" for order in chip_orders(chips) for kind, *_ in order):
        for distance in range(1, chips):
            greet((chip + distance) % chips * 2 + core)
        greeted = greeted + chips - 1
    else:
        pl.when(has_right)(functools.partial(greet, me + 2))
        pl.when(has_left)(functools.partial(greet, me - 2))
        greeted = greeted + has_right.astype(jnp.int32) + has_left.astype(jnp.int32)

    for name in copies:
        if name not in early:
            copies[name].start()

    def loaded(*names):
        for name in names:
            copies[name].wait()

    def remote(source, target, send, recv, **device):
        return pltpu.make_async_remote_copy(
            src_ref=source,
            dst_ref=target,
            send_sem=send,
            recv_sem=recv,
            device_id=device,
            device_id_type=MESH,
        )

    def row_copy(arg, sems, target):
        block = arg * 2 + core
        return remote(rows.at[block], rows.at[block], sems.at[arg], row_sem.at[block], ep=target)

    def cross_copy(arg):
        block = arg * 2 + core
        return remote(
            rows.at[block], rows.at[block], cross_sem.at[arg], row_sem.at[block], tp=partner
        )

    def table_copy(source, sems, target):
        block = source * 2 + core
        return remote(
            gates.at[block], gates.at[block], sems.at[source], table_sem.at[block], ep=target
        )

    def arrived_row(block):
        remote(rows.at[block], rows.at[block], side_sem.at[0], row_sem.at[block], ep=side).wait_recv()

    def arrived_table(block):
        remote(
            gates.at[block], gates.at[block], table_side.at[0], table_sem.at[block], ep=side
        ).wait_recv()

    def hidden_copy(arg):
        return remote(
            own_hidden.at[arg],
            peer_hidden.at[arg],
            hidden_send.at[arg],
            hidden_recv.at[arg],
            tp=partner,
        )

    def result_copy(arg):
        return remote(
            result.at[arg, other],
            side_result.at[arg],
            result_send.at[arg],
            result_recv.at[arg],
            ep=side,
        )

    def outward_copy(arg, target, target_sem, to):
        return remote(outward.at[arg], target, outward_send.at[arg], target_sem, ep=to)

    own_heads = pl.ds(core * mine, mine)
    state_copies = dict(
        state=lambda: remote(
            own_state, side_state, state_send.at[0], state_recv.at[0], ep=side
        ),
        decay=lambda: remote(
            own_decay, side_decay, state_send.at[1], state_recv.at[1], ep=side
        ),
        before=lambda: remote(
            before.at[own_heads],
            before.at[own_heads],
            state_send.at[2],
            state_recv.at[2],
            ep=side,
        ),
        chain=lambda: remote(
            next_state, before.at[own_heads], state_send.at[3], state_recv.at[3], ep=me + 2
        ),
    )

    def mixed_copy(n):
        lanes = pl.ds(pl.multiple_of(n * tile, tile), tile)
        return remote(
            mixed.at[partner, :, lanes],
            mixed_peer.at[:, lanes],
            mixed_send.at[n],
            mixed_recv.at[n],
            tp=partner,
        )

    loaded("x", "gain")

    def norm_rows(part):
        x = x_v[pl.ds(pl.multiple_of(part * part_rows, part_rows), part_rows), :].astype(f32)
        scale = lax.rsqrt(jnp.mean(x * x, axis=1, keepdims=True) + EPSILON)
        rows[(chip * SPLIT + part) * 2 + core] = (x * scale * gain_ref[...]).astype(bf16)

    def of_chip(column):
        value = jnp.int32(HEADS[0][column])
        for c in range(1, chips):
            value = jnp.where(chip == c, HEADS[c][column], value)
        return value

    opening = of_chip(2)
    if CROSSED:
        middle_chip = jnp.logical_and(has_left, has_right)
        shifted = (opening + half * (SPLIT // 2)) % SPLIT
        opening = jnp.where(middle_chip, shifted, opening)
    norm_rows(opening)
    pl.semaphore_wait(barrier, greeted)

    @pl.when(of_chip(0) == 1)
    def _():
        row_copy(chip * SPLIT + opening, right_sem, me + 2).start()

    @pl.when(of_chip(1) == 1)
    def _():
        row_copy(chip * SPLIT + opening, left_sem, me - 2).start()

    for part in range(1, SPLIT):
        norm_rows((opening + part) % SPLIT)
    for part in range(SPLIT):
        row_copy(chip * SPLIT + part, side_sem, side).start()
    loaded("index", "score")
    score = score_ref[...]
    weight = ROUTED_SCALE * score / jnp.sum(score, axis=0, keepdims=True)
    expert = lax.broadcasted_iota(jnp.int32, (count, length), 0)
    table = jnp.zeros((count, length), f32)
    for k in range(score.shape[0]):
        table = table + jnp.where(expert == index_ref[k : k + 1, :], weight[k : k + 1, :], 0.0)
    gates[chip * 2 + core] = table

    @pl.when(has_right)
    def _():
        table_copy(chip, table_right, me + 2).start()

    @pl.when(has_left)
    def _():
        table_copy(chip, table_left, me - 2).start()

    table_copy(chip, table_side, side).start()

    def send_right(arg, first):
        row_copy(arg, right_sem, me + 2).start()

    def send_left(arg, first):
        row_copy(arg, left_sem, me - 2).start()

    def forward(arg, first, onward=True):
        source = arg // SPLIT
        arrived_row(arg * 2 + core)
        to_right = jnp.logical_and(source < chip, has_right)
        to_left = jnp.logical_and(source > chip, has_left)

        @pl.when(first)
        def _():
            arrived_table(source * 2 + core)

            @pl.when(to_right)
            def _():
                table_copy(source, table_right, me + 2).start()

            @pl.when(to_left)
            def _():
                table_copy(source, table_left, me - 2).start()

            table_copy(source, table_side, side).start()

        if onward:

            @pl.when(to_right)
            def _():
                send_right(arg, first)

            @pl.when(to_left)
            def _():
                send_left(arg, first)

        row_copy(arg, side_sem, side).start()

    def cross(arg, first):
        forward(arg, first)
        cross_copy(arg).start()

    def mix_local(arg, first):
        @pl.when(arg == 0)
        def _():
            loaded("forget", "query", "value", "margin", "extra")

        row = lax.broadcasted_iota(jnp.int32, (length, length), 0)
        column = lax.broadcasted_iota(jnp.int32, (length, length), 1)
        upper = row < BLK
        left = column < BLK
        causal = jnp.logical_and(row >= column, upper == left)
        crossed = jnp.logical_and(jnp.logical_not(upper), left)
        ones = causal.astype(f32).astype(bf16)
        head_lane = lax.broadcasted_iota(jnp.int32, (length, heads), 1)
        extra_columns = extra_ref[...].T
        middle = BLK // 2 - 1

        def one_head(h):
            lanes = pl.ds(pl.multiple_of(h * HEAD_CHANNELS, HEAD_CHANNELS), HEAD_CHANNELS)
            query = jax.nn.silu(query_v[:, lanes].astype(f32))
            key = margin_ref[:, lanes] * jax.nn.sigmoid(-forget_v[:, lanes].astype(f32))
            extra = jnp.sum(
                jnp.where(head_lane == h, extra_columns, 0.0), axis=1, keepdims=True
            )
            decay = jnp.log1p(-key) + extra
            high = decay.astype(bf16)
            rest = decay - high.astype(f32)
            mid = rest.astype(bf16)
            low = (rest - mid.astype(f32)).astype(bf16)
            total = dot(ones, high) + dot(ones, mid) + dot(ones, low)
            center = jnp.where(upper, total[middle : middle + 1], total[BLK + middle : BLK + middle + 1])
            end = jnp.where(upper, total[BLK - 1 : BLK], total[2 * BLK - 1 : 2 * BLK])
            first = jnp.exp(total[BLK - 1 : BLK])
            second = jnp.exp(total[2 * BLK - 1 : 2 * BLK])
            query_end = query * jnp.exp(total)
            key_end = key * jnp.exp(end - total)
            near = dot_nt(
                (query * jnp.exp(total - center)).astype(bf16),
                (key * jnp.exp(center - total)).astype(bf16),
            )
            far = dot_nt(query_end.astype(bf16), key_end.astype(bf16))
            scores = jnp.where(causal, near, jnp.where(crossed, far, 0.0)).astype(bf16)
            value = value_v[:, lanes]
            local_out[:, lanes] = dot(scores, value)
            carried_query[:, lanes] = jnp.where(upper, query_end, query_end * first).astype(bf16)
            key_state = jnp.where(upper, key_end * second, key_end).astype(bf16)
            own_state[h] = dot_tn(value, key_state).astype(bf16)
            own_decay[pl.ds(h, 1), :] = first * second

        one_head(2 * arg)
        one_head(2 * arg + 1)

        @pl.when(arg == heads // 2 - 1)
        def _():
            state_copies["state"]().start()
            state_copies["decay"]().start()

    def mix_state(arg, first):
        state_copies["state"]().wait_recv()
        state_copies["decay"]().wait_recv()

        @pl.when(has_left)
        def _():
            state_copies["chain"]().wait_recv()
            state_copies["before"]().start()

        @pl.when(jnp.logical_not(has_left))
        def _():
            before[...] = jnp.zeros(before.shape, bf16)

        @pl.when(has_right)
        def _():
            def one_head(i, _):
                h = core * mine + i
                own, beside = own_state[h].astype(f32), side_state[h].astype(f32)
                own_d, beside_d = own_decay[pl.ds(h, 1), :], side_decay[pl.ds(h, 1), :]
                state0 = jnp.where(core == 0, own, beside)
                state1 = jnp.where(core == 0, beside, own)
                decay1 = jnp.where(core == 0, beside_d, own_d)
                carried = before[h].astype(f32) * (own_d * beside_d)
                next_state[i] = (carried + decay1 * state0 + state1).astype(bf16)
                return 0

            lax.fori_loop(0, mine, one_head, 0)
            state_copies["chain"]().start()

    def mix_finish(arg, first):
        @pl.when(arg == 0)
        def _():
            loaded("output_gate", "head_gain")

        @pl.when(jnp.logical_and(arg == 0, has_left))
        def _():
            state_copies["before"]().wait_recv()

        def one_head(h):
            lanes = pl.ds(pl.multiple_of(h * HEAD_CHANNELS, HEAD_CHANNELS), HEAD_CHANNELS)
            state = before[h].astype(f32)
            beside = side_state[h].astype(f32)
            later = side_decay[pl.ds(h, 1), :] * state + beside
            state = jnp.where(core == 0, state, later).astype(bf16)
            out = local_out[:, lanes] + dot_nt(carried_query[:, lanes], state)
            factor = lax.rsqrt(jnp.mean(out * out, axis=1, keepdims=True) + EPSILON)
            gate = jax.nn.silu(output_gate_v[:, lanes].astype(f32))
            gated[:, lanes] = (out * factor * head_gain_ref[:, lanes] * gate).astype(bf16)

        one_head(2 * arg)
        one_head(2 * arg + 1)

    def mix_project(arg, first):
        @pl.when(arg == 0)
        def _():
            loaded("out_weight")

        kept = length // 2
        lanes = pl.ds(pl.multiple_of(arg * tile, tile), tile)
        partial = dot(gated[...], out_weight_v[:, lanes]).astype(bf16)
        mixed[0, :, lanes] = partial[:kept]
        mixed[1, :, lanes] = partial[kept:]

        mixed_copy(arg).start()

    def mix_out(arg, first):
        for n in range(tiles):
            mixed_copy(n).wait_recv()

        recurrent_ref[...] = (mixed[half].astype(f32) + mixed_peer[...].astype(f32)).astype(bf16)

    def hidden_part(arg, first):
        shared = arg == routed
        chunk = arg // GROUP
        source, place = chunk // COARSE, chunk % COARSE

        @pl.when(shared)
        def _():
            loaded("shared_gate", "shared_up")

        @pl.when(jnp.logical_and(source == chip, first))
        def _():
            loaded("gate", "up")

        @pl.when(jnp.logical_not(shared))
        def _():
            for p in range(GROUP):
                arrived_row((arg + p) * 2 + other)

            @pl.when(first)
            def _():
                arrived_table(source * 2 + other)

        which = shared.astype(jnp.int32)
        pieces = []
        for parity in range(2):
            for p in range(GROUP):
                own = (chip * SPLIT + parity * GROUP + p) * 2 + core
                pieces.append(rows[jnp.where(shared, own, (arg + p) * 2 + parity)])
        x = jnp.concatenate(pieces, axis=0)
        lane = lax.broadcasted_iota(jnp.int32, (length, count), 1)
        block_low = jnp.where(shared, chip * 2 + core, source * 2)
        block_high = jnp.where(shared, chip * 2 + core, source * 2 + 1)

        def own_gate(block):
            column = jnp.sum(jnp.where(lane == me, gates[block].T, 0.0), axis=1, keepdims=True)
            return jnp.where(place == 0, column[:coarse_rows], column[coarse_rows:])

        routed_gate = jnp.concatenate([own_gate(block_low), own_gate(block_high)], axis=0)
        scale = jnp.where(shared, 1.0, routed_gate)
        gate_part = dot(x, gate_w[which])
        up_part = dot(x, up_w[which])
        own_hidden[chunk] = (jax.nn.silu(gate_part) * up_part * scale).astype(bf16)
        hidden_copy(chunk).start()

    def down_part(arg, first):
        shared = arg == routed
        chunk = arg // GROUP
        which = shared.astype(jnp.int32)

        @pl.when(shared)
        def _():
            loaded("shared_down0", "shared_down1")

        @pl.when(jnp.logical_and(chunk // COARSE == chip, first))
        def _():
            loaded("down0", "down1")

        hidden_copy(chunk).wait_recv()
        out = dot(own_hidden[chunk], down_w[which, 0]) + dot(peer_hidden[chunk], down_w[which, 1])
        out = out.astype(bf16)
        result[chunk, 0] = out[:coarse_rows]
        result[chunk, 1] = out[coarse_rows:]

        @pl.when(jnp.logical_not(shared))
        def _():
            result_copy(chunk).start()

    def part_slice(arg):
        return pl.ds(pl.multiple_of(arg % GROUP * part_rows, part_rows), part_rows)

    def chip_sum(arg, awaited):
        chunk = arg // GROUP

        @pl.when(awaited)
        def _():
            result_copy(chunk).wait_recv()

        inside = part_slice(arg)
        return result[chunk, core, inside].astype(f32) + side_result[chunk, inside].astype(f32)

    def final_copy(arg):
        slot = chip * SPLIT + arg % SPLIT
        there = arg // SPLIT * 2 + core
        return outward_copy(arg, final.at[slot], final_recv.at[slot], there)

    def send_sum(arg, first, direct):
        target = arg // SPLIT
        adjacent = jnp.abs(target - chip) == 1
        total = chip_sum(arg, arg % GROUP == 0)
        if direct:
            outward[arg] = total.astype(bf16)
            final_copy(arg).start()
            return
        inner = jnp.logical_and(has_left, has_right)
        towards = jnp.where(target > chip, me + 2, me - 2)
        relay = outward_copy(arg, inward.at[arg], inward_recv.at[arg], towards)

        @pl.when(inner)
        def _():
            relay.wait_recv()
            outward[arg] = (total + inward[arg].astype(f32)).astype(bf16)

        @pl.when(jnp.logical_not(inner))
        def _():
            outward[arg] = total.astype(bf16)

        @pl.when(adjacent)
        def _():
            final_copy(arg).start()

        @pl.when(jnp.logical_not(adjacent))
        def _():
            relay.start()

    def finish(arg, first, left_all, right_all):
        part = arg % SPLIT
        place = pl.ds(pl.multiple_of(part * part_rows, part_rows), part_rows)
        shared = result[last, part // GROUP, part_slice(arg)].astype(f32)
        total = chip_sum(arg, arg % GROUP == 0) + shared
        for s in range(chips):
            taken = jnp.abs(chip - s) == 1
            if left_all:
                taken = jnp.logical_or(taken, chip > s)
            if right_all:
                taken = jnp.logical_or(taken, chip < s)
            slot = s * SPLIT + part

            @pl.when(taken)
            def _():
                outward_copy(arg, final.at[slot], final_recv.at[slot], side).wait_recv()

            total = total + jnp.where(taken, final[slot].astype(f32), 0.0)
        expert_ref[place, :] = total.astype(bf16)

    def drain_all(_, first):
        def drain(arg, _):
            source, part = arg // SPLIT, arg % SPLIT
            row_copy(arg, side_sem, side).wait_send()
            to_right = jnp.logical_and(source <= chip, has_right)
            to_left = jnp.logical_and(source >= chip, has_left)
            row_right, row_left = to_right, to_left
            if CROSSED:
                inner = jnp.logical_and(source > 0, source < chips - 1)
                kept = (part + half * (SPLIT // 2)) % SPLIT < SPLIT // 2

                def crosses(end):
                    if CROSSED == 2:
                        return inner
                    return jnp.logical_and(inner, jnp.abs(source - end) == 1)

                held = jnp.logical_not(kept)
                to_last = jnp.logical_and(chip == chips - 2, crosses(chips - 1))
                to_first = jnp.logical_and(chip == 1, crosses(0))
                row_right = jnp.logical_and(to_right, jnp.logical_not(jnp.logical_and(held, to_last)))
                row_left = jnp.logical_and(to_left, jnp.logical_not(jnp.logical_and(held, to_first)))
                ends = jnp.logical_or(
                    jnp.logical_and(chip == chips - 1, crosses(chips - 1)),
                    jnp.logical_and(chip == 0, crosses(0)),
                )

                @pl.when(jnp.logical_and(ends, kept))
                def _():
                    cross_copy(arg).wait_send()

            @pl.when(row_right)
            def _():
                row_copy(arg, right_sem, me + 2).wait_send()

            @pl.when(row_left)
            def _():
                row_copy(arg, left_sem, me - 2).wait_send()

            @pl.when(source != chip)
            def _():
                outward_copy(arg, inward.at[arg], inward_recv.at[arg], side).wait_send()

            @pl.when(part == 0)
            def _():
                table_copy(source, table_side, side).wait_send()

                @pl.when(to_right)
                def _():
                    table_copy(source, table_right, me + 2).wait_send()

                @pl.when(to_left)
                def _():
                    table_copy(source, table_left, me - 2).wait_send()

            return 0

        lax.fori_loop(0, routed, drain, 0)

        def drain_chunk(chunk, _):
            hidden_copy(chunk).wait_send()
            result_copy(chunk).wait_send()
            return 0

        lax.fori_loop(0, last, drain_chunk, 0)
        hidden_copy(last).wait_send()
        state_copies["state"]().wait_send()
        state_copies["decay"]().wait_send()

        @pl.when(has_left)
        def _():
            state_copies["before"]().wait_send()

        @pl.when(has_right)
        def _():
            state_copies["chain"]().wait_send()

        for n in range(tiles):
            mixed_copy(n).wait_send()

    actions = dict(
        SR=send_right,
        SL=send_left,
        RF=forward,
        RX=cross,
        RN=functools.partial(forward, onward=False),
        MA=mix_local,
        ST=mix_state,
        H=hidden_part,
        D=down_part,
        S=functools.partial(send_sum, direct=False),
        SX=functools.partial(send_sum, direct=True),
        FIN=functools.partial(finish, left_all=False, right_all=False),
        FL=functools.partial(finish, left_all=True, right_all=False),
        FR=functools.partial(finish, left_all=False, right_all=True),
        FB=functools.partial(finish, left_all=True, right_all=True),
        MB=mix_finish,
        MP=mix_project,
        MO=mix_out,
        DR=drain_all,
    )
    mine_words = []
    for n in range(steps // 2):
        word = jnp.int32(words[0][n])
        for c in range(1, chips):
            word = jnp.where(chip == c, words[c][n], word)
        mine_words.append(word)

    def turn(i, _):
        place, digit = i // 2, i % 2
        word = mine_words[0]
        for n in range(1, steps // 2):
            word = jnp.where(place == n, mine_words[n], word)
        code = jnp.where(
            digit == 0, word % 32768, word // 32768
        )
        kind, arg, turned = code // 128, code // 2 % 64, code % 2
        first = arg % SPLIT == 0
        shift = (arg % SPLIT + half * (SPLIT // 2)) % SPLIT
        arg = jnp.where(turned == 1, arg // SPLIT * SPLIT + shift, arg)
        for name, action in actions.items():

            @pl.when(kind == NUMBER[name])
            def _():
                action(arg, first)

        return 0

    lax.fori_loop(0, steps, turn, 0)


def fused_fits(position_decay_extra, chosen_expert_index, routed_gate_weight):
    count, tensor = lax.axis_size("ep"), lax.axis_size("tp")
    length, heads = position_decay_extra.shape
    tokens, top = chosen_expert_index.shape
    every_row_fits = 2 * top >= count and routed_gate_weight.shape[0] == 1
    sizes = length == tokens == 2 * BLK and heads % 2 == 0
    return every_row_fits and sizes and tensor == 2 and count % 2 == 0 and count == 2 * len(ORDERS)


def fused_layer(
    recurrence_query_input,
    forget_gate_input,
    recurrence_value_input,
    output_gate_input,
    forget_lower_margin,
    position_decay_extra,
    head_norm_gain,
    recurrence_out_weight,
    expert_hidden_state,
    chosen_expert_index,
    chosen_expert_score,
    expert_norm_gain,
    routed_gate_weight,
    routed_up_weight,
    routed_down_weight,
    shared_gate_weight,
    shared_up_weight,
    shared_down_weight,
):
    f32, bf16 = jnp.float32, jnp.bfloat16
    count = lax.axis_size("ep")
    chips = count // 2
    routed = chips * SPLIT
    length, channels = recurrence_query_input.shape
    heads = position_decay_extra.shape[1]
    width, width_out = expert_hidden_state.shape[1], recurrence_out_weight.shape[1]
    units, features = routed_gate_weight.shape[2], routed_down_weight.shape[2]
    part_rows = length // SPLIT
    hbm = pl.BlockSpec(memory_space=pltpu.HBM)
    vmem = pl.BlockSpec(memory_space=pltpu.VMEM)
    dma = pltpu.SemaphoreType.DMA
    mixer_rows = pltpu.VMEM((length, channels), bf16)
    coarse_rows = length // COARSE
    chunks = chips * COARSE + 1
    hidden = pltpu.VMEM((chunks, 2 * coarse_rows, units), bf16)
    partial = pltpu.VMEM((routed, part_rows, features), bf16)
    state = pltpu.VMEM((heads, HEAD_CHANNELS, HEAD_CHANNELS), bf16)
    decay = pltpu.VMEM((heads, HEAD_CHANNELS), f32)
    large = [
        pltpu.with_memory_space_constraint(array, pltpu.HBM)
        for array in (
            recurrence_query_input,
            forget_gate_input,
            recurrence_value_input,
            output_gate_input,
            recurrence_out_weight,
            expert_hidden_state,
            routed_gate_weight,
            routed_up_weight,
            routed_down_weight,
            shared_gate_weight,
            shared_up_weight,
            shared_down_weight,
            forget_lower_margin[None, :],
            position_decay_extra.T,
            head_norm_gain[None, :],
            chosen_expert_index.T,
            chosen_expert_score.T,
            expert_norm_gain[None, :],
        )
    ]
    return pl.pallas_call(
        functools.partial(fused_kernel, count),
        out_shape=(
            jax.ShapeDtypeStruct((length // 2, width_out), bf16),
            jax.ShapeDtypeStruct((length, features), bf16),
        ),
        in_specs=[hbm] * 18,
        out_specs=(vmem, vmem),
        scratch_shapes=[
            *(pltpu.VMEM(array.shape, array.dtype) for array in large[12:]),
            mixer_rows,
            mixer_rows,
            mixer_rows,
            mixer_rows,
            pltpu.VMEM(recurrence_out_weight.shape, bf16),
            pltpu.VMEM((length, width), bf16),
            pltpu.VMEM((2, width, units), bf16),
            pltpu.VMEM((2, width, units), bf16),
            pltpu.VMEM((2, 2, units, features), bf16),
            pltpu.VMEM((routed * 2, part_rows, width), bf16),
            pltpu.VMEM((count, count, length), f32),
            hidden,
            hidden,
            pltpu.VMEM((chunks, 2, coarse_rows, features), bf16),
            pltpu.VMEM((chunks, coarse_rows, features), bf16),
            partial,
            partial,
            partial,
            pltpu.VMEM((length, channels), f32),
            mixer_rows,
            state,
            decay,
            state,
            decay,
            state,
            pltpu.VMEM((heads // 2, HEAD_CHANNELS, HEAD_CHANNELS), bf16),
            mixer_rows,
            pltpu.VMEM((2, length // 2, width_out), bf16),
            pltpu.VMEM((length // 2, width_out), bf16),
            dma((20,)),
            dma((routed * 2,)),
            dma((count,)),
            dma((routed,)),
            dma((routed,)),
            dma((routed,)),
            dma((routed,)),
            dma((chips,)),
            dma((chips,)),
            dma((chips,)),
            dma((chunks,)),
            dma((chunks,)),
            dma((chunks,)),
            dma((chunks,)),
            dma((routed,)),
            dma((routed,)),
            dma((routed,)),
            dma((4,)),
            dma((4,)),
            dma((4,)),
            dma((4,)),
        ],
        compiler_params=pltpu.CompilerParams(
            collective_id=0, has_side_effects=True, vmem_limit_bytes=46 * 1024 * 1024
        ),
        cost_estimate=pl.CostEstimate(
            flops=9_000_000_000, bytes_accessed=18_000_000, transcendentals=0
        ),
        name="fused_kernel",
    )(
        *large,
    )


def per_device(
    recurrence_query_input,
    forget_gate_input,
    recurrence_value_input,
    output_gate_input,
    forget_lower_margin,
    position_decay_extra,
    head_norm_gain,
    recurrence_out_weight,
    expert_hidden_state,
    chosen_expert_index,
    chosen_expert_score,
    expert_norm_gain,
    routed_gate_weight,
    routed_up_weight,
    routed_down_weight,
    shared_gate_weight,
    shared_up_weight,
    shared_down_weight,
):
    if fused_fits(position_decay_extra, chosen_expert_index, routed_gate_weight):
        return fused_layer(
            recurrence_query_input,
            forget_gate_input,
            recurrence_value_input,
            output_gate_input,
            forget_lower_margin,
            position_decay_extra,
            head_norm_gain,
            recurrence_out_weight,
            expert_hidden_state,
            chosen_expert_index,
            chosen_expert_score,
            expert_norm_gain,
            routed_gate_weight,
            routed_up_weight,
            routed_down_weight,
            shared_gate_weight,
            shared_up_weight,
            shared_down_weight,
        )
    recurrence_output = mixer_half(
        recurrence_query_input,
        forget_gate_input,
        recurrence_value_input,
        output_gate_input,
        forget_lower_margin,
        position_decay_extra,
        head_norm_gain,
        recurrence_out_weight,
    )
    expert_out = expert_half(
        expert_hidden_state,
        chosen_expert_index,
        chosen_expert_score,
        expert_norm_gain,
        routed_gate_weight,
        routed_up_weight,
        routed_down_weight,
        shared_gate_weight,
        shared_up_weight,
        shared_down_weight,
    )
    return (recurrence_output, expert_out)


def solution(mesh):
    in_specs = (
        P(("grp", "ep"), "tp"),
        P(("grp", "ep"), "tp"),
        P(("grp", "ep"), "tp"),
        P(("grp", "ep"), "tp"),
        P("tp"),
        P(("grp", "ep"), "tp"),
        P("tp"),
        P("tp", None),
        P(("grp", "ep"), None),
        P(("grp", "ep"), None),
        P(("grp", "ep"), None),
        P(),
        P("ep", None, "tp"),
        P("ep", None, "tp"),
        P("ep", None, "tp"),
        P(None, "tp"),
        P(None, "tp"),
        P(None, "tp"),
    )
    out_specs = (P(("grp", "ep", "tp"), None), P(("grp", "ep"), "tp"))
    return jax.shard_map(
        per_device, mesh=mesh, in_specs=in_specs, out_specs=out_specs, check_vma=False
    )
```
